32 devices in a mesh: sp: 16 (over z, y, x), tp: 2 (over core).
Axes of the slice: x: 2, y: 2, z: 4, core: 2. Of those that a mesh axis runs over, the one named last changes fastest.
Arguments:
- tokens: bfloat16 [4096, 2048], P('sp', 'tp'), may hold values from -24 to 24
- value_weight: bfloat16 [2, 2048, 2048], P(None, 'sp', 'tp'), may hold values from -0.125 to 0.125
- outer_weight: bfloat16 [2, 2048, 2048], P(None, 'sp', 'tp'), may hold values from -0.125 to 0.125
- inner_weight: bfloat16 [2, 2048, 2048], P(None, 'sp', 'tp'), may hold values from -0.125 to 0.125
- conv_taps: float32 [2, 3, 2048], P(None, None, 'tp'), may hold values from -3.5 to 3.5
- output_weight: bfloat16 [2, 2048, 2048], P(None, 'tp', 'sp'), may hold values from -2 to 2
- norm_gain: float32 [2, 2048], P(None, 'tp'), may hold values from 0.1 to 1.9
- norm_bias: float32 [2, 2048], P(None, 'tp'), may hold values from -3 to 3
Outputs:
- mixed_out: bfloat16 [4096, 2048], P('sp', 'tp')
The draws below stay inside these ranges and needn't reach their ends.
All inputs are finite; a program needn't handle non-finite values.
Results may differ from the reference program's by a relative error of at most 0.03.
Values may be sent and summed in bfloat16 or wider, within the bound.
A program may use at most 64 MiB of HBM per device.

```python
import jax
import jax.numpy as jnp
from jax import lax

D = 2048
CW = 2048
CONV_K = 3
LAYERS = 2
TOKENS = 4096
N_TP = 2


def column_scale(key, width):
    position = jnp.arange(width, dtype=jnp.float32) / width
    rough = jax.random.uniform(key, (width,), jnp.float32, 0.6, 1.4)
    return jnp.exp(jnp.log(4.0) * position) * rough


def draw_tokens(key, part):
    first, second = jax.random.split(jax.random.fold_in(key, 11), 2)
    scales = column_scale(second, D)
    base = jnp.clip(jax.random.normal(first, (TOKENS, D), jnp.float32), -5.0, 5.0)
    return jnp.clip(base * scales[None, :], -24.0, 24.0).astype(jnp.bfloat16)


def draw_output_weight(key, part):
    first, second = jax.random.split(jax.random.fold_in(key, 23), 2)
    scales = column_scale(second, D)
    base = jnp.clip(jax.random.normal(first, (LAYERS, CW, D), jnp.float32), -5.0, 5.0)
    values = base * scales[None, None, :] * CW ** (-0.5)
    return jnp.clip(values, -2.0, 2.0).astype(jnp.bfloat16)


def block_levels(rng, shape, pieces, low, top_value):
    loudness, own = 1.0, jax.random.fold_in(rng, 6)
    for dim, shards_of in pieces:
        draws = jnp.exp(jax.random.uniform(jax.random.fold_in(own, dim), (shards_of,), jnp.float32, low / len(pieces), top_value / len(pieces)))
        loudness = loudness * jnp.repeat(draws, shape[dim] // shards_of).reshape([-1 if axis == dim else 1 for axis in range(len(shape))])
    return loudness


def scatter_about(own_key, extent, spread, reach, cuts=(), kind=jnp.bfloat16):
    level = block_levels(own_key, extent, cuts, -0.22, 0.18) if cuts else 1.0
    array = jax.random.normal(own_key, extent, jnp.float32) * spread * level
    return jnp.minimum(jnp.maximum(array, -reach), reach).astype(kind)


def setup_inputs(seed: int = 0) -> dict:
    key_list = jax.random.split(jax.random.key(seed), 9)
    return {
        "tokens": draw_tokens(jax.random.fold_in(key_list[8], 71), 0),
        "value_weight": scatter_about(key_list[1], (LAYERS, D, CW), D ** -0.5, 0.125, ((1, 16), (2, 2))),
        "outer_weight": scatter_about(key_list[2], (LAYERS, D, CW), D ** -0.5, 0.125, ((1, 16), (2, 2))),
        "inner_weight": scatter_about(key_list[3], (LAYERS, D, CW), D ** -0.5, 0.125, ((1, 16), (2, 2))),
        "conv_taps": scatter_about(key_list[4], (LAYERS, CONV_K, CW), CONV_K ** -0.5, 3.5, ((2, 2),), jnp.float32),
        "output_weight": draw_output_weight(jax.random.fold_in(key_list[8], 71), 0),
        "norm_gain": jnp.clip(1.0 + 0.18 * jax.random.normal(key_list[6], (LAYERS, D), jnp.float32), 0.1, 1.9),
        "norm_bias": scatter_about(key_list[7], (LAYERS, D), 0.5, 3.0, ((1, 2),), jnp.float32),
    }


def reference(tokens, value_weight, outer_weight, inner_weight, conv_taps, output_weight, norm_gain, norm_bias):
    alpha = (2.0 * LAYERS) ** 0.25
    state = tokens
    width = CW // N_TP
    for layer in range(LAYERS):
        u_part = jnp.dot(state, value_weight[layer], preferred_element_type=jnp.float32).astype(jnp.bfloat16)
        outer = jnp.dot(state, outer_weight[layer], preferred_element_type=jnp.float32).astype(jnp.bfloat16)
        inner = jnp.dot(state, inner_weight[layer], preferred_element_type=jnp.float32).astype(jnp.bfloat16)
        gated_in = inner.astype(jnp.float32) * u_part.astype(jnp.float32)
        padded = jnp.concatenate([jnp.zeros((CONV_K - 1, CW), jnp.float32), gated_in], axis=0)
        conv = jnp.zeros_like(gated_in)
        for tap in range(CONV_K):
            conv = conv + conv_taps[layer, tap][None, :] * padded[tap:tap + gated_in.shape[0]]
        gated = (outer.astype(jnp.float32) * conv).astype(jnp.bfloat16)
        branch = jnp.zeros((gated.shape[0], D), jnp.float32)
        for block in range(N_TP):
            part_sum = jnp.dot(gated[:, block * width:(block + 1) * width], output_weight[layer, block * width:(block + 1) * width], preferred_element_type=jnp.float32).astype(jnp.bfloat16)
            branch = branch + lax.optimization_barrier(part_sum).astype(jnp.float32)
        pre = alpha * state.astype(jnp.float32) + branch
        mean = lax.optimization_barrier(jnp.mean(pre, axis=-1, keepdims=True))
        var = lax.optimization_barrier(jnp.mean(jnp.square(pre - mean), axis=-1, keepdims=True))
        normed = (pre - mean) * lax.rsqrt(var + 1e-05)
        state = (normed * norm_gain[layer][None, :] + norm_bias[layer][None, :]).astype(jnp.bfloat16)
    return state
```

```python
import jax
import jax.numpy as jnp
from jax import lax
from jax.experimental import pallas as pl
from jax.experimental.pallas import tpu as pltpu
from jax.sharding import PartitionSpec as P

LANES = 128
EPS = 1e-5


def flip(j, i):
    if i & 1:
        j = j + 1 - 2 * lax.rem(j, 2)
    if i & 2:
        j = j + 2 - 4 * lax.rem(lax.div(j, 2), 2)
    return j


def plane_size(sp, channels):
    q = 4
    while q > 1 and (sp % q or channels // q < LANES or channels % q):
        q //= 2
    return q


def make_kernel(sp, tp, q, layers, taps_count, rows, feats, depth, width, out_cols, alpha):
    line = sp // q
    units = layers * 4
    model = feats * tp
    per_half = sp // tp
    steps = line - 1
    halves = 2 if q == 4 else 1
    half_rows = rows // halves
    timed = line == 4 and q == 4 and tp == 2
    slots = line // tp if timed else 1
    block_cols = q * out_cols

    def kernel(
        tok, val, outw, inn, taps, prj, gain, bias, res,
        xg, win, wout, ubuf, obuf, zpad, gated, part, rec1, snd2, rec2, acc, stat, stat_in, halo,
        a_send, a_recv, a_loc, u_send, u_recv, d_send, d_recv,
        g_send, g_recv, g_loc, t_send, t_recv, p_send, p_recv, r_send, r_recv, s_send, s_recv, h_send, h_recv,
        b_send, b_recv,
    ):
        me = lax.axis_index("sp")
        c = lax.axis_index("tp")
        l = lax.div(me, q)
        j = lax.rem(me, q)

        def at_sp(other):
            return {"sp": other, "tp": c}

        def at_tp(r):
            return {"sp": me, "tp": lax.rem(c + r, tp)}

        def remote(src, dst, ssem, rsem, dev):
            return pltpu.make_async_remote_copy(
                src_ref=src, dst_ref=dst, send_sem=ssem, recv_sem=rsem,
                device_id=dev, device_id_type=pl.DeviceIdType.MESH,
            )

        def peer(i):
            return l * q + flip(j, i)

        barrier = pltpu.get_barrier_semaphore()

        def greet(dev):
            pl.semaphore_signal(barrier, inc=1, device_id=dev, device_id_type=pl.DeviceIdType.MESH)

        for i in range(1, q):
            greet(at_sp(peer(i)))
        for r in range(1, tp):
            greet(at_tp(r))

        @pl.when(l > 0)
        def _():
            greet(at_sp(me - q))

        @pl.when(l < line - 1)
        def _():
            greet(at_sp(me + q))

        neighbours = (l > 0).astype(jnp.int32) + (l < line - 1).astype(jnp.int32)
        pl.semaphore_wait(barrier, (q - 1) + (tp - 1) + neighbours)


        ORDER = (val, inn, outw, prj)

        def own_piece(k, jd):
            layer, w = divmod(k, 4)
            at = pl.ds(pl.multiple_of(jd * width, width), width)
            if w == 3:
                return prj.at[layer, at, :]
            return ORDER[w].at[layer, :, at]

        def landed(k, s):
            layer, w = divmod(k, 4)
            if w == 3:
                return wout.at[layer, s]
            return win.at[layer, w, pl.ds(pl.multiple_of(s * depth, depth), depth), :]

        def block(k, b):
            layer, w = divmod(k, 4)
            if w == 3:
                return wout.at[layer, pl.ds(b * q, q)]
            return win.at[layer, w, pl.ds(pl.multiple_of(b * (q * depth), q * depth), q * depth), :]

        def a_copy(k, i):
            return remote(own_piece(k, flip(j, i)), landed(k, me), a_send.at[k, i], a_recv.at[k, i], at_sp(peer(i)))

        def a_local(k):
            return pltpu.make_async_copy(own_piece(k, j), landed(k, me), a_loc.at[k])

        def scatter_start(k):
            a_local(k).start()
            for i in range(q - 1, 0, -1):
                a_copy(k, i).start()

        def scatter_wait(k):
            a_local(k).wait()
            for i in range(q - 1, 0, -1):
                a_copy(k, i).wait()

        def up(k, s):
            return remote(block(k, l - s), block(k, l - s), u_send.at[k, s], u_recv.at[k, s], at_sp(me + q))

        def down(k, s):
            return remote(block(k, l + s), block(k, l + s), d_send.at[k, s], d_recv.at[k, s], at_sp(me - q))

        def line_begin(k):
            scatter_wait(k)

            @pl.when(l < line - 1)
            def _():
                up(k, 0).start()

            @pl.when(l > 0)
            def _():
                down(k, 0).start()

        def line_pass(k, s):
            @pl.when((l - s >= 0) & (l < line - 1))
            def _():
                up(k, s - 1).wait_recv()
                up(k, s).start()

            @pl.when((l + s < line) & (l > 0))
            def _():
                down(k, s - 1).wait_recv()
                down(k, s).start()

        def line_end(k, s):
            @pl.when((l == line - 1) & (l - 1 - s >= 0))
            def _():
                up(k, s).wait_recv()

            @pl.when((l == 0) & (l + 1 + s < line))
            def _():
                down(k, s).wait_recv()

        def arrived(k):
            for s in range(steps):
                line_end(k, s)

        def line_sent(k, s):
            @pl.when((l - s >= 0) & (l < line - 1))
            def _():
                up(k, s).wait_send()

            @pl.when((l + s < line) & (l > 0))
            def _():
                down(k, s).wait_send()


        def part_of(h):
            return pl.ds(h * half_rows, half_rows)

        def spot(layer, jj, h):
            at = pl.ds(pl.multiple_of(jj * rows + h * half_rows, half_rows), half_rows)
            return xg.at[layer, c, at, :]

        def mine(layer, h):
            return tok.at[part_of(h)] if layer == 0 else spot(layer, j, h)

        def g_copy(layer, i, h):
            if i == 3:
                src = spot(layer, flip(j, 1 + h), h)
                return remote(src, src, g_send.at[layer, i, h], g_recv.at[layer, i, h], at_sp(peer(2 - h)))
            return remote(
                mine(layer, h), spot(layer, j, h), g_send.at[layer, i, h], g_recv.at[layer, i, h], at_sp(peer(i))
            )

        def g_local(h):
            return pltpu.make_async_copy(tok.at[part_of(h)], spot(0, j, h), g_loc.at[h])

        def t_copy(layer, r, i, h):
            src = mine(layer, h) if i == 0 else spot(layer, flip(j, i), h)
            return remote(
                src, spot(layer, flip(j, i), h), t_send.at[layer, r, i, h], t_recv.at[layer, r, i, h], at_tp(r)
            )

        def cross_start(layer, i, h):
            for r in range(1, tp):
                t_copy(layer, r, i, h).start()

        def gather_start(layer, h):
            if layer == 0:
                g_local(h).start()
            for i in range(1, min(q, 3)):
                g_copy(layer, i, h).start()
            cross_start(layer, 0, h)

        def gather_pass(layer, h):
            first = 1 + h if q == 4 else 1
            for i in range(1, min(q, 3)):
                i = first if i == 1 else 3 - first
                g_copy(layer, i, h).wait_recv()
                if q == 4 and i == first:
                    g_copy(layer, 3, h).start()
                cross_start(layer, i, h)

        def gather_last(layer, h):
            if q == 4:
                g_copy(layer, 3, h).wait_recv()
                cross_start(layer, 3, h)

        def gather_wait(layer):
            for h in range(halves):
                if layer == 0:
                    g_local(h).wait()
                for i in range(q):
                    for r in range(1, tp):
                        t_copy(layer, r, i, h).wait_recv()

        def gather_sent(layer):
            for h in range(halves):
                for i in range(1, q):
                    g_copy(layer, i, h).wait_send()
                for i in range(q):
                    for r in range(1, tp):
                        t_copy(layer, r, i, h).wait_send()

        def tile_at(jj):
            return pl.ds(pl.multiple_of(jj * rows, rows), rows)

        def project(layer, w, store):
            def tile(i, carry):
                at = tile_at(i)
                total = jnp.zeros((rows, width), jnp.float32)
                for cc in range(tp):
                    total = total + jnp.dot(
                        xg[layer, cc, at, :],
                        win[layer, w, pl.ds(cc * feats, feats), :],
                        preferred_element_type=jnp.float32,
                    )
                store(i, total.astype(jnp.bfloat16))
                return carry

            lax.fori_loop(0, q, tile, 0)

        def put_u(i, v):
            ubuf[tile_at(i), :] = v

        def put_o(i, v):
            obuf[tile_at(i), :] = v

        def put_z(i, v):
            at = tile_at(i)
            zpad[pl.ds(pl.multiple_of(8 + i * rows, 8), rows), :] = v.astype(jnp.float32) * ubuf[at, :].astype(jnp.float32)

        def h_copy(layer):
            return remote(
                halo.at[layer, 0], halo.at[layer, 1], h_send.at[layer], h_recv.at[layer], at_sp(me + q)
            )

        def halo_start(layer):
            halo[layer, 0] = zpad[pl.ds(q * rows, 8), :]

            @pl.when(l < line - 1)
            def _():
                h_copy(layer).start()

        def halo_wait(layer):
            zpad[0:8, :] = jnp.zeros((8, width), jnp.float32)

            @pl.when(l > 0)
            def _():
                h_copy(layer).wait_recv()
                zpad[0:8, :] = halo[layer, 1]

            @pl.when(l < line - 1)
            def _():
                h_copy(layer).wait_send()

        def convolve(layer):
            at_c = pl.ds(pl.multiple_of(j * width, width), width)
            rates = [taps[layer, pl.ds(k, 1), at_c] for k in range(taps_count)]
            for i in range(q):
                conv = jnp.zeros((rows, width), jnp.float32)
                for k in range(taps_count):
                    first = 8 - (taps_count - 1) + k + i * rows
                    conv = conv + rates[k] * zpad[first:first + rows, :]
                at = pl.ds(i * rows, rows)
                gated[at, :] = (obuf[at, :].astype(jnp.float32) * conv).astype(jnp.bfloat16)


        def p_copy(layer, r, i):
            at = tile_at(flip(j, i))
            return remote(
                part.at[layer, lax.rem(c + r, tp), at, :], rec1.at[layer, r - 1, at, :],
                p_send.at[layer, r, i], p_recv.at[layer, r, i], at_tp(r),
            )

        def r_copy(layer, i, h):
            at = part_of(h)
            return remote(
                snd2.at[layer, i, at, :], rec2.at[layer, i, at, :],
                r_send.at[layer, i, h], r_recv.at[layer, i, h], at_sp(peer(i)),
            )

        def v_copy(layer, h):
            at = part_of(h)
            return remote(
                snd2.at[layer, 3, at, :], rec2.at[layer, 3, at, :],
                r_send.at[layer, 3, h], r_recv.at[layer, 3, h], at_sp(peer(1 + h)),
            )

        def reduce_tile(layer, i):
            at = tile_at(flip(j, i))
            total = part[layer, c, at, :].astype(jnp.float32)
            for r in range(1, tp):
                p_copy(layer, r, i).wait()
                total = total + rec1[layer, r - 1, at, :].astype(jnp.float32)
            if i == 0:
                acc[...] = total
                return
            snd2[layer, i] = total.astype(jnp.bfloat16)
            if i == 3:
                for h in range(2):
                    v_copy(layer, h).start()
            elif halves == 1:
                r_copy(layer, i, 0).start()
            elif i == 1:
                r_copy(layer, 1, 0).start()

        def relay(layer, h):
            if halves == 2:
                v_copy(layer, h).wait()
                i, at = 2 - h, part_of(h)
                snd2[layer, i, at, :] = (
                    snd2[layer, i, at, :].astype(jnp.float32) + rec2[layer, 3, at, :].astype(jnp.float32)
                ).astype(jnp.bfloat16)
                r_copy(layer, i, h).start()
                if h == 0:
                    r_copy(layer, 2, 1).start()

        def out_product(layer):
            for i in range(q - 1, -1, -1):
                at = tile_at(flip(j, i))

                def half(n, carry):
                    cc = lax.rem(c + 1 + n, tp)
                    weight = jnp.concatenate([wout[layer, cc * per_half + b] for b in range(per_half)], axis=1)
                    part[layer, cc, at, :] = jnp.dot(
                        gated[at, :], weight, preferred_element_type=jnp.float32
                    ).astype(jnp.bfloat16)
                    return carry

                lax.fori_loop(0, tp, half, 0)
                for r in range(1, tp):
                    p_copy(layer, r, i).start()
                if i < q - 1:
                    reduce_tile(layer, i + 1)
            reduce_tile(layer, 0)


        last = layers - 1

        def nth_block(n):
            upper = (l >= line // 2).astype(jnp.int32)
            inner = ((l > 0) & (l < line - 1)).astype(jnp.int32)
            b = n
            if n < 2:
                b = n + inner * (1 - 2 * n)
            return b + upper * (line - 1 - 2 * b)

        def cols_of(m):
            return pl.ds(pl.multiple_of(m * block_cols, block_cols), block_cols)

        def q_copy(n, i):
            b = nth_block(n)
            m = lax.rem(b, slots)
            at = tile_at(flip(j, i))
            return remote(
                part.at[last, lax.div(b, slots), at, cols_of(m)], rec1.at[last, 0, at, cols_of(m)],
                p_send.at[last, m, i], p_recv.at[last, m, i], at_tp(1),
            )

        def b_copy(m, i, h):
            at = part_of(h)
            return remote(
                snd2.at[last, i, at, cols_of(m)], rec2.at[last, i, at, cols_of(m)],
                b_send.at[m, i, h], b_recv.at[m, i, h], at_sp(peer(i if i < 3 else 1 + h)),
            )

        def block_product(n):
            b = nth_block(n)
            m = lax.rem(b, slots)
            own = lax.div(b, slots) == c
            weight = jnp.concatenate([wout[last, b * q + e] for e in range(q)], axis=1)
            for i in range(q - 1, -1, -1):
                at = tile_at(flip(j, i))
                part[last, lax.div(b, slots), at, cols_of(m)] = jnp.dot(
                    gated[at, :], weight, preferred_element_type=jnp.float32
                ).astype(jnp.bfloat16)

                @pl.when(jnp.logical_not(own))
                def _():
                    q_copy(n, i).start()

            @pl.when(own)
            def _():
                for i in range(q - 1, -1, -1):
                    at = tile_at(flip(j, i))
                    q_copy(n, i).wait_recv()
                    total = part[last, c, at, cols_of(m)].astype(jnp.float32)
                    total = total + rec1[last, 0, at, cols_of(m)].astype(jnp.float32)
                    if i == 0:
                        acc[:, cols_of(m)] = total
                        continue
                    snd2[last, i, :, cols_of(m)] = total.astype(jnp.bfloat16)
                    if i == 3:
                        b_copy(m, 3, 0).start()
                        b_copy(m, 3, 1).start()
                    else:
                        b_copy(m, i, i - 1).start()

        def block_relay(n):
            b = nth_block(n)
            m = lax.rem(b, slots)

            @pl.when(lax.div(b, slots) == c)
            def _():
                for h in range(2):
                    b_copy(m, 3, h).wait_recv()
                    i, at = 2 - h, part_of(h)
                    snd2[last, i, at, cols_of(m)] = (
                        snd2[last, i, at, cols_of(m)].astype(jnp.float32)
                        + rec2[last, 3, at, cols_of(m)].astype(jnp.float32)
                    ).astype(jnp.bfloat16)
                    b_copy(m, i, h).start()

        def block_sent():
            for n in range(line):
                b = nth_block(n)

                @pl.when(lax.div(b, slots) != c)
                def _():
                    for i in range(q):
                        q_copy(n, i).wait_send()

            for m in range(slots):
                for i in range(1, 4):
                    for h in range(2):
                        b_copy(m, i, h).wait_send()

        def s_copy(layer, r, h):
            return remote(
                stat.at[layer, h], stat_in.at[layer, r, h], s_send.at[layer, r, h], s_recv.at[layer, r, h], at_tp(r)
            )

        def finish(layer, h):
            at = part_of(h)
            pre = alpha * mine(layer, h)[...].astype(jnp.float32) + acc[at, :]
            for i in range(1, min(q, 3)):
                if timed and layer == last:
                    for m in range(slots):
                        b_copy(m, i, h).wait_recv()
                else:
                    r_copy(layer, i, h).wait()
                pre = pre + rec2[layer, i, at, :].astype(jnp.float32)
            acc[at, :] = pre
            own = jnp.sum(pre, axis=-1, keepdims=True)
            away = pre - own * (1.0 / feats)
            spread = jnp.sum(away * away, axis=-1, keepdims=True)
            lane = lax.broadcasted_iota(jnp.int32, (half_rows, LANES), 1)
            stat[layer, h] = jnp.where(lane == 0, own, spread)
            for r in range(1, tp):
                s_copy(layer, r, h).start()
            sums, spreads = [own], [spread]
            for r in range(1, tp):
                s_copy(layer, r, h).wait()
                sums.append(stat_in[layer, r, h, :, 0:1])
                spreads.append(stat_in[layer, r, h, :, 1:2])
            mean = sum(sums[1:], sums[0]) * (1.0 / model)
            var = sum(spreads[1:], spreads[0])
            for s in sums:
                off = s * (1.0 / feats) - mean
                var = var + feats * off * off
            scale = lax.rsqrt(var * (1.0 / model) + EPS)
            normed = (acc[at, :] - mean) * scale
            y = (normed * gain[pl.ds(layer, 1), :] + bias[pl.ds(layer, 1), :]).astype(jnp.bfloat16)
            if layer == last:
                res[at, :] = y
            else:
                mine(layer + 1, h)[...] = y


        tasks = []

        def at_time(when, fn, *args):
            tasks.append((when, len(tasks), fn, args))

        def first_half(layer, w0, w1, w2):
            def start():
                gather_wait(layer)
                arrived(layer * 4)
                project(layer, 0, put_u)

            def middle():
                arrived(layer * 4 + 1)
                project(layer, 1, put_z)
                halo_start(layer)

            def gates():
                arrived(layer * 4 + 2)
                project(layer, 2, put_o)
                halo_wait(layer)
                convolve(layer)

            at_time(w0, start)
            at_time(w1, middle)
            at_time(w2, gates)

        def second_half(layer, when):
            def go():
                arrived(layer * 4 + 3)
                out_product(layer)

            at_time(when, go)

        if timed:
            quick, slow, piece = 11.6, 17.4, 2.9
            for k in range(4):
                at_time(0.01 * k + (0.02 if k else 0.0), scatter_start, k)
            for h in range(halves):
                at_time(0.015, gather_start, 0, h)
                at_time(8.0 + 4.0 * h, gather_pass, 0, h)
                at_time(16.0 + 4.0 * h, gather_last, 0, h)
            for k in range(4, units):
                at_time(21.0 + piece * (k - 4), scatter_start, k)
            for k in range(units):
                for s in range(1, steps):
                    at_time(3.5 + quick * k + 6.0 * s, line_pass, k, s)
                at_time(3.0 + quick * k, line_begin, k)
            reach = [3.0 + slow * (k + 1) for k in range(units)]
            for layer in range(layers):
                base = reach[4 * layer]
                if layer:
                    base = max(base, reach[4 * layer - 1] + 37.0)
                w1 = max(base + 1.0, reach[4 * layer + 1])
                w2 = max(w1 + 1.0, reach[4 * layer + 2])
                first_half(layer, base, w1, w2)
                if layer < last:
                    o = max(w2 + 2.0, reach[4 * layer + 3])
                    second_half(layer, o)
                    at_time(o + 8.0, relay, layer, 0)
                    at_time(o + 9.0, relay, layer, 1)
                    for h in range(halves):
                        f = o + 14.0 + 6.0 * h
                        at_time(f, finish, layer, h)
                        at_time(f + 0.1, gather_start, layer + 1, h)
                        at_time(f + 9.0, gather_pass, layer + 1, h)
                        at_time(f + 15.0, gather_last, layer + 1, h)
                else:
                    k = 4 * layer + 3
                    for n in range(line):
                        o = max(w2 + 2.0, reach[k] - slow + n * 6.0)
                        if n:
                            at_time(o, line_end, k, n - 1)
                        at_time(o, block_product, n)
                        at_time(o + 5.0, block_relay, n)
                    for h in range(halves):
                        at_time(reach[k] + 30.0 + h, finish, layer, h)
                    at_time(reach[k] + 33.0, block_sent)
        else:
            for k in range(units):
                at_time(-2.0 if k < 2 else -1.0, scatter_start, k)
            for h in range(halves):
                at_time(-1.5, gather_start, 0, h)
            begin = [k + k // 4 for k in range(units)]
            for k in range(units):
                at_time(begin[k], line_begin, k)
                for s in range(1, steps):
                    at_time(begin[k] + s, line_pass, k, s)
            end = begin[-1] + max(steps, 1) + 1
            ready = [begin[k] + steps for k in range(units)]
            for layer in range(layers):
                if layer == 0:
                    base = ready[0] + 0.5
                else:
                    base = max(ready[4 * layer - 1] + 4.0, end if layer > 1 else 0) + 0.5
                for h in range(halves):
                    at_time(base - 1.3, gather_pass, layer, h)
                    at_time(base - 1.2, gather_last, layer, h)
                w1 = max(base + 0.1, ready[4 * layer + 1] + 0.5)
                w2 = max(w1 + 0.1, ready[4 * layer + 2] + 0.5)
                first_half(layer, base, w1, w2)
                o = max(w2 + 0.1, ready[4 * layer + 3] + 0.5)
                second_half(layer, o)
                for h in range(2):
                    at_time(o + 0.1, relay, layer, h)
                for h in range(halves):
                    at_time(o + 0.3, finish, layer, h)
                    if layer < last:
                        at_time(o + 0.4, gather_start, layer + 1, h)

        for _, _, fn, args in sorted(tasks, key=lambda task: task[:2]):
            fn(*args)
        for layer in range(layers):
            gather_sent(layer)
        for k in range(units):
            for s in range(steps):
                line_sent(k, s)

    return kernel


def solution(mesh):
    sp, tp = mesh.shape["sp"], mesh.shape["tp"]

    def shards(tokens, value_weight, outer_weight, inner_weight, conv_taps, output_weight, norm_gain, norm_bias):
        rows, feats = tokens.shape
        layers, depth, channels = value_weight.shape
        taps_count = conv_taps.shape[1]
        q = plane_size(sp, channels)
        width = channels // q
        line = sp // q
        model = feats * tp
        alpha = (2.0 * layers) ** 0.25
        out_cols = output_weight.shape[2]
        bf, f32 = jnp.bfloat16, jnp.float32
        kernel = make_kernel(sp, tp, q, layers, taps_count, rows, feats, depth, width, out_cols, alpha)
        dma = pltpu.SemaphoreType.DMA
        units, steps = 4 * layers, max(line - 1, 1)
        others = max(tp - 1, 1)
        halves = 2 if q == 4 else 1
        half_rows = rows // halves
        vm = pl.BlockSpec(memory_space=pltpu.VMEM)
        return pl.pallas_call(
            kernel,
            out_shape=jax.ShapeDtypeStruct((rows, feats), bf),
            in_specs=[vm] * 8,
            out_specs=vm,
            scratch_shapes=[
                pltpu.VMEM((layers, tp, q * rows, feats), bf),
                pltpu.VMEM((layers, 3, model, width), bf),
                pltpu.VMEM((layers, sp, width, out_cols), bf),
                pltpu.VMEM((q * rows, width), bf),
                pltpu.VMEM((q * rows, width), bf),
                pltpu.VMEM((q * rows + 8, width), f32),
                pltpu.VMEM((q * rows, width), bf),
                pltpu.VMEM((layers, tp, q * rows, feats), bf),
                pltpu.VMEM((layers, others, q * rows, feats), bf),
                pltpu.VMEM((layers, q, rows, feats), bf),
                pltpu.VMEM((layers, q, rows, feats), bf),
                pltpu.VMEM((rows, feats), f32),
                pltpu.VMEM((layers, halves, half_rows, LANES), f32),
                pltpu.VMEM((layers, tp, halves, half_rows, LANES), f32),
                pltpu.VMEM((layers, 2, 8, width), f32),
                dma((units, q)), dma((units, q)), dma((units,)),
                dma((units, steps)), dma((units, steps)), dma((units, steps)), dma((units, steps)),
                dma((layers, q, halves)), dma((layers, q, halves)), dma((halves,)),
                dma((layers, tp, q, halves)), dma((layers, tp, q, halves)),
                dma((layers, tp, q)), dma((layers, tp, q)),
                dma((layers, q, 2)), dma((layers, q, 2)),
                dma((layers, tp, halves)), dma((layers, tp, halves)),
                dma((layers,)), dma((layers,)),
                dma((2, 4, 2)), dma((2, 4, 2)),
            ],
            compiler_params=pltpu.CompilerParams(
                collective_id=0, has_side_effects=True, vmem_limit_bytes=60 * 1024 * 1024
            ),
        )(tokens, value_weight, outer_weight, inner_weight, conv_taps, output_weight, norm_gain, norm_bias)

    in_specs = (
        P("sp", "tp"),
        P(None, "sp", "tp"),
        P(None, "sp", "tp"),
        P(None, "sp", "tp"),
        P(None, None, "tp"),
        P(None, "tp", "sp"),
        P(None, "tp"),
        P(None, "tp"),
    )
    return jax.shard_map(shards, mesh=mesh, in_specs=in_specs, out_specs=P("sp", "tp"), check_vma=False)
```

```python
import jax
import jax.numpy as jnp
from jax import lax
from jax.experimental import pallas as pl
from jax.experimental.pallas import tpu as pltpu
from jax.sharding import PartitionSpec as P

LANES = 128
EPS = 1e-5


def flip(j, i):
    if i & 1:
        j = j + 1 - 2 * lax.rem(j, 2)
    if i & 2:
        j = j + 2 - 4 * lax.rem(lax.div(j, 2), 2)
    return j


def plane_size(sp, channels):
    q = 4
    while q > 1 and (sp % q or channels // q < LANES or channels % q):
        q //= 2
    return q


def helped(line, q, tp, layers):
    return line == 4 and q == 4 and tp == 2 and layers == 2


def make_kernel(sp, tp, q, layers, taps_count, rows, feats, depth, width, out_cols, alpha):
    line = sp // q
    units = layers * 4
    model = feats * tp
    per_half = sp // tp
    steps = line - 1
    halves = 2 if q == 4 else 1
    half_rows = rows // halves
    timed = helped(line, q, tp, layers)
    slots = line // tp if timed else 1
    block_cols = q * out_cols

    def kernel(
        tok, val, outw, inn, taps, prj, gain, bias, res,
        xg, win, wout, ubuf, obuf, zpad, gated, part, rec1, snd2, rec2, acc, stat, stat_in, halo,
        a_send, a_recv, a_loc, u_send, u_recv, d_send, d_recv,
        g_send, g_recv, g_loc, t_send, t_recv, p_send, p_recv, r_send, r_recv, s_send, s_recv, h_send, h_recv,
        b_send, b_recv, n_send, n_recv, k_send, k_recv,
    ):
        me = lax.axis_index("sp")
        c = lax.axis_index("tp")
        l = lax.div(me, q)
        j = lax.rem(me, q)

        def at_sp(other):
            return {"sp": other, "tp": c}

        def at_tp(r):
            return {"sp": me, "tp": lax.rem(c + r, tp)}

        def remote(src, dst, ssem, rsem, dev):
            return pltpu.make_async_remote_copy(
                src_ref=src, dst_ref=dst, send_sem=ssem, recv_sem=rsem,
                device_id=dev, device_id_type=pl.DeviceIdType.MESH,
            )

        def peer(i):
            return l * q + flip(j, i)

        barrier = pltpu.get_barrier_semaphore()

        def greet(dev):
            pl.semaphore_signal(barrier, inc=1, device_id=dev, device_id_type=pl.DeviceIdType.MESH)

        for i in range(1, q):
            greet(at_sp(peer(i)))
        for r in range(1, tp):
            greet(at_tp(r))

        @pl.when(l > 0)
        def _():
            greet(at_sp(me - q))

        @pl.when(l < line - 1)
        def _():
            greet(at_sp(me + q))

        neighbours = (l > 0).astype(jnp.int32) + (l < line - 1).astype(jnp.int32)
        pl.semaphore_wait(barrier, (q - 1) + (tp - 1) + neighbours)


        ORDER = (val, inn, outw, prj)

        def own_piece(k, jd):
            layer, w = divmod(k, 4)
            at = pl.ds(pl.multiple_of(jd * width, width), width)
            if w == 3:
                return prj.at[layer, at, :]
            return ORDER[w].at[layer, :, at]

        def landed(k, s):
            layer, w = divmod(k, 4)
            if w == 3:
                return wout.at[layer, s]
            return win.at[layer, w, pl.ds(pl.multiple_of(s * depth, depth), depth), :]

        def block(k, b):
            layer, w = divmod(k, 4)
            if w == 3:
                return wout.at[layer, pl.ds(b * q, q)]
            return win.at[layer, w, pl.ds(pl.multiple_of(b * (q * depth), q * depth), q * depth), :]

        def a_copy(k, i):
            return remote(own_piece(k, flip(j, i)), landed(k, me), a_send.at[k, i], a_recv.at[k, i], at_sp(peer(i)))

        def a_local(k):
            return pltpu.make_async_copy(own_piece(k, j), landed(k, me), a_loc.at[k])

        def scatter_start(k):
            a_local(k).start()
            for i in range(q - 1, 0, -1):
                a_copy(k, i).start()

        def scatter_wait(k):
            a_local(k).wait()
            for i in range(q - 1, 0, -1):
                a_copy(k, i).wait()

        def up(k, s):
            return remote(block(k, l - s), block(k, l - s), u_send.at[k, s], u_recv.at[k, s], at_sp(me + q))

        def down(k, s):
            return remote(block(k, l + s), block(k, l + s), d_send.at[k, s], d_recv.at[k, s], at_sp(me - q))

        def line_begin(k):
            scatter_wait(k)

            @pl.when(l < line - 1)
            def _():
                up(k, 0).start()

            @pl.when(l > 0)
            def _():
                down(k, 0).start()

        def line_pass(k, s):
            @pl.when((l - s >= 0) & (l < line - 1))
            def _():
                up(k, s - 1).wait_recv()
                up(k, s).start()

            @pl.when((l + s < line) & (l > 0))
            def _():
                down(k, s - 1).wait_recv()
                down(k, s).start()


        def lower_inner(fn):
            pl.when(l == 1)(fn)

        def upper_inner(fn):
            pl.when(l == 2)(fn)

        def outer(fn):
            pl.when((l == 0) | (l == 3))(fn)

        def inner(fn):
            pl.when((l == 1) | (l == 2))(fn)

        def outer_begin(k):
            @pl.when(l == 0)
            def _():
                scatter_wait(k)
                up(k, 0).start()

            @pl.when(l == 3)
            def _():
                scatter_wait(k)
                down(k, 0).start()

        def inner_ready(k):
            @inner
            def _():
                scatter_wait(k)

        def inward(k, s):
            @lower_inner
            def _():
                if s:
                    up(k, s - 1).wait_recv()
                up(k, s).start()

            @upper_inner
            def _():
                if s:
                    down(k, s - 1).wait_recv()
                down(k, s).start()

        def outward(k, s):
            @lower_inner
            def _():
                if s:
                    down(k, s - 1).wait_recv()
                down(k, s).start()

            @upper_inner
            def _():
                if s:
                    up(k, s - 1).wait_recv()
                up(k, s).start()

        def ends(k):
            return (1, line - 2) if timed and k < 3 else (0, line - 1)

        def line_end(k, s):
            low, high = ends(k)

            @pl.when((l == high) & (l - 1 - s >= 0))
            def _():
                up(k, s).wait_recv()

            @pl.when((l == low) & (l + 1 + s < line))
            def _():
                down(k, s).wait_recv()

        def arrived(k):
            for s in range(steps):
                line_end(k, s)

        def line_sent(k, s):
            low, high = ends(k)

            @pl.when((l - s >= 0) & (l < high))
            def _():
                up(k, s).wait_send()

            @pl.when((l + s < line) & (l > low))
            def _():
                down(k, s).wait_send()


        def part_of(h):
            return pl.ds(h * half_rows, half_rows)

        def spot(layer, jj, h):
            at = pl.ds(pl.multiple_of(jj * rows + h * half_rows, half_rows), half_rows)
            return xg.at[layer, c, at, :]

        def mine(layer, h):
            return tok.at[part_of(h)] if layer == 0 else spot(layer, j, h)

        def g_copy(layer, i, h):
            if i == 3:
                src = spot(layer, flip(j, 1 + h), h)
                return remote(src, src, g_send.at[layer, i, h], g_recv.at[layer, i, h], at_sp(peer(2 - h)))
            return remote(
                mine(layer, h), spot(layer, j, h), g_send.at[layer, i, h], g_recv.at[layer, i, h], at_sp(peer(i))
            )

        def g_local(h):
            return pltpu.make_async_copy(tok.at[part_of(h)], spot(0, j, h), g_loc.at[h])

        def t_copy(layer, r, i, h):
            src = mine(layer, h) if i == 0 else spot(layer, flip(j, i), h)
            return remote(
                src, spot(layer, flip(j, i), h), t_send.at[layer, r, i, h], t_recv.at[layer, r, i, h], at_tp(r)
            )

        def cross_start(layer, i, h):
            for r in range(1, tp):
                t_copy(layer, r, i, h).start()

        def gather_start(layer, h):
            if layer == 0:
                g_local(h).start()
            for i in range(1, min(q, 3)):
                g_copy(layer, i, h).start()
            cross_start(layer, 0, h)

        def gather_pass(layer, h):
            first = 1 + h if q == 4 else 1
            for i in range(1, min(q, 3)):
                i = first if i == 1 else 3 - first
                g_copy(layer, i, h).wait_recv()
                if q == 4 and i == first:
                    g_copy(layer, 3, h).start()
                cross_start(layer, i, h)

        def gather_last(layer, h):
            if q == 4:
                g_copy(layer, 3, h).wait_recv()
                cross_start(layer, 3, h)

        def gather_wait(layer, which):
            for h in range(halves):
                if layer == 0 and 0 in which:
                    g_local(h).wait()
                for i in which:
                    for r in range(1, tp):
                        t_copy(layer, r, i, h).wait_recv()

        def gather_sent(layer):
            for h in range(halves):
                for i in range(1, q):
                    g_copy(layer, i, h).wait_send()
                for i in range(q):
                    for r in range(1, tp):
                        t_copy(layer, r, i, h).wait_send()

        def tile_at(jj):
            return pl.ds(pl.multiple_of(jj * rows, rows), rows)


        far = layers
        ALL, MOST, REST = (0, q), (1, q - 1), (0, 1)

        def project(rows_set, layer, w, store, span):
            first = flip(j, q - 1) if span is not ALL else 0

            def tile(n, carry):
                i = lax.rem(first + span[0] + n, q)
                at = tile_at(i)
                total = jnp.zeros((rows, width), jnp.float32)
                for cc in range(tp):
                    total = total + jnp.dot(
                        xg[rows_set, cc, at, :],
                        win[layer, w, pl.ds(cc * feats, feats), :],
                        preferred_element_type=jnp.float32,
                    )
                store(i, total.astype(jnp.bfloat16))
                return carry

            lax.fori_loop(0, span[1], tile, 0)

        def put_u(bank):
            def put(i, v):
                ubuf[bank, tile_at(i), :] = v

            return put

        def put_o(bank):
            def put(i, v):
                obuf[bank, tile_at(i), :] = v

            return put

        def put_z(bank):
            def put(i, v):
                at = pl.ds(pl.multiple_of(8 + i * rows, 8), rows)
                zpad[bank, at, :] = v.astype(jnp.float32) * ubuf[bank, tile_at(i), :].astype(jnp.float32)

            return put

        def h_copy(layer):
            return remote(
                halo.at[layer, 0], halo.at[layer, 1], h_send.at[layer], h_recv.at[layer], at_sp(me + q)
            )

        def halo_start(layer):
            halo[layer, 0] = zpad[0, pl.ds(q * rows, 8), :]

            @pl.when(l < line - 1)
            def _():
                h_copy(layer).start()

        def halo_wait(layer):
            zpad[0, 0:8, :] = jnp.zeros((8, width), jnp.float32)

            @pl.when(l > 0)
            def _():
                h_copy(layer).wait_recv()
                zpad[0, 0:8, :] = halo[layer, 1]

            @pl.when(l < line - 1)
            def _():
                h_copy(layer).wait_send()

        def convolve(layer, bank):
            at_c = pl.ds(pl.multiple_of(j * width, width), width)
            rates = [taps[k, pl.ds(layer, 1), at_c] for k in range(taps_count)]
            for i in range(q):
                conv = jnp.zeros((rows, width), jnp.float32)
                for k in range(taps_count):
                    first = 8 - (taps_count - 1) + k + i * rows
                    conv = conv + rates[k] * zpad[bank, first:first + rows, :]
                at = pl.ds(i * rows, rows)
                gated[bank, at, :] = (obuf[bank, at, :].astype(jnp.float32) * conv).astype(jnp.bfloat16)


        def fellow():
            return at_sp(me + q * (1 - 2 * lax.rem(l, 2)))

        def n_copy(n):
            h = n % 2
            src = tok.at[part_of(h)] if n < 2 else spot(far, flip(j, 1 + h), h)
            return remote(
                src, spot(far, j if n < 2 else flip(j, 1 + h), h), n_send.at[n], n_recv.at[n], fellow()
            )

        def e_copy(h):
            return remote(
                tok.at[part_of(h)], spot(far, j, h), g_send.at[far, 1 + h, h], g_recv.at[far, 1 + h, h],
                at_sp(peer(1 + h)),
            )

        def k_copy(i):
            at = tile_at(flip(j, i))
            return remote(gated.at[1, at, :], gated.at[0, at, :], k_send.at[i], k_recv.at[i], fellow())

        def far_send():
            @outer
            def _():
                for h in range(2):
                    e_copy(h).start()
                for n in range(2):
                    n_copy(n).start()

        def far_pass():
            @outer
            def _():
                for h in range(2):
                    e_copy(h).wait_recv()
                    n_copy(2 + h).start()

        def far_in(h):
            @inner
            def _():
                n_copy(h).wait_recv()
                g_copy(far, 2 - h, h).start()
                cross_start(far, 0, h)

        def far_side():
            @inner
            def _():
                for h in range(2):
                    g_copy(far, 2 - h, h).wait_recv()
                    cross_start(far, 2 - h, h)

        def far_diag():
            @inner
            def _():
                for h in range(2):
                    n_copy(2 + h).wait_recv()
                    g_copy(far, 3, h).start()
                    cross_start(far, 1 + h, h)

        def inner_gather_start(h):
            @inner
            def _():
                gather_start(0, h)

        def inner_pass(rows_set, h):
            @inner
            def _():
                gather_pass(rows_set, h)

        def inner_last(rows_set, h):
            @inner
            def _():
                gather_last(rows_set, h)

        def inner_project(bank, ws, span):
            rows_set = far if bank else 0

            @inner
            def _():
                if ws[0] == 0:
                    gather_wait(rows_set, (3,) if span is REST else (0, 1, 2))
                for w in ws:
                    if bank == 0 and span is MOST:
                        arrived(w)
                    project(rows_set, 0, w, (put_u, put_z, put_o)[w](bank), span)
                if bank == 0 and span is REST:
                    @lower_inner
                    def _():
                        halo[0, 0] = zpad[0, pl.ds(q * rows, 8), :]
                        h_copy(0).start()

        def far_gates():
            tail = pl.ds(q * rows, 8)

            @lower_inner
            def _():
                zpad[1, 0:8, :] = jnp.zeros((8, width), jnp.float32)
                zpad[0, 0:8, :] = zpad[1, tail, :]

            @upper_inner
            def _():
                h_copy(0).wait_recv()
                zpad[0, 0:8, :] = halo[0, 1]
                zpad[1, 0:8, :] = zpad[0, tail, :]

            @inner
            def _():
                convolve(0, 1)
                k_copy(q - 1).start()

        def own_gates():
            @inner
            def _():
                convolve(0, 0)

        def far_rest():
            @inner
            def _():
                for i in range(q - 2, -1, -1):
                    k_copy(i).start()

        def far_sent():
            @outer
            def _():
                for h in range(2):
                    e_copy(h).wait_send()
                for n in range(4):
                    n_copy(n).wait_send()

            @inner
            def _():
                gather_sent(0)
                for h in range(2):
                    g_copy(far, 2 - h, h).wait_send()
                    g_copy(far, 3, h).wait_send()
                    for i in range(q):
                        for r in range(1, tp):
                            t_copy(far, r, i, h).wait_send()
                for i in range(q):
                    k_copy(i).wait_send()

            @lower_inner
            def _():
                h_copy(0).wait_send()


        def p_copy(layer, r, i):
            at = tile_at(flip(j, i))
            return remote(
                part.at[layer, lax.rem(c + r, tp), at, :], rec1.at[layer, r - 1, at, :],
                p_send.at[layer, r, i], p_recv.at[layer, r, i], at_tp(r),
            )

        def r_copy(layer, i, h):
            at = part_of(h)
            return remote(
                snd2.at[layer, i, at, :], rec2.at[layer, i, at, :],
                r_send.at[layer, i, h], r_recv.at[layer, i, h], at_sp(peer(i)),
            )

        def v_copy(layer, h):
            at = part_of(h)
            return remote(
                snd2.at[layer, 3, at, :], rec2.at[layer, 3, at, :],
                r_send.at[layer, 3, h], r_recv.at[layer, 3, h], at_sp(peer(1 + h)),
            )

        def reduce_tile(layer, i):
            at = tile_at(flip(j, i))
            total = part[layer, c, at, :].astype(jnp.float32)
            for r in range(1, tp):
                p_copy(layer, r, i).wait()
                total = total + rec1[layer, r - 1, at, :].astype(jnp.float32)
            if i == 0:
                acc[...] = total
                return
            snd2[layer, i] = total.astype(jnp.bfloat16)
            if i == 3:
                for h in range(2):
                    v_copy(layer, h).start()
            elif halves == 1:
                r_copy(layer, i, 0).start()
            elif i == 1:
                r_copy(layer, 1, 0).start()

        def relay(layer, h):
            if halves == 2:
                v_copy(layer, h).wait()
                i, at = 2 - h, part_of(h)
                snd2[layer, i, at, :] = (
                    snd2[layer, i, at, :].astype(jnp.float32) + rec2[layer, 3, at, :].astype(jnp.float32)
                ).astype(jnp.bfloat16)
                r_copy(layer, i, h).start()
                if h == 0:
                    r_copy(layer, 2, 1).start()

        def out_product(layer):
            for i in range(q - 1, -1, -1):
                at = tile_at(flip(j, i))
                if timed and layer == 0:
                    @outer
                    def _():
                        k_copy(i).wait_recv()

                def half(n, carry):
                    cc = lax.rem(c + 1 + n, tp)
                    weight = jnp.concatenate([wout[layer, cc * per_half + b] for b in range(per_half)], axis=1)
                    part[layer, cc, at, :] = jnp.dot(
                        gated[0, at, :], weight, preferred_element_type=jnp.float32
                    ).astype(jnp.bfloat16)
                    return carry

                lax.fori_loop(0, tp, half, 0)
                for r in range(1, tp):
                    p_copy(layer, r, i).start()
                if i < q - 1:
                    reduce_tile(layer, i + 1)
            reduce_tile(layer, 0)


        last = layers - 1

        def nth_block(n):
            upper = (l >= line // 2).astype(jnp.int32)
            inner = ((l > 0) & (l < line - 1)).astype(jnp.int32)
            b = n
            if n < 2:
                b = n + inner * (1 - 2 * n)
            return b + upper * (line - 1 - 2 * b)

        def cols_of(m):
            return pl.ds(pl.multiple_of(m * block_cols, block_cols), block_cols)

        def q_copy(n, i):
            b = nth_block(n)
            m = lax.rem(b, slots)
            at = tile_at(flip(j, i))
            return remote(
                part.at[last, lax.div(b, slots), at, cols_of(m)], rec1.at[last, 0, at, cols_of(m)],
                p_send.at[last, m, i], p_recv.at[last, m, i], at_tp(1),
            )

        def b_copy(m, i, h):
            at = part_of(h)
            return remote(
                snd2.at[last, i, at, cols_of(m)], rec2.at[last, i, at, cols_of(m)],
                b_send.at[m, i, h], b_recv.at[m, i, h], at_sp(peer(i if i < 3 else 1 + h)),
            )

        def block_product(n):
            b = nth_block(n)
            m = lax.rem(b, slots)
            own = lax.div(b, slots) == c
            weight = jnp.concatenate([wout[last, b * q + e] for e in range(q)], axis=1)
            for i in range(q - 1, -1, -1):
                at = tile_at(flip(j, i))
                part[last, lax.div(b, slots), at, cols_of(m)] = jnp.dot(
                    gated[0, at, :], weight, preferred_element_type=jnp.float32
                ).astype(jnp.bfloat16)

                @pl.when(jnp.logical_not(own))
                def _():
                    q_copy(n, i).start()

            @pl.when(own)
            def _():
                for i in range(q - 1, -1, -1):
                    at = tile_at(flip(j, i))
                    q_copy(n, i).wait_recv()
                    total = part[last, c, at, cols_of(m)].astype(jnp.float32)
                    total = total + rec1[last, 0, at, cols_of(m)].astype(jnp.float32)
                    if i == 0:
                        acc[:, cols_of(m)] = total
                        continue
                    snd2[last, i, :, cols_of(m)] = total.astype(jnp.bfloat16)
                    if i == 3:
                        b_copy(m, 3, 0).start()
                        b_copy(m, 3, 1).start()
                    else:
                        b_copy(m, i, i - 1).start()

        def block_relay(n):
            b = nth_block(n)
            m = lax.rem(b, slots)

            @pl.when(lax.div(b, slots) == c)
            def _():
                for h in range(2):
                    b_copy(m, 3, h).wait_recv()
                    i, at = 2 - h, part_of(h)
                    snd2[last, i, at, cols_of(m)] = (
                        snd2[last, i, at, cols_of(m)].astype(jnp.float32)
                        + rec2[last, 3, at, cols_of(m)].astype(jnp.float32)
                    ).astype(jnp.bfloat16)
                    b_copy(m, i, h).start()

        def block_sent():
            for n in range(line):
                b = nth_block(n)

                @pl.when(lax.div(b, slots) != c)
                def _():
                    for i in range(q):
                        q_copy(n, i).wait_send()

            for m in range(slots):
                for i in range(1, 4):
                    for h in range(2):
                        b_copy(m, i, h).wait_send()

        def s_copy(layer, r, h):
            return remote(
                stat.at[layer, h], stat_in.at[layer, r, h], s_send.at[layer, r, h], s_recv.at[layer, r, h], at_tp(r)
            )

        def finish(layer, h):
            at = part_of(h)
            pre = alpha * mine(layer, h)[...].astype(jnp.float32) + acc[at, :]
            for i in range(1, min(q, 3)):
                if timed and layer == last:
                    for m in range(slots):
                        b_copy(m, i, h).wait_recv()
                else:
                    r_copy(layer, i, h).wait()
                pre = pre + rec2[layer, i, at, :].astype(jnp.float32)
            acc[at, :] = pre
            own = jnp.sum(pre, axis=-1, keepdims=True)
            away = pre - own * (1.0 / feats)
            spread = jnp.sum(away * away, axis=-1, keepdims=True)
            lane = lax.broadcasted_iota(jnp.int32, (half_rows, LANES), 1)
            stat[layer, h] = jnp.where(lane == 0, own, spread)
            for r in range(1, tp):
                s_copy(layer, r, h).start()
            sums, spreads = [own], [spread]
            for r in range(1, tp):
                s_copy(layer, r, h).wait()
                sums.append(stat_in[layer, r, h, :, 0:1])
                spreads.append(stat_in[layer, r, h, :, 1:2])
            mean = sum(sums[1:], sums[0]) * (1.0 / model)
            var = sum(spreads[1:], spreads[0])
            for s in sums:
                off = s * (1.0 / feats) - mean
                var = var + feats * off * off
            scale = lax.rsqrt(var * (1.0 / model) + EPS)
            normed = (acc[at, :] - mean) * scale
            y = (normed * gain[pl.ds(layer, 1), :] + bias[pl.ds(layer, 1), :]).astype(jnp.bfloat16)
            if layer == last:
                res[at, :] = y
            else:
                mine(layer + 1, h)[...] = y


        tasks = []

        def at_time(when, fn, *args):
            tasks.append((when, len(tasks), fn, args))

        def first_half(layer, w0, w1, w2):
            def start():
                gather_wait(layer, range(q))
                arrived(layer * 4)
                project(layer, layer, 0, put_u(0), ALL)

            def middle():
                arrived(layer * 4 + 1)
                project(layer, layer, 1, put_z(0), ALL)
                halo_start(layer)

            def gates():
                arrived(layer * 4 + 2)
                project(layer, layer, 2, put_o(0), ALL)
                halo_wait(layer)
                convolve(layer, 0)

            at_time(w0, start)
            at_time(w1, middle)
            at_time(w2, gates)

        def most_of(layer):
            gather_wait(layer, (0, 1, 2))
            for w in range(3):
                arrived(layer * 4 + w)
                project(layer, layer, w, (put_u, put_z, put_o)[w](0), MOST)

        def rest_of(layer):
            gather_wait(layer, (3,))
            project(layer, layer, 0, put_u(0), REST)
            project(layer, layer, 1, put_z(0), REST)
            halo_start(layer)
            project(layer, layer, 2, put_o(0), REST)
            halo_wait(layer)
            convolve(layer, 0)

        def second_half(layer, when):
            def go():
                arrived(layer * 4 + 3)
                out_product(layer)

            at_time(when, go)

        if timed:
            at_time(-1.0, far_send)
            for when, k in ((0.0, 0), (0.1, 1), (0.2, 3), (0.3, 4), (0.5, 2), (0.6, 5), (27.0, 6), (44.2, 7)):
                at_time(when, scatter_start, k)
            for h in range(halves):
                at_time(0.4, inner_gather_start, h)
                at_time((8.6, 13.6)[h], far_in, h)
                at_time((20.0, 26.0)[h], inner_pass, 0, h)
                at_time(43.0 + 0.1 * h, inner_last, 0, h)
                at_time(51.0 + 0.1 * h, inner_last, far, h)
            at_time(15.1, far_pass)
            at_time(37.5, far_side)
            at_time(42.5, far_diag)
            for k, when in enumerate((3.5, 6.5, 15.0, 15.2, 15.3, 18.0, 30.0, 47.0)):
                at_time(when, outer_begin, k)
            for k, when in enumerate((3.5, 6.5, 27.5, 9.5, 12.5, 30.0, 44.5, 55.5)):
                at_time(when, inner_ready, k)
            for k, when in enumerate((3.6, 6.6, 27.6, 9.6, 49.0, 54.0, 66.0, 77.0)):
                at_time(when, inward, k, 0)
            for k, when in enumerate((19.0, 25.0, 31.0, 48.0, 54.1, 60.0, 71.0, 83.0)):
                at_time(when, inward, k, 1)
            for k, when in enumerate((9.7, 12.6, 30.1, 44.6, 55.6)):
                at_time(when, outward, k + 3, 0)
            for k, when in enumerate((23.5, 62.0, 73.0, 85.0, 97.0)):
                at_time(when, outward, k + 3, 1)
            for k, when in enumerate((54.2, 68.0, 79.0, 91.0, 103.0)):
                at_time(when, outward, k + 3, 2)
            at_time(33.2, inner_project, 0, (0,), MOST)
            at_time(37.0, inner_project, 0, (1,), MOST)
            at_time(44.7, inner_project, 0, (2,), MOST)
            at_time(44.9, inner_project, 0, (0, 1, 2), REST)
            at_time(45.5, inner_project, 1, (0, 1, 2), MOST)
            at_time(53.0, inner_project, 1, (0, 1, 2), REST)
            at_time(53.1, far_gates)
            at_time(53.2, own_gates)
            at_time(54.3, far_rest)
            o = 58.0
            second_half(0, o)
            at_time(o + 8.0, relay, 0, 0)
            at_time(o + 9.0, relay, 0, 1)
            for h in range(halves):
                f = o + 14.0 + 6.0 * h
                at_time(f, finish, 0, h)
                at_time(f + 0.1, gather_start, 1, h)
                at_time(f + 9.0, gather_pass, 1, h)
                at_time(f + 15.0, gather_last, 1, h)
            at_time(103.5, most_of, 1)
            at_time(106.0, rest_of, 1)
            for n in range(line):
                p = (110.0, 114.0, 119.0, 125.0)[n]
                if n:
                    at_time(p, line_end, 7, n - 1)
                at_time(p, block_product, n)
                at_time((126.0, 126.0, 126.5, 129.0)[n], block_relay, n)
            at_time(127.5, far_sent)
            at_time(128.0, gather_sent, 1)
            for k in range(units):
                for s in range(steps):
                    at_time(129.5, line_sent, k, s)
            for h in range(halves):
                at_time(130.0 + h, finish, last, h)
            at_time(140.0, block_sent)
        else:
            for k in range(units):
                at_time(-2.0 if k < 2 else -1.0, scatter_start, k)
            for h in range(halves):
                at_time(-1.5, gather_start, 0, h)
            begin = [k + k // 4 for k in range(units)]
            for k in range(units):
                at_time(begin[k], line_begin, k)
                for s in range(1, steps):
                    at_time(begin[k] + s, line_pass, k, s)
            end = begin[-1] + max(steps, 1) + 1
            ready = [begin[k] + steps for k in range(units)]
            for layer in range(layers):
                if layer == 0:
                    base = ready[0] + 0.5
                else:
                    base = max(ready[4 * layer - 1] + 4.0, end if layer > 1 else 0) + 0.5
                for h in range(halves):
                    at_time(base - 1.3, gather_pass, layer, h)
                    at_time(base - 1.2, gather_last, layer, h)
                w1 = max(base + 0.1, ready[4 * layer + 1] + 0.5)
                w2 = max(w1 + 0.1, ready[4 * layer + 2] + 0.5)
                first_half(layer, base, w1, w2)
                o = max(w2 + 0.1, ready[4 * layer + 3] + 0.5)
                second_half(layer, o)
                for h in range(2):
                    at_time(o + 0.1, relay, layer, h)
                for h in range(halves):
                    at_time(o + 0.3, finish, layer, h)
                    if layer < last:
                        at_time(o + 0.4, gather_start, layer + 1, h)

        for _, _, fn, args in sorted(tasks, key=lambda task: task[:2]):
            fn(*args)
        if not timed:
            for layer in range(layers):
                gather_sent(layer)
            for k in range(units):
                for s in range(steps):
                    line_sent(k, s)

    return kernel


def solution(mesh):
    sp, tp = mesh.shape["sp"], mesh.shape["tp"]

    def shards(tokens, value_weight, outer_weight, inner_weight, conv_taps, output_weight, norm_gain, norm_bias):
        rows, feats = tokens.shape
        layers, depth, channels = value_weight.shape
        taps_count = conv_taps.shape[1]
        q = plane_size(sp, channels)
        width = channels // q
        line = sp // q
        model = feats * tp
        alpha = (2.0 * layers) ** 0.25
        out_cols = output_weight.shape[2]
        bf, f32 = jnp.bfloat16, jnp.float32
        kernel = make_kernel(sp, tp, q, layers, taps_count, rows, feats, depth, width, out_cols, alpha)
        dma = pltpu.SemaphoreType.DMA
        units, steps = 4 * layers, max(line - 1, 1)
        others = max(tp - 1, 1)
        banks = 2 if helped(line, q, tp, layers) else 1
        sets = layers + banks - 1
        halves = 2 if q == 4 else 1
        half_rows = rows // halves
        vm = pl.BlockSpec(memory_space=pltpu.VMEM)
        return pl.pallas_call(
            kernel,
            out_shape=jax.ShapeDtypeStruct((rows, feats), bf),
            in_specs=[vm] * 8,
            out_specs=vm,
            scratch_shapes=[
                pltpu.VMEM((layers + banks - 1, tp, q * rows, feats), bf),
                pltpu.VMEM((layers, 3, model, width), bf),
                pltpu.VMEM((layers, sp, width, out_cols), bf),
                pltpu.VMEM((banks, q * rows, width), bf),
                pltpu.VMEM((banks, q * rows, width), bf),
                pltpu.VMEM((banks, q * rows + 8, width), f32),
                pltpu.VMEM((banks, q * rows, width), bf),
                pltpu.VMEM((layers, tp, q * rows, feats), bf),
                pltpu.VMEM((layers, others, q * rows, feats), bf),
                pltpu.VMEM((layers, q, rows, feats), bf),
                pltpu.VMEM((layers, q, rows, feats), bf),
                pltpu.VMEM((rows, feats), f32),
                pltpu.VMEM((layers, halves, half_rows, LANES), f32),
                pltpu.VMEM((layers, tp, halves, half_rows, LANES), f32),
                pltpu.VMEM((layers, 2, 8, width), f32),
                dma((units, q)), dma((units, q)), dma((units,)),
                dma((units, steps)), dma((units, steps)), dma((units, steps)), dma((units, steps)),
                dma((sets, q, halves)), dma((sets, q, halves)), dma((halves,)),
                dma((sets, tp, q, halves)), dma((sets, tp, q, halves)),
                dma((layers, tp, q)), dma((layers, tp, q)),
                dma((layers, q, 2)), dma((layers, q, 2)),
                dma((layers, tp, halves)), dma((layers, tp, halves)),
                dma((layers,)), dma((layers,)),
                dma((2, 4, 2)), dma((2, 4, 2)), dma((4,)), dma((4,)), dma((4,)), dma((4,)),
            ],
            compiler_params=pltpu.CompilerParams(
                collective_id=0, has_side_effects=True, vmem_limit_bytes=60 * 1024 * 1024
            ),
        )(tokens, value_weight, outer_weight, inner_weight, jnp.swapaxes(conv_taps, 0, 1), output_weight, norm_gain, norm_bias)

    in_specs = (
        P("sp", "tp"),
        P(None, "sp", "tp"),
        P(None, "sp", "tp"),
        P(None, "sp", "tp"),
        P(None, None, "tp"),
        P(None, "tp", "sp"),
        P(None, "tp"),
        P(None, "tp"),
    )
    return jax.shard_map(shards, mesh=mesh, in_specs=in_specs, out_specs=P("sp", "tp"), check_vma=False)
```

```python
import jax
import jax.numpy as jnp
from jax import lax
from jax.experimental import pallas as pl
from jax.experimental.pallas import tpu as pltpu
from jax.sharding import PartitionSpec as P

LANES = 128
EPS = 1e-5


def flip(j, i):
    if i & 1:
        j = j + 1 - 2 * lax.rem(j, 2)
    if i & 2:
        j = j + 2 - 4 * lax.rem(lax.div(j, 2), 2)
    return j


def plane_size(sp, channels):
    q = 4
    while q > 1 and (sp % q or channels // q < LANES or channels % q):
        q //= 2
    return q


def helped(line, q, tp, layers):
    return line == 4 and q == 4 and tp == 2 and layers == 2


def make_kernel(sp, tp, q, layers, taps_count, rows, feats, depth, width, out_cols, alpha):
    line = sp // q
    units = layers * 4
    model = feats * tp
    per_half = sp // tp
    steps = line - 1
    halves = 2 if q == 4 else 1
    half_rows = rows // halves
    timed = helped(line, q, tp, layers)
    slots = line // tp if timed else 1
    block_cols = q * out_cols

    def kernel(
        tok, val, outw, inn, taps, prj, gain, bias, res,
        xg, win, wout, ubuf, obuf, zpad, gated, part, rec1, snd2, rec2, acc, stat, stat_in, halo,
        a_send, a_recv, a_loc, u_send, u_recv, d_send, d_recv,
        g_send, g_recv, g_loc, t_send, t_recv, p_send, p_recv, r_send, r_recv, s_send, s_recv, h_send, h_recv,
        b_send, b_recv, n_send, n_recv, k_send, k_recv,
        v_send, v_recv, w_send, w_recv,
    ):
        me = lax.axis_index("sp")
        c = lax.axis_index("tp")
        l = lax.div(me, q)
        j = lax.rem(me, q)

        def at_sp(other):
            return {"sp": other, "tp": c}

        def at_tp(r):
            return {"sp": me, "tp": lax.rem(c + r, tp)}

        def remote(src, dst, ssem, rsem, dev):
            return pltpu.make_async_remote_copy(
                src_ref=src, dst_ref=dst, send_sem=ssem, recv_sem=rsem,
                device_id=dev, device_id_type=pl.DeviceIdType.MESH,
            )

        def peer(i):
            return l * q + flip(j, i)

        barrier = pltpu.get_barrier_semaphore()

        def greet(dev):
            pl.semaphore_signal(barrier, inc=1, device_id=dev, device_id_type=pl.DeviceIdType.MESH)

        for i in range(1, q):
            greet(at_sp(peer(i)))
        for r in range(1, tp):
            greet(at_tp(r))

        @pl.when(l > 0)
        def _():
            greet(at_sp(me - q))

        @pl.when(l < line - 1)
        def _():
            greet(at_sp(me + q))

        neighbours = (l > 0).astype(jnp.int32) + (l < line - 1).astype(jnp.int32)
        pl.semaphore_wait(barrier, (q - 1) + (tp - 1) + neighbours)


        ORDER = (val, inn, outw, prj)

        def own_piece(k, jd):
            layer, w = divmod(k, 4)
            at = pl.ds(pl.multiple_of(jd * width, width), width)
            if w == 3:
                return prj.at[layer, at, :]
            return ORDER[w].at[layer, :, at]

        def landed(k, s):
            layer, w = divmod(k, 4)
            if w == 3:
                return wout.at[layer, s]
            return win.at[layer, w, pl.ds(pl.multiple_of(s * depth, depth), depth), :]

        def block(k, b):
            layer, w = divmod(k, 4)
            if w == 3:
                return wout.at[layer, pl.ds(b * q, q)]
            return win.at[layer, w, pl.ds(pl.multiple_of(b * (q * depth), q * depth), q * depth), :]

        def a_copy(k, i):
            return remote(own_piece(k, flip(j, i)), landed(k, me), a_send.at[k, i], a_recv.at[k, i], at_sp(peer(i)))

        def a_local(k):
            return pltpu.make_async_copy(own_piece(k, j), landed(k, me), a_loc.at[k])

        def scatter_start(k):
            a_local(k).start()
            for i in range(q - 1, 0, -1):
                a_copy(k, i).start()

        def scatter_wait(k):
            a_local(k).wait()
            for i in range(q - 1, 0, -1):
                a_copy(k, i).wait()

        def up(k, s):
            return remote(block(k, l - s), block(k, l - s), u_send.at[k, s], u_recv.at[k, s], at_sp(me + q))

        def down(k, s):
            return remote(block(k, l + s), block(k, l + s), d_send.at[k, s], d_recv.at[k, s], at_sp(me - q))

        def line_begin(k):
            scatter_wait(k)

            @pl.when(l < line - 1)
            def _():
                up(k, 0).start()

            @pl.when(l > 0)
            def _():
                down(k, 0).start()

        def line_pass(k, s):
            @pl.when((l - s >= 0) & (l < line - 1))
            def _():
                up(k, s - 1).wait_recv()
                up(k, s).start()

            @pl.when((l + s < line) & (l > 0))
            def _():
                down(k, s - 1).wait_recv()
                down(k, s).start()


        def lower_inner(fn):
            pl.when(l == 1)(fn)

        def upper_inner(fn):
            pl.when(l == 2)(fn)

        def outer(fn):
            pl.when((l == 0) | (l == 3))(fn)

        def inner(fn):
            pl.when((l == 1) | (l == 2))(fn)

        def outer_begin(k):
            @pl.when(l == 0)
            def _():
                scatter_wait(k)
                up(k, 0).start()

            @pl.when(l == 3)
            def _():
                scatter_wait(k)
                down(k, 0).start()

        def inner_ready(k):
            @inner
            def _():
                scatter_wait(k)

        def inward(k, s):
            @lower_inner
            def _():
                if s:
                    up(k, s - 1).wait_recv()
                up(k, s).start()

            @upper_inner
            def _():
                if s:
                    down(k, s - 1).wait_recv()
                down(k, s).start()

        def outward(k, s):
            @lower_inner
            def _():
                if s:
                    down(k, s - 1).wait_recv()
                down(k, s).start()

            @upper_inner
            def _():
                if s:
                    up(k, s - 1).wait_recv()
                up(k, s).start()

        def ends(k):
            return (1, line - 2) if timed and k < 3 else (0, line - 1)

        def line_end(k, s):
            low, high = ends(k)

            @pl.when((l == high) & (l - 1 - s >= 0))
            def _():
                up(k, s).wait_recv()

            @pl.when((l == low) & (l + 1 + s < line))
            def _():
                down(k, s).wait_recv()

        def arrived(k):
            for s in range(steps):
                line_end(k, s)

        def line_sent(k, s):
            low, high = ends(k)

            @pl.when((l - s >= 0) & (l < high))
            def _():
                up(k, s).wait_send()

            @pl.when((l + s < line) & (l > low))
            def _():
                down(k, s).wait_send()


        def part_of(h):
            return pl.ds(h * half_rows, half_rows)

        def spot(layer, jj, h):
            at = pl.ds(pl.multiple_of(jj * rows + h * half_rows, half_rows), half_rows)
            return xg.at[layer, c, at, :]

        def mine(layer, h):
            return tok.at[part_of(h)] if layer == 0 else spot(layer, j, h)

        def g_copy(layer, i, h):
            if i == 3:
                src = spot(layer, flip(j, 1 + h), h)
                return remote(src, src, g_send.at[layer, i, h], g_recv.at[layer, i, h], at_sp(peer(2 - h)))
            return remote(
                mine(layer, h), spot(layer, j, h), g_send.at[layer, i, h], g_recv.at[layer, i, h], at_sp(peer(i))
            )

        def g_local(h):
            return pltpu.make_async_copy(tok.at[part_of(h)], spot(0, j, h), g_loc.at[h])

        def t_copy(layer, r, i, h):
            src = mine(layer, h) if i == 0 else spot(layer, flip(j, i), h)
            return remote(
                src, spot(layer, flip(j, i), h), t_send.at[layer, r, i, h], t_recv.at[layer, r, i, h], at_tp(r)
            )

        def cross_start(layer, i, h):
            for r in range(1, tp):
                t_copy(layer, r, i, h).start()

        def gather_start(layer, h):
            if layer == 0:
                g_local(h).start()
            for i in range(1, min(q, 3)):
                g_copy(layer, i, h).start()
            cross_start(layer, 0, h)

        def gather_pass(layer, h, onward=True):
            first = 1 + h if q == 4 else 1
            for i in range(1, min(q, 3)):
                i = first if i == 1 else 3 - first
                g_copy(layer, i, h).wait_recv()
                if q == 4 and i == first and onward:
                    g_copy(layer, 3, h).start()
                cross_start(layer, i, h)

        def gather_last(layer, h):
            if q == 4:
                g_copy(layer, 3, h).wait_recv()
                cross_start(layer, 3, h)

        def gather_wait(layer, which):
            for h in range(halves):
                if layer == 0 and 0 in which:
                    g_local(h).wait()
                for i in which:
                    for r in range(1, tp):
                        t_copy(layer, r, i, h).wait_recv()

        def gather_sent(layer):
            for h in range(halves):
                for i in range(1, q):
                    g_copy(layer, i, h).wait_send()
                for i in range(q):
                    for r in range(1, tp):
                        t_copy(layer, r, i, h).wait_send()

        def tile_at(jj):
            return pl.ds(pl.multiple_of(jj * rows, rows), rows)


        far = layers
        ALL, MOST, REST = (0, q), (1, q - 1), (0, 1)

        def project(rows_set, layer, w, store, span):
            first = flip(j, q - 1) if span is not ALL else 0

            def tile(n, carry):
                i = lax.rem(first + span[0] + n, q)
                at = tile_at(i)
                total = jnp.zeros((rows, width), jnp.float32)
                for cc in range(tp):
                    total = total + jnp.dot(
                        xg[rows_set, cc, at, :],
                        win[layer, w, pl.ds(cc * feats, feats), :],
                        preferred_element_type=jnp.float32,
                    )
                store(i, total.astype(jnp.bfloat16))
                return carry

            lax.fori_loop(0, span[1], tile, 0)

        def put_u(bank):
            def put(i, v):
                ubuf[bank, tile_at(i), :] = v

            return put

        def put_o(bank):
            def put(i, v):
                obuf[bank, tile_at(i), :] = v

            return put

        def put_z(bank):
            def put(i, v):
                at = pl.ds(pl.multiple_of(8 + i * rows, 8), rows)
                zpad[bank, at, :] = v.astype(jnp.float32) * ubuf[bank, tile_at(i), :].astype(jnp.float32)

            return put

        def h_copy(layer):
            return remote(
                halo.at[layer, 0], halo.at[layer, 1], h_send.at[layer], h_recv.at[layer], at_sp(me + q)
            )

        def halo_start(layer):
            halo[layer, 0] = zpad[0, pl.ds(q * rows, 8), :]

            @pl.when(l < line - 1)
            def _():
                h_copy(layer).start()

        def halo_wait(layer):
            zpad[0, 0:8, :] = jnp.zeros((8, width), jnp.float32)

            @pl.when(l > 0)
            def _():
                h_copy(layer).wait_recv()
                zpad[0, 0:8, :] = halo[layer, 1]

        def convolve(layer, bank, tiles):
            at_c = pl.ds(pl.multiple_of(j * width, width), width)
            rates = [taps[k, pl.ds(layer, 1), at_c] for k in range(taps_count)]
            for i in tiles:
                conv = jnp.zeros((rows, width), jnp.float32)
                for k in range(taps_count):
                    first = 8 - (taps_count - 1) + k + i * rows
                    conv = conv + rates[k] * zpad[bank, first:first + rows, :]
                at = pl.ds(i * rows, rows)
                gated[bank, at, :] = (obuf[bank, at, :].astype(jnp.float32) * conv).astype(jnp.bfloat16)


        def fellow():
            return at_sp(me + q * (1 - 2 * lax.rem(l, 2)))

        def n_copy(n):
            h = n % 2
            src = tok.at[part_of(h)] if n < 2 else spot(far, flip(j, 1 + h), h)
            return remote(
                src, spot(far, j if n < 2 else flip(j, 1 + h), h), n_send.at[n], n_recv.at[n], fellow()
            )

        def e_copy(h):
            return remote(
                tok.at[part_of(h)], spot(far, j, h), g_send.at[far, 1 + h, h], g_recv.at[far, 1 + h, h],
                at_sp(peer(1 + h)),
            )

        def k_copy(i):
            at = tile_at(flip(j, i))
            return remote(gated.at[1, at, :], gated.at[0, at, :], k_send.at[i], k_recv.at[i], fellow())

        def far_send():
            @outer
            def _():
                for h in range(2):
                    e_copy(h).start()
                for n in range(2):
                    n_copy(n).start()

        def far_pass():
            @outer
            def _():
                for h in range(2):
                    e_copy(h).wait_recv()
                    n_copy(2 + h).start()

        def far_in(h):
            @inner
            def _():
                n_copy(h).wait_recv()
                g_copy(far, 2 - h, h).start()
                cross_start(far, 0, h)

        def far_side():
            @inner
            def _():
                for h in range(2):
                    g_copy(far, 2 - h, h).wait_recv()
                    cross_start(far, 2 - h, h)

        def far_diag():
            @inner
            def _():
                for h in range(2):
                    n_copy(2 + h).wait_recv()
                    g_copy(far, 3, h).start()
                    cross_start(far, 1 + h, h)

        def inner_gather_start(h):
            @inner
            def _():
                gather_start(0, h)

        def inner_pass(rows_set, h):
            @inner
            def _():
                gather_pass(rows_set, h, False)

        def inner_onward(rows_set, h):
            @inner
            def _():
                g_copy(rows_set, 3, h).start()

        def inner_last(rows_set, h):
            @inner
            def _():
                gather_last(rows_set, h)

        def inner_wait(rows_set, which):
            @inner
            def _():
                gather_wait(rows_set, which)

        def inner_project(bank, ws, span):
            @inner
            def _():
                for w in ws:
                    project(far if bank else 0, 0, w, (put_u, put_z, put_o)[w](bank), span)

        def inner_arrived(k):
            @inner
            def _():
                arrived(k)

        def own_edge():
            @lower_inner
            def _():
                halo[0, 0] = zpad[0, pl.ds(q * rows, 8), :]
                h_copy(0).start()

        tail = pl.ds(q * rows, 8)

        def far_gates():
            @pl.when((l == 1) | ((l == 2) & (j == 0)))
            def _():
                zpad[1, 0:8, :] = jnp.zeros((8, width), jnp.float32)

            @pl.when((l == 2) & (j > 0))
            def _():
                zpad[1, 0:8, :] = zpad[0, tail, :]

            @inner
            def _():
                convolve(0, 1, range(q))
                k_copy(q - 1).start()

        def far_first():
            @pl.when((l == 2) & (j == 0))
            def _():
                zpad[1, 0:8, :] = zpad[0, tail, :]
                convolve(0, 1, range(1))

        def own_gates():
            @lower_inner
            def _():
                zpad[0, 0:8, :] = zpad[1, tail, :]

            @upper_inner
            def _():
                h_copy(0).wait_recv()
                zpad[0, 0:8, :] = halo[0, 1]

            @inner
            def _():
                convolve(0, 0, range(q))

        def far_rest(*which):
            @inner
            def _():
                for i in which:
                    k_copy(i).start()

        def parts_sent():
            for i in range(q):
                p_copy(0, 1, i).wait_send()

        def far_sent():
            @outer
            def _():
                for h in range(2):
                    e_copy(h).wait_send()
                for n in range(4):
                    n_copy(n).wait_send()

            @inner
            def _():
                gather_sent(0)
                for h in range(2):
                    g_copy(far, 2 - h, h).wait_send()
                    g_copy(far, 3, h).wait_send()
                    for i in range(q):
                        for r in range(1, tp):
                            t_copy(far, r, i, h).wait_send()
                for i in range(q):
                    k_copy(i).wait_send()

            @lower_inner
            def _():
                h_copy(0).wait_send()


        def p_copy(layer, r, i):
            at = tile_at(flip(j, i))
            return remote(
                part.at[layer, lax.rem(c + r, tp), at, :], rec1.at[layer, r - 1, at, :],
                p_send.at[layer, r, i], p_recv.at[layer, r, i], at_tp(r),
            )


        bit_rows = half_rows // 2

        def bit_of(h, e):
            return pl.ds(h * half_rows + e * bit_rows, bit_rows)

        def r_copy(layer, i, h):
            at = part_of(h)
            return remote(
                snd2.at[layer, i, at, :], rec2.at[layer, i, at, :],
                r_send.at[layer, i, h], r_recv.at[layer, i, h], at_sp(peer(i)),
            )

        def w_copy(layer, h, e):
            at = bit_of(h, e)
            return remote(
                snd2.at[layer, 2 - h, at, :], rec2.at[layer, 2 - h, at, :],
                w_send.at[layer, h, e], w_recv.at[layer, h, e], at_sp(peer(2 - h)),
            )

        def v_copy(layer, h, e):
            at = bit_of(h, e)
            return remote(
                snd2.at[layer, 3, at, :], rec2.at[layer, 3, at, :],
                v_send.at[layer, h, e], v_recv.at[layer, h, e], at_sp(peer(1 + h)),
            )

        def reduce_tile(layer, i):
            at = tile_at(flip(j, i))
            total = part[layer, c, at, :].astype(jnp.float32)
            for r in range(1, tp):
                if timed:
                    p_copy(layer, r, i).wait_recv()
                else:
                    p_copy(layer, r, i).wait()
                total = total + rec1[layer, r - 1, at, :].astype(jnp.float32)
            if i == 0:
                acc[...] = total
                return
            snd2[layer, i] = total.astype(jnp.bfloat16)
            if i == 3:
                for e in range(2):
                    for h in range(2):
                        v_copy(layer, h, e).start()
            elif halves == 1:
                r_copy(layer, i, 0).start()
            elif i == 1:
                r_copy(layer, 1, 0).start()

        def relay(layer, h, e):
            if halves == 2:
                v_copy(layer, h, e).wait()
                i, at = 2 - h, bit_of(h, e)
                snd2[layer, i, at, :] = (
                    snd2[layer, i, at, :].astype(jnp.float32) + rec2[layer, 3, at, :].astype(jnp.float32)
                ).astype(jnp.bfloat16)
                w_copy(layer, h, e).start()
                if h == 0 and e == 1:
                    r_copy(layer, 2, 1).start()

        def out_product(layer):
            for i in range(q - 1, -1, -1):
                at = tile_at(flip(j, i))

                def half(n, carry):
                    cc = lax.rem(c + 1 + n, tp)
                    weight = jnp.concatenate([wout[layer, cc * per_half + b] for b in range(per_half)], axis=1)
                    part[layer, cc, at, :] = jnp.dot(
                        gated[0, at, :], weight, preferred_element_type=jnp.float32
                    ).astype(jnp.bfloat16)
                    return carry

                lax.fori_loop(0, tp, half, 0)
                for r in range(1, tp):
                    p_copy(layer, r, i).start()
                if i < q - 1:
                    reduce_tile(layer, i + 1)
            reduce_tile(layer, 0)


        def late_half():
            return (l < line // 2).astype(jnp.int32)

        def half_product(second):
            cc = late_half() if second else 1 - late_half()
            weight = jnp.concatenate([wout[0, cc * per_half + b] for b in range(per_half)], axis=1)
            for i in range(q - 1, -1, -1):
                at = tile_at(flip(j, i))
                if not second:
                    @outer
                    def _():
                        k_copy(i).wait_recv()

                part[0, cc, at, :] = jnp.dot(
                    gated[0, at, :], weight, preferred_element_type=jnp.float32
                ).astype(jnp.bfloat16)

                @pl.when(cc != c)
                def _():
                    p_copy(0, 1, i).start()

                if i < q - 1:
                    @pl.when(cc == c)
                    def _():
                        reduce_tile(0, i + 1)

            @pl.when(cc == c)
            def _():
                reduce_tile(0, 0)

        def half_relay(second, h, e):
            @pl.when((late_half() == c) if second else (late_half() != c))
            def _():
                relay(0, h, e)


        last = layers - 1

        def nth_block(n):
            upper = (l >= line // 2).astype(jnp.int32)
            inner = ((l > 0) & (l < line - 1)).astype(jnp.int32)
            b = n
            if n < 2:
                b = n + inner * (1 - 2 * n)
            return b + upper * (line - 1 - 2 * b)

        def cols_of(m):
            return pl.ds(pl.multiple_of(m * block_cols, block_cols), block_cols)

        def q_copy(n, i):
            b = nth_block(n)
            m = lax.rem(b, slots)
            at = tile_at(flip(j, i))
            return remote(
                part.at[last, lax.div(b, slots), at, cols_of(m)], rec1.at[last, 0, at, cols_of(m)],
                p_send.at[last, m, i], p_recv.at[last, m, i], at_tp(1),
            )

        def b_copy(m, i, h):
            at = part_of(h)
            return remote(
                snd2.at[last, i, at, cols_of(m)], rec2.at[last, i, at, cols_of(m)],
                b_send.at[m, i, h], b_recv.at[m, i, h], at_sp(peer(i if i < 3 else 1 + h)),
            )

        def block_product(n):
            b = nth_block(n)
            m = lax.rem(b, slots)
            own = lax.div(b, slots) == c
            weight = jnp.concatenate([wout[last, b * q + e] for e in range(q)], axis=1)
            for i in range(q - 1, -1, -1):
                at = tile_at(flip(j, i))
                part[last, lax.div(b, slots), at, cols_of(m)] = jnp.dot(
                    gated[0, at, :], weight, preferred_element_type=jnp.float32
                ).astype(jnp.bfloat16)

                @pl.when(jnp.logical_not(own))
                def _():
                    q_copy(n, i).start()

            @pl.when(own)
            def _():
                for i in range(q - 1, -1, -1):
                    at = tile_at(flip(j, i))
                    q_copy(n, i).wait_recv()
                    total = part[last, c, at, cols_of(m)].astype(jnp.float32)
                    total = total + rec1[last, 0, at, cols_of(m)].astype(jnp.float32)
                    if i == 0:
                        acc[:, cols_of(m)] = total
                        continue
                    snd2[last, i, :, cols_of(m)] = total.astype(jnp.bfloat16)
                    if i == 3:
                        b_copy(m, 3, 0).start()
                        b_copy(m, 3, 1).start()
                    elif i == 1:
                        b_copy(m, 1, 0).start()

        def block_relay(n):
            b = nth_block(n)
            m = lax.rem(b, slots)

            @pl.when(lax.div(b, slots) == c)
            def _():
                for h in range(2):
                    b_copy(m, 3, h).wait_recv()
                    i, at = 2 - h, part_of(h)
                    snd2[last, i, at, cols_of(m)] = (
                        snd2[last, i, at, cols_of(m)].astype(jnp.float32)
                        + rec2[last, 3, at, cols_of(m)].astype(jnp.float32)
                    ).astype(jnp.bfloat16)
                    b_copy(m, i, h).start()
                    if h == 0:
                        b_copy(m, 2, 1).start()

        def block_sent():
            for n in range(line):
                b = nth_block(n)

                @pl.when(lax.div(b, slots) != c)
                def _():
                    for i in range(q):
                        q_copy(n, i).wait_send()

            for m in range(slots):
                for i in range(1, 4):
                    for h in range(2):
                        b_copy(m, i, h).wait_send()

        def s_copy(layer, r, h):
            return remote(
                stat.at[layer, h], stat_in.at[layer, r, h], s_send.at[layer, r, h], s_recv.at[layer, r, h], at_tp(r)
            )

        def finish(layer, h):
            at = part_of(h)
            pre = alpha * mine(layer, h)[...].astype(jnp.float32) + acc[at, :]
            for i in range(1, min(q, 3)):
                if timed and layer == last:
                    for m in range(slots):
                        b_copy(m, i, h).wait_recv()
                elif halves == 2 and i == 2 - h:
                    for e in range(2):
                        w_copy(layer, h, e).wait()
                else:
                    r_copy(layer, i, h).wait()
                pre = pre + rec2[layer, i, at, :].astype(jnp.float32)
            acc[at, :] = pre
            own = jnp.sum(pre, axis=-1, keepdims=True)
            away = pre - own * (1.0 / feats)
            spread = jnp.sum(away * away, axis=-1, keepdims=True)
            lane = lax.broadcasted_iota(jnp.int32, (half_rows, LANES), 1)
            stat[layer, h] = jnp.where(lane == 0, own, spread)
            for r in range(1, tp):
                s_copy(layer, r, h).start()
            sums, spreads = [own], [spread]
            for r in range(1, tp):
                s_copy(layer, r, h).wait()
                sums.append(stat_in[layer, r, h, :, 0:1])
                spreads.append(stat_in[layer, r, h, :, 1:2])
            mean = sum(sums[1:], sums[0]) * (1.0 / model)
            var = sum(spreads[1:], spreads[0])
            for s in sums:
                off = s * (1.0 / feats) - mean
                var = var + feats * off * off
            scale = lax.rsqrt(var * (1.0 / model) + EPS)
            normed = (acc[at, :] - mean) * scale
            y = (normed * gain[pl.ds(layer, 1), :] + bias[pl.ds(layer, 1), :]).astype(jnp.bfloat16)
            if layer == last:
                res[at, :] = y
            else:
                mine(layer + 1, h)[...] = y


        tasks = []

        def at_time(when, fn, *args):
            tasks.append((when, len(tasks), fn, args))

        def first_half(layer, w0, w1, w2):
            def start():
                gather_wait(layer, range(q))
                arrived(layer * 4)
                project(layer, layer, 0, put_u(0), ALL)

            def middle():
                arrived(layer * 4 + 1)
                project(layer, layer, 1, put_z(0), ALL)
                halo_start(layer)

            def gates():
                arrived(layer * 4 + 2)
                project(layer, layer, 2, put_o(0), ALL)
                halo_wait(layer)
                convolve(layer, 0, range(q))
                halo_sent(layer)

            at_time(w0, start)
            at_time(w1, middle)
            at_time(w2, gates)

        def most_of(layer, ws):
            for w in ws:
                arrived(layer * 4 + w)
                project(layer, layer, w, (put_u, put_z, put_o)[w](0), MOST)

        def rest_of(layer):
            gather_wait(layer, (3,))
            project(layer, layer, 0, put_u(0), REST)
            project(layer, layer, 1, put_z(0), REST)
            halo_start(layer)

        def gates_of(layer):
            project(layer, layer, 2, put_o(0), REST)
            halo_wait(layer)
            convolve(layer, 0, range(q))

        def halo_sent(layer):
            @pl.when(l < line - 1)
            def _():
                h_copy(layer).wait_send()

        def second_half(layer, when):
            def go():
                arrived(layer * 4 + 3)
                out_product(layer)

            at_time(when, go)

        if timed:
            at_time(-1.0, far_send)
            for when, k in ((0.0, 0), (0.1, 1), (0.2, 3), (0.3, 4), (0.5, 2), (0.6, 5), (13.7, 6), (13.8, 7)):
                at_time(when, scatter_start, k)
            for h in range(halves):
                at_time(0.4, inner_gather_start, h)
                at_time((8.6, 13.6)[h], far_in, h)
                at_time((20.0, 26.0)[h], inner_pass, 0, h)
                at_time(42.55 + 0.01 * h, inner_onward, 0, h)
                at_time(53.19 + 0.001 * h, inner_last, 0, h)
                at_time(51.0 + 0.05 * h, inner_last, far, h)
            at_time(15.1, far_pass)
            at_time(37.5, far_side)
            at_time(42.5, far_diag)
            for k, when in enumerate((3.5, 6.5, 15.0, 15.2, 15.3, 18.0, 22.0, 24.0)):
                at_time(when, outer_begin, k)
            for k, when in enumerate((3.5, 6.5, 27.5, 9.5, 12.5, 30.0, 42.6, 42.7)):
                at_time(when, inner_ready, k)
            for k, when in enumerate((3.6, 6.6, 27.6, 9.6, 54.22, 55.25, 66.0, 77.0)):
                at_time(when, inward, k, 0)
            for k, when in enumerate((19.0, 25.0, 31.0, 51.5, 55.1, 60.0, 71.0, 83.0)):
                at_time(when, inward, k, 1)
            for k, when in enumerate((9.7, 12.6, 30.1, 42.61, 42.71)):
                at_time(when, outward, k + 3, 0)
            for k, when in enumerate((23.5, 62.0, 73.0, 85.0, 97.0)):
                at_time(when, outward, k + 3, 1)
            for k, when in enumerate((54.2, 68.0, 79.0, 91.0)):
                at_time(when, outward, k + 3, 2)
            at_time(33.1, inner_wait, 0, (0, 1, 2))
            at_time(33.1, inner_arrived, 0)
            at_time(33.2, inner_project, 0, (0,), MOST)
            at_time(37.0, inner_arrived, 1)
            at_time(37.0, inner_project, 0, (1,), MOST)
            at_time(43.5, inner_wait, far, (0, 1, 2))
            at_time(43.6, inner_project, 1, (0, 1), MOST)
            at_time(45.5, inner_arrived, 2)
            at_time(45.6, inner_project, 1, (2,), MOST)
            at_time(52.0, inner_wait, far, (3,))
            at_time(52.1, inner_project, 1, (0, 1, 2), REST)
            at_time(53.1, far_gates)
            at_time(53.15, far_rest, 2, 1)
            at_time(53.18, inner_project, 0, (2,), MOST)
            at_time(53.2, inner_wait, 0, (3,))
            at_time(53.21, inner_project, 0, (0, 1), REST)
            at_time(53.22, own_edge)
            at_time(53.23, far_first)
            at_time(53.24, far_rest, 0)
            at_time(54.21, inner_project, 0, (2,), REST)
            at_time(55.3, own_gates)
            o = 58.0
            at_time(o, line_end, 3, 0)
            at_time(o, half_product, False)
            for e in range(2):
                for h in range(2):
                    at_time(o + 4.0 + 0.1 * e + 0.01 * h, half_relay, False, h, e)
            at_time(o + 4.2, line_end, 3, 1)
            at_time(o + 4.2, line_end, 3, 2)
            at_time(o + 4.3, half_product, True)
            for e in range(2):
                for h in range(2):
                    at_time(o + 9.0 + 0.1 * e + 0.01 * h, half_relay, True, h, e)
            for h in range(halves):
                f = o + 14.0 + 6.0 * h
                at_time(f, finish, 0, h)
                at_time(f + 0.1, gather_start, 1, h)
                at_time(f + 9.0, gather_pass, 1, h)
                at_time(93.0 + 0.1 * h, gather_last, 1, h)
            at_time(88.0, gather_wait, 1, (0, 1, 2))
            at_time(88.1, most_of, 1, (0, 1))
            at_time(92.0, most_of, 1, (2,))
            at_time(94.0, rest_of, 1)
            at_time(103.0, outward, units - 1, 2)
            at_time(106.2, gates_of, 1)
            at_time(128.0, halo_sent, 1)
            for n in range(line):
                p = (110.0, 114.0, 119.0, 125.0)[n]
                if n:
                    at_time(p, line_end, 7, n - 1)
                at_time(p, block_product, n)
                at_time((126.0, 126.0, 126.5, 129.0)[n], block_relay, n)
            at_time(127.5, far_sent)
            at_time(127.6, parts_sent)
            at_time(128.0, gather_sent, 1)
            for k in range(units):
                for s in range(steps):
                    at_time(129.5, line_sent, k, s)
            for h in range(halves):
                at_time(130.0 + h, finish, last, h)
            at_time(140.0, block_sent)
        else:
            for k in range(units):
                at_time(-2.0 if k < 2 else -1.0, scatter_start, k)
            for h in range(halves):
                at_time(-1.5, gather_start, 0, h)
            begin = [k + k // 4 for k in range(units)]
            for k in range(units):
                at_time(begin[k], line_begin, k)
                for s in range(1, steps):
                    at_time(begin[k] + s, line_pass, k, s)
            end = begin[-1] + max(steps, 1) + 1
            ready = [begin[k] + steps for k in range(units)]
            for layer in range(layers):
                if layer == 0:
                    base = ready[0] + 0.5
                else:
                    base = max(ready[4 * layer - 1] + 4.0, end if layer > 1 else 0) + 0.5
                for h in range(halves):
                    at_time(base - 1.3, gather_pass, layer, h)
                    at_time(base - 1.2, gather_last, layer, h)
                w1 = max(base + 0.1, ready[4 * layer + 1] + 0.5)
                w2 = max(w1 + 0.1, ready[4 * layer + 2] + 0.5)
                first_half(layer, base, w1, w2)
                o = max(w2 + 0.1, ready[4 * layer + 3] + 0.5)
                second_half(layer, o)
                for e in range(2):
                    for h in range(2):
                        at_time(o + 0.1, relay, layer, h, e)
                for h in range(halves):
                    at_time(o + 0.3, finish, layer, h)
                    if layer < last:
                        at_time(o + 0.4, gather_start, layer + 1, h)

        for _, _, fn, args in sorted(tasks, key=lambda task: task[:2]):
            fn(*args)
        if not timed:
            for layer in range(layers):
                gather_sent(layer)
            for k in range(units):
                for s in range(steps):
                    line_sent(k, s)

    return kernel


def solution(mesh):
    sp, tp = mesh.shape["sp"], mesh.shape["tp"]

    def shards(tokens, value_weight, outer_weight, inner_weight, conv_taps, output_weight, norm_gain, norm_bias):
        rows, feats = tokens.shape
        layers, depth, channels = value_weight.shape
        taps_count = conv_taps.shape[1]
        q = plane_size(sp, channels)
        width = channels // q
        line = sp // q
        model = feats * tp
        alpha = (2.0 * layers) ** 0.25
        out_cols = output_weight.shape[2]
        bf, f32 = jnp.bfloat16, jnp.float32
        kernel = make_kernel(sp, tp, q, layers, taps_count, rows, feats, depth, width, out_cols, alpha)
        dma = pltpu.SemaphoreType.DMA
        units, steps = 4 * layers, max(line - 1, 1)
        others = max(tp - 1, 1)
        banks = 2 if helped(line, q, tp, layers) else 1
        sets = layers + banks - 1
        halves = 2 if q == 4 else 1
        half_rows = rows // halves
        vm = pl.BlockSpec(memory_space=pltpu.VMEM)
        return pl.pallas_call(
            kernel,
            out_shape=jax.ShapeDtypeStruct((rows, feats), bf),
            in_specs=[vm] * 8,
            out_specs=vm,
            scratch_shapes=[
                pltpu.VMEM((layers + banks - 1, tp, q * rows, feats), bf),
                pltpu.VMEM((layers, 3, model, width), bf),
                pltpu.VMEM((layers, sp, width, out_cols), bf),
                pltpu.VMEM((banks, q * rows, width), bf),
                pltpu.VMEM((banks, q * rows, width), bf),
                pltpu.VMEM((banks, q * rows + 8, width), f32),
                pltpu.VMEM((banks, q * rows, width), bf),
                pltpu.VMEM((layers, tp, q * rows, feats), bf),
                pltpu.VMEM((layers, others, q * rows, feats), bf),
                pltpu.VMEM((layers, q, rows, feats), bf),
                pltpu.VMEM((layers, q, rows, feats), bf),
                pltpu.VMEM((rows, feats), f32),
                pltpu.VMEM((layers, halves, half_rows, LANES), f32),
                pltpu.VMEM((layers, tp, halves, half_rows, LANES), f32),
                pltpu.VMEM((layers, 2, 8, width), f32),
                dma((units, q)), dma((units, q)), dma((units,)),
                dma((units, steps)), dma((units, steps)), dma((units, steps)), dma((units, steps)),
                dma((sets, q, halves)), dma((sets, q, halves)), dma((halves,)),
                dma((sets, tp, q, halves)), dma((sets, tp, q, halves)),
                dma((layers, tp, q)), dma((layers, tp, q)),
                dma((layers, q, 2)), dma((layers, q, 2)),
                dma((layers, tp, halves)), dma((layers, tp, halves)),
                dma((layers,)), dma((layers,)),
                dma((2, 4, 2)), dma((2, 4, 2)), dma((4,)), dma((4,)), dma((4,)), dma((4,)),
                dma((layers, 2, 2)), dma((layers, 2, 2)), dma((layers, 2, 2)), dma((layers, 2, 2)),
            ],
            compiler_params=pltpu.CompilerParams(
                collective_id=0, has_side_effects=True, vmem_limit_bytes=60 * 1024 * 1024
            ),
        )(tokens, value_weight, outer_weight, inner_weight, jnp.swapaxes(conv_taps, 0, 1), output_weight, norm_gain, norm_bias)

    in_specs = (
        P("sp", "tp"),
        P(None, "sp", "tp"),
        P(None, "sp", "tp"),
        P(None, "sp", "tp"),
        P(None, None, "tp"),
        P(None, "tp", "sp"),
        P(None, "tp"),
        P(None, "tp"),
    )
    return jax.shard_map(shards, mesh=mesh, in_specs=in_specs, out_specs=P("sp", "tp"), check_vma=False)
```

```python
import jax
import jax.numpy as jnp
from jax import lax
from jax.experimental import pallas as pl
from jax.experimental.pallas import tpu as pltpu
from jax.sharding import PartitionSpec as P

LANES = 128
EPS = 1e-5


def flip(j, i):
    if i & 1:
        j = j + 1 - 2 * lax.rem(j, 2)
    if i & 2:
        j = j + 2 - 4 * lax.rem(lax.div(j, 2), 2)
    return j


def plane_size(sp, channels):
    q = 4
    while q > 1 and (sp % q or channels // q < LANES or channels % q):
        q //= 2
    return q


def helped(line, q, tp, layers):
    return line == 4 and q == 4 and tp == 2 and layers == 2


def make_kernel(sp, tp, q, layers, taps_count, rows, feats, depth, width, out_cols, alpha):
    line = sp // q
    units = layers * 4
    model = feats * tp
    per_half = sp // tp
    steps = line - 1
    halves = 2 if q == 4 else 1
    half_rows = rows // halves
    timed = helped(line, q, tp, layers)
    slots = line // tp if timed else 1
    block_cols = q * out_cols

    def kernel(
        tok, val, outw, inn, taps, prj, gain, bias, res,
        xg, win, wout, ubuf, obuf, zpad, gated, part, rec1, snd2, rec2, acc, stat, stat_in, halo,
        a_send, a_recv, u_send, u_recv, d_send, d_recv,
        g_send, g_recv, g_loc, t_send, t_recv, p_send, p_recv, r_send, r_recv, s_send, s_recv, h_send, h_recv,
        b_send, b_recv, n_send, n_recv, k_send, k_recv,
        v_recv, w_recv, e_recv,
    ):
        me = lax.axis_index("sp")
        c = lax.axis_index("tp")
        l = lax.div(me, q)
        j = lax.rem(me, q)

        def at_sp(other):
            return {"sp": other, "tp": c}

        def at_tp(r):
            return {"sp": me, "tp": lax.rem(c + r, tp)}

        def remote(src, dst, ssem, rsem, dev):
            return pltpu.make_async_remote_copy(
                src_ref=src, dst_ref=dst, send_sem=ssem, recv_sem=rsem,
                device_id=dev, device_id_type=pl.DeviceIdType.MESH,
            )

        def peer(i):
            return l * q + flip(j, i)

        barrier = pltpu.get_barrier_semaphore()

        def greet(dev):
            pl.semaphore_signal(barrier, inc=1, device_id=dev, device_id_type=pl.DeviceIdType.MESH)

        for i in range(1, q):
            greet(at_sp(peer(i)))
        for r in range(1, tp):
            greet(at_tp(r))

        @pl.when(l > 0)
        def _():
            greet(at_sp(me - q))

        @pl.when(l < line - 1)
        def _():
            greet(at_sp(me + q))

        neighbours = (l > 0).astype(jnp.int32) + (l < line - 1).astype(jnp.int32)
        pl.semaphore_wait(barrier, (q - 1) + (tp - 1) + neighbours)


        ORDER = (val, inn, outw, prj)

        def own_piece(k, jd):
            layer, w = divmod(k, 4)
            at = pl.ds(pl.multiple_of(jd * width, width), width)
            if w == 3:
                return prj.at[layer, at, :]
            return ORDER[w].at[layer, :, at]

        def landed(k, s):
            layer, w = divmod(k, 4)
            if w == 3:
                return wout.at[layer, s]
            return win.at[layer, w, pl.ds(pl.multiple_of(s * depth, depth), depth), :]

        def block(k, b):
            layer, w = divmod(k, 4)
            if w == 3:
                return wout.at[layer, pl.ds(b * q, q)]
            return win.at[layer, w, pl.ds(pl.multiple_of(b * (q * depth), q * depth), q * depth), :]

        def a_copy(k, i):
            return remote(own_piece(k, flip(j, i)), landed(k, me), a_send.at[k], a_recv.at[k], at_sp(peer(i)))

        def a_local(k):
            return pltpu.make_async_copy(own_piece(k, j), landed(k, me), a_recv.at[k])

        def scatter_start(k):
            a_local(k).start()
            for i in range(q - 1, 0, -1):
                a_copy(k, i).start()


        def take(ref, sem):
            pltpu.make_async_copy(ref, ref, sem).wait()

        def scatter_wait(k):
            take(block(k, l), a_recv.at[k])

        def scatter_sent(k):
            layer, w = divmod(k, 4)
            if q > 1:
                n = q - 1
                take(wout.at[layer, pl.ds(0, n)] if w == 3 else win.at[layer, w, pl.ds(0, n * depth), :], a_send.at[k])

        def up(k, s):
            sems = (u_send.at[k], u_recv.at[k, s]) if timed else (u_send.at[k, s], u_recv.at[k, s])
            return remote(block(k, l - s), block(k, l - s), *sems, at_sp(me + q))

        def down(k, s):
            sems = (u_send.at[k], u_recv.at[k, steps - 1 - s]) if timed else (d_send.at[k, s], d_recv.at[k, s])
            return remote(block(k, l + s), block(k, l + s), *sems, at_sp(me - q))

        def line_begin(k):
            scatter_wait(k)

            @pl.when(l < line - 1)
            def _():
                up(k, 0).start()

            @pl.when(l > 0)
            def _():
                down(k, 0).start()

        def line_pass(k, s):
            @pl.when((l - s >= 0) & (l < line - 1))
            def _():
                up(k, s - 1).wait_recv()
                up(k, s).start()

            @pl.when((l + s < line) & (l > 0))
            def _():
                down(k, s - 1).wait_recv()
                down(k, s).start()


        def lower_inner(fn):
            pl.when(l == 1)(fn)

        def upper_inner(fn):
            pl.when(l == 2)(fn)

        def outer(fn):
            pl.when((l == 0) | (l == 3))(fn)

        def inner(fn):
            pl.when((l == 1) | (l == 2))(fn)

        def outer_begin(k):
            @pl.when(l == 0)
            def _():
                scatter_wait(k)
                up(k, 0).start()

            @pl.when(l == 3)
            def _():
                scatter_wait(k)
                down(k, 0).start()

        def inner_ready(k):
            @inner
            def _():
                scatter_wait(k)

        def inward(k, s):
            @lower_inner
            def _():
                if s:
                    up(k, s - 1).wait_recv()
                up(k, s).start()

            @upper_inner
            def _():
                if s:
                    down(k, s - 1).wait_recv()
                down(k, s).start()

        def outward(k, s):
            @lower_inner
            def _():
                if s:
                    down(k, s - 1).wait_recv()
                down(k, s).start()

            @upper_inner
            def _():
                if s:
                    up(k, s - 1).wait_recv()
                up(k, s).start()

        def ends(k):
            return (1, line - 2) if timed and k < 3 else (0, line - 1)

        def line_end(k, s):
            low, high = ends(k)

            @pl.when((l == high) & (l - 1 - s >= 0))
            def _():
                up(k, s).wait_recv()

            @pl.when((l == low) & (l + 1 + s < line))
            def _():
                down(k, s).wait_recv()

        def arrived(k):
            for s in range(steps):
                line_end(k, s)

        def line_sent(k, s):
            @pl.when((l - s >= 0) & (l < line - 1))
            def _():
                up(k, s).wait_send()

            @pl.when((l + s < line) & (l > 0))
            def _():
                down(k, s).wait_send()

        def all_sent(k):
            each = q * depth * width // feats
            scatter_sent(k)

            @outer
            def _():
                take(xg.at[0, 0, pl.ds(0, each), :], u_send.at[k])

            @inner
            def _():
                take(xg.at[0, 0, pl.ds(0, (2 if k < 3 else 5) * each), :], u_send.at[k])


        def part_of(h):
            return pl.ds(h * half_rows, half_rows)

        def spot(layer, jj, h):
            at = pl.ds(pl.multiple_of(jj * rows + h * half_rows, half_rows), half_rows)
            return xg.at[layer, c, at, :]

        def mine(layer, h):
            return tok.at[part_of(h)] if layer == 0 else spot(layer, j, h)

        def g_copy(layer, i, h):
            if i == 3:
                src = spot(layer, flip(j, 1 + h), h)
                return remote(src, src, g_send.at[layer], g_recv.at[layer, i - 1, h], at_sp(peer(2 - h)))
            return remote(
                mine(layer, h), spot(layer, j, h), g_send.at[layer], g_recv.at[layer, i - 1, h], at_sp(peer(i))
            )

        def g_piece(i, e):
            first = (j if i == 2 else flip(j, 2)) * rows + half_rows + e * (half_rows // 2)
            src = xg.at[1, c, pl.ds(pl.multiple_of(first, half_rows // 2), half_rows // 2), :]
            got = e_recv.at[e] if i == 2 else g_recv.at[1, 2, 1]
            return remote(src, src, g_send.at[1], got, at_sp(peer(2 if i == 2 else 1)))

        def g_local(h):
            return pltpu.make_async_copy(tok.at[part_of(h)], spot(0, j, h), g_loc.at[0])

        def rows_like(n):
            return xg.at[0, 0, pl.ds(0, n * rows), :]

        def t_copy(layer, r, i, h):
            src = mine(layer, h) if i == 0 else spot(layer, flip(j, i), h)
            return remote(
                src, spot(layer, flip(j, i), h), t_send.at[layer, r - 1], t_recv.at[layer, r - 1, i // 3], at_tp(r)
            )

        def cross_start(layer, i, h):
            for r in range(1, tp):
                t_copy(layer, r, i, h).start()

        def gather_start(layer, h):
            if layer == 0:
                g_local(h).start()
            for i in range(1, min(q, 3)):
                if timed and layer == 1 and i == 2 and h == 1:
                    for e in range(2):
                        g_piece(2, e).start()
                else:
                    g_copy(layer, i, h).start()
            cross_start(layer, 0, h)

        def gather_pass(layer, h, onward=True):
            first = 1 + h if q == 4 else 1
            for i in range(1, min(q, 3)):
                i = first if i == 1 else 3 - first
                if timed and layer == 1 and i == 2 and h == 1:
                    for e in range(2):
                        g_piece(2, e).wait_recv()
                        g_piece(3, e).start()
                else:
                    g_copy(layer, i, h).wait_recv()
                    if q == 4 and i == first and onward:
                        g_copy(layer, 3, h).start()
                cross_start(layer, i, h)

        def gather_last(layer, h):
            if q == 4:
                g_copy(layer, 3, h).wait_recv()
                cross_start(layer, 3, h)

        def gather_wait(layer, rest):
            for r in range(1, tp):
                take(rows_like(1 if rest else min(q, 3)), t_recv.at[layer, r - 1, 1 if rest else 0])
            if layer == 0 and not rest:
                take(rows_like(1), g_loc.at[0])

        def gather_sent(layer):
            if q > 1:
                take(rows_like(q - 1), g_send.at[layer])
            for r in range(1, tp):
                take(rows_like(q), t_send.at[layer, r - 1])

        def tile_at(jj):
            return pl.ds(pl.multiple_of(jj * rows, rows), rows)


        far = layers
        ALL, MOST, REST = (0, q), (1, q - 1), (0, 1)

        def project(rows_set, layer, w, store, span):
            first = flip(j, q - 1) if span is not ALL else 0

            def tile(n, carry):
                i = lax.rem(first + span[0] + n, q)
                at = tile_at(i)
                total = jnp.zeros((rows, width), jnp.float32)
                for cc in range(tp):
                    total = total + jnp.dot(
                        xg[rows_set, cc, at, :],
                        win[layer, w, pl.ds(cc * feats, feats), :],
                        preferred_element_type=jnp.float32,
                    )
                store(i, total.astype(jnp.bfloat16))
                return carry

            lax.fori_loop(0, span[1], tile, 0)

        def put_u(bank):
            def put(i, v):
                ubuf[bank, tile_at(i), :] = v

            return put

        def put_o(bank):
            def put(i, v):
                obuf[bank, tile_at(i), :] = v

            return put

        def put_z(bank):
            def put(i, v):
                at = pl.ds(pl.multiple_of(8 + i * rows, 8), rows)
                zpad[bank, at, :] = v.astype(jnp.float32) * ubuf[bank, tile_at(i), :].astype(jnp.float32)

            return put

        def h_copy(layer):
            return remote(
                halo.at[layer, 0], halo.at[layer, 1], h_send.at[layer], h_recv.at[layer], at_sp(me + q)
            )

        def halo_start(layer):
            halo[layer, 0] = zpad[0, pl.ds(q * rows, 8), :]

            @pl.when(l < line - 1)
            def _():
                h_copy(layer).start()

        def halo_wait(layer):
            zpad[0, 0:8, :] = jnp.zeros((8, width), jnp.float32)

            @pl.when(l > 0)
            def _():
                h_copy(layer).wait_recv()
                zpad[0, 0:8, :] = halo[layer, 1]

        def convolve(layer, bank, tiles):
            at_c = pl.ds(pl.multiple_of(j * width, width), width)
            rates = [taps[k, pl.ds(layer, 1), at_c] for k in range(taps_count)]
            for i in tiles:
                conv = jnp.zeros((rows, width), jnp.float32)
                for k in range(taps_count):
                    first = 8 - (taps_count - 1) + k + i * rows
                    conv = conv + rates[k] * zpad[bank, first:first + rows, :]
                at = pl.ds(i * rows, rows)
                gated[bank, at, :] = (obuf[bank, at, :].astype(jnp.float32) * conv).astype(jnp.bfloat16)


        def fellow():
            return at_sp(me + q * (1 - 2 * lax.rem(l, 2)))

        def n_copy(n):
            h = n % 2
            src = tok.at[part_of(h)] if n < 2 else spot(far, flip(j, 1 + h), h)
            return remote(
                src, spot(far, j if n < 2 else flip(j, 1 + h), h), n_send.at[0], n_recv.at[n], fellow()
            )

        def e_copy(h):
            return remote(
                tok.at[part_of(h)], spot(far, j, h), g_send.at[far], g_recv.at[far, h, h],
                at_sp(peer(1 + h)),
            )

        def k_copy(i):
            at = tile_at(flip(j, i))
            return remote(gated.at[1, at, :], gated.at[0, at, :], k_send.at[0], k_recv.at[i], fellow())

        def far_send():
            @outer
            def _():
                for h in range(2):
                    e_copy(h).start()
                for n in range(2):
                    n_copy(n).start()

        def far_pass():
            @outer
            def _():
                for h in range(2):
                    e_copy(h).wait_recv()
                    n_copy(2 + h).start()

        def far_in(h):
            @inner
            def _():
                n_copy(h).wait_recv()
                g_copy(far, 2 - h, h).start()
                cross_start(far, 0, h)

        def far_side():
            @inner
            def _():
                for h in range(2):
                    g_copy(far, 2 - h, h).wait_recv()
                    cross_start(far, 2 - h, h)

        def far_diag():
            @inner
            def _():
                for h in range(2):
                    n_copy(2 + h).wait_recv()
                    g_copy(far, 3, h).start()
                    cross_start(far, 1 + h, h)

        def inner_gather_start(h):
            @inner
            def _():
                gather_start(0, h)

        def inner_pass(rows_set, h):
            @inner
            def _():
                gather_pass(rows_set, h, False)

        def inner_onward(rows_set, h):
            @inner
            def _():
                g_copy(rows_set, 3, h).start()

        def inner_last(rows_set, h):
            @inner
            def _():
                gather_last(rows_set, h)

        def inner_wait(rows_set, rest):
            @inner
            def _():
                gather_wait(rows_set, rest)

        def inner_project(bank, ws, span):
            @inner
            def _():
                for w in ws:
                    project(far if bank else 0, 0, w, (put_u, put_z, put_o)[w](bank), span)

        def inner_arrived(k):
            @inner
            def _():
                arrived(k)

        def own_edge():
            @lower_inner
            def _():
                halo[0, 0] = zpad[0, pl.ds(q * rows, 8), :]
                h_copy(0).start()

        tail = pl.ds(q * rows, 8)

        def far_gates():
            @pl.when((l == 1) | ((l == 2) & (j == 0)))
            def _():
                zpad[1, 0:8, :] = jnp.zeros((8, width), jnp.float32)

            @pl.when((l == 2) & (j > 0))
            def _():
                zpad[1, 0:8, :] = zpad[0, tail, :]

            @inner
            def _():
                convolve(0, 1, range(q))
                k_copy(q - 1).start()

        def far_first():
            @pl.when((l == 2) & (j == 0))
            def _():
                zpad[1, 0:8, :] = zpad[0, tail, :]
                convolve(0, 1, range(1))

        def own_gates():
            @lower_inner
            def _():
                zpad[0, 0:8, :] = zpad[1, tail, :]

            @upper_inner
            def _():
                h_copy(0).wait_recv()
                zpad[0, 0:8, :] = halo[0, 1]

            @inner
            def _():
                convolve(0, 0, range(q))

        def far_rest(*which):
            @inner
            def _():
                for i in which:
                    k_copy(i).start()

        def far_sent():
            @outer
            def _():
                take(rows_like(1), g_send.at[far])
                take(rows_like(2), n_send.at[0])

            @inner
            def _():
                gather_sent(0)
                take(rows_like(2), g_send.at[far])
                for r in range(1, tp):
                    take(rows_like(q), t_send.at[far, r - 1])
                take(gated.at[1], k_send.at[0])

            @lower_inner
            def _():
                h_copy(0).wait_send()


        def p_copy(layer, r, i):
            at = tile_at(flip(j, i))
            return remote(
                part.at[layer, lax.rem(c + r, tp), at, :], rec1.at[layer, r - 1, at, :],
                p_send.at[layer, r - 1], p_recv.at[layer, r - 1, i], at_tp(r),
            )


        bit_rows = half_rows // 2

        def bit_of(h, e):
            return pl.ds(h * half_rows + e * bit_rows, bit_rows)

        def r_copy(layer, i, h):
            at = part_of(h)
            return remote(
                snd2.at[layer, i, at, :], rec2.at[layer, i, at, :],
                r_send.at[layer], r_recv.at[layer, i - 1], at_sp(peer(i)),
            )

        def w_copy(layer, h, e):
            at = bit_of(h, e)
            return remote(
                snd2.at[layer, 2 - h, at, :], rec2.at[layer, 2 - h, at, :],
                r_send.at[layer], w_recv.at[layer, h, e], at_sp(peer(2 - h)),
            )

        def v_copy(layer, h, e):
            at = bit_of(h, e)
            return remote(
                snd2.at[layer, 3, at, :], rec2.at[layer, 3, at, :],
                r_send.at[layer], v_recv.at[layer, h, e], at_sp(peer(1 + h)),
            )

        def reduce_tile(layer, i):
            at = tile_at(flip(j, i))
            total = part[layer, c, at, :].astype(jnp.float32)
            for r in range(1, tp):
                p_copy(layer, r, i).wait_recv()
                total = total + rec1[layer, r - 1, at, :].astype(jnp.float32)
            if i == 0:
                acc[...] = total
                return
            snd2[layer, i] = total.astype(jnp.bfloat16)
            if i == 3:
                for e in range(2):
                    for h in range(2):
                        v_copy(layer, h, e).start()
            elif halves == 1:
                r_copy(layer, i, 0).start()
            elif i == 1:
                r_copy(layer, 1, 0).start()

        def relay(layer, h, e):
            if halves == 2:
                v_copy(layer, h, e).wait_recv()
                i, at = 2 - h, bit_of(h, e)
                snd2[layer, i, at, :] = (
                    snd2[layer, i, at, :].astype(jnp.float32) + rec2[layer, 3, at, :].astype(jnp.float32)
                ).astype(jnp.bfloat16)
                w_copy(layer, h, e).start()
                if h == 0 and e == 1:
                    r_copy(layer, 2, 1).start()

        def out_product(layer):
            for i in range(q - 1, -1, -1):
                at = tile_at(flip(j, i))

                def half(n, carry):
                    cc = lax.rem(c + 1 + n, tp)
                    weight = jnp.concatenate([wout[layer, cc * per_half + b] for b in range(per_half)], axis=1)
                    part[layer, cc, at, :] = jnp.dot(
                        gated[0, at, :], weight, preferred_element_type=jnp.float32
                    ).astype(jnp.bfloat16)
                    return carry

                lax.fori_loop(0, tp, half, 0)
                for r in range(1, tp):
                    p_copy(layer, r, i).start()
                if i < q - 1:
                    reduce_tile(layer, i + 1)
            reduce_tile(layer, 0)


        def late_half():
            return (l < line // 2).astype(jnp.int32)

        def half_product(second):
            cc = late_half() if second else 1 - late_half()
            weight = jnp.concatenate([wout[0, cc * per_half + b] for b in range(per_half)], axis=1)
            for i in range(q - 1, -1, -1):
                at = tile_at(flip(j, i))
                if not second:
                    @outer
                    def _():
                        k_copy(i).wait_recv()

                part[0, cc, at, :] = jnp.dot(
                    gated[0, at, :], weight, preferred_element_type=jnp.float32
                ).astype(jnp.bfloat16)

                @pl.when(cc != c)
                def _():
                    p_copy(0, 1, i).start()

                if i < q - 1:
                    @pl.when(cc == c)
                    def _():
                        reduce_tile(0, i + 1)

            @pl.when(cc == c)
            def _():
                reduce_tile(0, 0)

        def half_relay(second, h, e):
            @pl.when((late_half() == c) if second else (late_half() != c))
            def _():
                relay(0, h, e)


        last = layers - 1

        def nth_block(n):
            upper = (l >= line // 2).astype(jnp.int32)
            inner = ((l > 0) & (l < line - 1)).astype(jnp.int32)
            b = n
            if n < 2:
                b = n + inner * (1 - 2 * n)
            return b + upper * (line - 1 - 2 * b)

        def cols_of(m):
            return pl.ds(pl.multiple_of(m * block_cols, block_cols), block_cols)

        def q_copy(n, i):
            b = nth_block(n)
            m = lax.rem(b, slots)
            at = tile_at(flip(j, i))
            return remote(
                part.at[last, lax.div(b, slots), at, cols_of(m)], rec1.at[last, 0, at, cols_of(m)],
                p_send.at[last, 0], p_recv.at[last, m, i], at_tp(1),
            )

        def b_copy(m, i, h):
            at = part_of(h)
            return remote(
                snd2.at[last, i, at, cols_of(m)], rec2.at[last, i, at, cols_of(m)],
                b_send.at[0], b_recv.at[m, i - 1, h], at_sp(peer(i if i < 3 else 1 + h)),
            )

        def block_product(n):
            b = nth_block(n)
            m = lax.rem(b, slots)
            own = lax.div(b, slots) == c
            weight = jnp.concatenate([wout[last, b * q + e] for e in range(q)], axis=1)
            for i in range(q - 1, -1, -1):
                at = tile_at(flip(j, i))
                part[last, lax.div(b, slots), at, cols_of(m)] = jnp.dot(
                    gated[0, at, :], weight, preferred_element_type=jnp.float32
                ).astype(jnp.bfloat16)

                @pl.when(jnp.logical_not(own))
                def _():
                    q_copy(n, i).start()

            @pl.when(own)
            def _():
                for i in range(q - 1, -1, -1):
                    at = tile_at(flip(j, i))
                    q_copy(n, i).wait_recv()
                    total = part[last, c, at, cols_of(m)].astype(jnp.float32)
                    total = total + rec1[last, 0, at, cols_of(m)].astype(jnp.float32)
                    if i == 0:
                        acc[:, cols_of(m)] = total
                        continue
                    snd2[last, i, :, cols_of(m)] = total.astype(jnp.bfloat16)
                    if i == 3:
                        b_copy(m, 3, 0).start()
                        b_copy(m, 3, 1).start()
                    elif i == 1:
                        b_copy(m, 1, 0).start()

        def block_relay(n):
            b = nth_block(n)
            m = lax.rem(b, slots)

            @pl.when(lax.div(b, slots) == c)
            def _():
                for h in range(2):
                    b_copy(m, 3, h).wait_recv()
                    i, at = 2 - h, part_of(h)
                    snd2[last, i, at, cols_of(m)] = (
                        snd2[last, i, at, cols_of(m)].astype(jnp.float32)
                        + rec2[last, 3, at, cols_of(m)].astype(jnp.float32)
                    ).astype(jnp.bfloat16)
                    b_copy(m, i, h).start()
                    if h == 0:
                        b_copy(m, 2, 1).start()

        def sums_sent(layer):
            for r in range(1, tp):
                take(part.at[layer, 0], p_send.at[layer, r - 1])
                take(stat.at[layer], s_send.at[layer, r - 1])
            if q > 1:
                take(snd2.at[layer, pl.ds(0, q - 1)], b_send.at[0] if timed and layer == last else r_send.at[layer])

        def s_copy(layer, r, h):
            return remote(
                stat.at[layer, h], stat_in.at[layer, r, h], s_send.at[layer, r - 1], s_recv.at[layer, r - 1, h], at_tp(r)
            )

        def finish(layer, h):
            at = part_of(h)
            pre = alpha * mine(layer, h)[...].astype(jnp.float32) + acc[at, :]
            for i in range(1, min(q, 3)):
                if timed and layer == last:
                    for m in range(slots):
                        b_copy(m, i, h).wait_recv()
                elif halves == 2 and i == 2 - h:
                    for e in range(2):
                        w_copy(layer, h, e).wait_recv()
                else:
                    r_copy(layer, i, h).wait_recv()
                pre = pre + rec2[layer, i, at, :].astype(jnp.float32)
            acc[at, :] = pre
            own = jnp.sum(pre, axis=-1, keepdims=True)
            away = pre - own * (1.0 / feats)
            spread = jnp.sum(away * away, axis=-1, keepdims=True)
            lane = lax.broadcasted_iota(jnp.int32, (half_rows, LANES), 1)
            stat[layer, h] = jnp.where(lane == 0, own, spread)
            for r in range(1, tp):
                s_copy(layer, r, h).start()
            sums, spreads = [own], [spread]
            for r in range(1, tp):
                s_copy(layer, r, h).wait_recv()
                sums.append(stat_in[layer, r, h, :, 0:1])
                spreads.append(stat_in[layer, r, h, :, 1:2])
            mean = sum(sums[1:], sums[0]) * (1.0 / model)
            var = sum(spreads[1:], spreads[0])
            for s in sums:
                off = s * (1.0 / feats) - mean
                var = var + feats * off * off
            scale = lax.rsqrt(var * (1.0 / model) + EPS)
            normed = (acc[at, :] - mean) * scale
            y = (normed * gain[pl.ds(layer, 1), :] + bias[pl.ds(layer, 1), :]).astype(jnp.bfloat16)
            if layer == last:
                res[at, :] = y
            else:
                mine(layer + 1, h)[...] = y


        tasks = []

        def at_time(when, fn, *args):
            tasks.append((when, len(tasks), fn, args))

        def first_half(layer, w0, w1, w2):
            def start():
                gather_wait(layer, False)
                if q > 3:
                    gather_wait(layer, True)
                arrived(layer * 4)
                project(layer, layer, 0, put_u(0), ALL)

            def middle():
                arrived(layer * 4 + 1)
                project(layer, layer, 1, put_z(0), ALL)
                halo_start(layer)

            def gates():
                arrived(layer * 4 + 2)
                project(layer, layer, 2, put_o(0), ALL)
                halo_wait(layer)
                convolve(layer, 0, range(q))
                halo_sent(layer)

            at_time(w0, start)
            at_time(w1, middle)
            at_time(w2, gates)

        def most_of(layer, ws):
            for w in ws:
                arrived(layer * 4 + w)
                project(layer, layer, w, (put_u, put_z, put_o)[w](0), MOST)

        def rest_of(layer):
            gather_wait(layer, True)
            project(layer, layer, 0, put_u(0), REST)
            project(layer, layer, 1, put_z(0), REST)
            halo_start(layer)

        def gates_of(layer):
            project(layer, layer, 2, put_o(0), REST)
            halo_wait(layer)
            convolve(layer, 0, range(q))

        def halo_sent(layer):
            @pl.when(l < line - 1)
            def _():
                h_copy(layer).wait_send()

        def second_half(layer, when):
            def go():
                arrived(layer * 4 + 3)
                out_product(layer)

            at_time(when, go)

        if timed:
            at_time(-1.0, far_send)
            for when, k in ((0.0, 0), (0.1, 1), (0.2, 3), (0.3, 4), (0.5, 2), (0.6, 5), (13.7, 6), (13.8, 7)):
                at_time(when, scatter_start, k)
            for h in range(halves):
                at_time(0.4, inner_gather_start, h)
                at_time((8.6, 13.6)[h], far_in, h)
                at_time((20.0, 26.0)[h], inner_pass, 0, h)
                at_time(42.55 + 0.01 * h, inner_onward, 0, h)
                at_time(53.19 + 0.001 * h, inner_last, 0, h)
                at_time(51.0 + 0.05 * h, inner_last, far, h)
            at_time(15.1, far_pass)
            at_time(37.5, far_side)
            at_time(42.5, far_diag)
            for k, when in enumerate((3.5, 6.5, 15.0, 15.2, 15.3, 18.0, 22.0, 24.0)):
                at_time(when, outer_begin, k)
            for k, when in enumerate((3.5, 6.5, 27.5, 9.5, 12.5, 30.0, 42.6, 42.7)):
                at_time(when, inner_ready, k)
            for k, when in enumerate((3.6, 6.6, 27.6, 9.6, 54.22, 55.25, 66.0, 77.0)):
                at_time(when, inward, k, 0)
            for k, when in enumerate((19.0, 25.0, 31.0, 51.5, 55.1, 60.0, 71.0, 83.0)):
                at_time(when, inward, k, 1)
            for k, when in enumerate((9.7, 12.6, 30.1, 42.61, 42.71)):
                at_time(when, outward, k + 3, 0)
            for k, when in enumerate((23.5, 62.0, 73.0, 85.0, 97.0)):
                at_time(when, outward, k + 3, 1)
            for k, when in enumerate((54.2, 68.0, 79.0, 91.0)):
                at_time(when, outward, k + 3, 2)
            at_time(33.1, inner_wait, 0, False)
            at_time(33.1, inner_arrived, 0)
            at_time(33.2, inner_project, 0, (0,), MOST)
            at_time(37.0, inner_arrived, 1)
            at_time(37.0, inner_project, 0, (1,), MOST)
            at_time(43.5, inner_wait, far, False)
            at_time(43.6, inner_project, 1, (0, 1), MOST)
            at_time(45.5, inner_arrived, 2)
            at_time(45.6, inner_project, 1, (2,), MOST)
            at_time(52.0, inner_wait, far, True)
            at_time(52.1, inner_project, 1, (0, 1, 2), REST)
            at_time(53.1, far_gates)
            at_time(53.15, far_rest, 2, 1)
            at_time(53.18, inner_project, 0, (2,), MOST)
            at_time(53.2, inner_wait, 0, True)
            at_time(53.21, inner_project, 0, (0, 1), REST)
            at_time(53.22, own_edge)
            at_time(53.23, far_first)
            at_time(53.24, far_rest, 0)
            at_time(54.21, inner_project, 0, (2,), REST)
            at_time(55.3, own_gates)
            o = 58.0
            at_time(o, line_end, 3, 0)
            at_time(o, half_product, False)
            for e in range(2):
                for h in range(2):
                    at_time(o + 4.0 + 0.1 * e + 0.01 * h, half_relay, False, h, e)
            at_time(o + 4.2, line_end, 3, 1)
            at_time(o + 4.2, line_end, 3, 2)
            at_time(o + 4.3, half_product, True)
            for e in range(2):
                for h in range(2):
                    at_time(o + 9.0 + 0.1 * e + 0.01 * h, half_relay, True, h, e)
            for h in range(halves):
                f = o + 14.0 + 6.0 * h
                at_time(f, finish, 0, h)
                at_time(f + 0.1, gather_start, 1, h)
                at_time(f + 9.0, gather_pass, 1, h)
                at_time(93.0 + 0.1 * h, gather_last, 1, h)
            at_time(88.0, gather_wait, 1, False)
            at_time(88.1, most_of, 1, (0, 1))
            at_time(92.0, most_of, 1, (2,))
            at_time(94.0, rest_of, 1)
            at_time(103.0, outward, units - 1, 2)
            at_time(106.2, gates_of, 1)
            at_time(128.0, halo_sent, 1)
            for n in range(line):
                p = (110.0, 114.0, 119.0, 125.0)[n]
                if n:
                    at_time(p, line_end, 7, n - 1)
                at_time(p, block_product, n)
                at_time((126.0, 126.0, 126.5, 129.0)[n], block_relay, n)
            at_time(127.5, far_sent)
            at_time(128.0, gather_sent, 1)
            at_time(128.1, sums_sent, 0)
            for k in range(units):
                at_time(129.5, all_sent, k)
            for h in range(halves):
                at_time(130.0 + h, finish, last, h)
            at_time(140.0, sums_sent, last)
        else:
            for k in range(units):
                at_time(-2.0 if k < 2 else -1.0, scatter_start, k)
            for h in range(halves):
                at_time(-1.5, gather_start, 0, h)
            begin = [k + k // 4 for k in range(units)]
            for k in range(units):
                at_time(begin[k], line_begin, k)
                for s in range(1, steps):
                    at_time(begin[k] + s, line_pass, k, s)
            end = begin[-1] + max(steps, 1) + 1
            ready = [begin[k] + steps for k in range(units)]
            for layer in range(layers):
                if layer == 0:
                    base = ready[0] + 0.5
                else:
                    base = max(ready[4 * layer - 1] + 4.0, end if layer > 1 else 0) + 0.5
                for h in range(halves):
                    at_time(base - 1.3, gather_pass, layer, h)
                    at_time(base - 1.2, gather_last, layer, h)
                w1 = max(base + 0.1, ready[4 * layer + 1] + 0.5)
                w2 = max(w1 + 0.1, ready[4 * layer + 2] + 0.5)
                first_half(layer, base, w1, w2)
                o = max(w2 + 0.1, ready[4 * layer + 3] + 0.5)
                second_half(layer, o)
                for e in range(2):
                    for h in range(2):
                        at_time(o + 0.1, relay, layer, h, e)
                for h in range(halves):
                    at_time(o + 0.3, finish, layer, h)
                    if layer < last:
                        at_time(o + 0.4, gather_start, layer + 1, h)

        for _, _, fn, args in sorted(tasks, key=lambda task: task[:2]):
            fn(*args)
        if not timed:
            for layer in range(layers):
                gather_sent(layer)
                sums_sent(layer)
            for k in range(units):
                scatter_sent(k)
                for s in range(steps):
                    line_sent(k, s)

    return kernel


def solution(mesh):
    sp, tp = mesh.shape["sp"], mesh.shape["tp"]

    def shards(tokens, value_weight, outer_weight, inner_weight, conv_taps, output_weight, norm_gain, norm_bias):
        rows, feats = tokens.shape
        layers, depth, channels = value_weight.shape
        taps_count = conv_taps.shape[1]
        q = plane_size(sp, channels)
        width = channels // q
        line = sp // q
        model = feats * tp
        alpha = (2.0 * layers) ** 0.25
        out_cols = output_weight.shape[2]
        bf, f32 = jnp.bfloat16, jnp.float32
        kernel = make_kernel(sp, tp, q, layers, taps_count, rows, feats, depth, width, out_cols, alpha)
        dma = pltpu.SemaphoreType.DMA
        units, steps = 4 * layers, max(line - 1, 1)
        others = max(tp - 1, 1)
        banks = 2 if helped(line, q, tp, layers) else 1
        sets = layers + banks - 1
        relays = 1 if banks == 2 else layers
        if banks == 2:
            lines = [dma((units,)), dma((units, steps)), dma((1,)), dma((1,))]
        else:
            lines = [dma((units, steps))] * 4
        halves = 2 if q == 4 else 1
        half_rows = rows // halves
        vm = pl.BlockSpec(memory_space=pltpu.VMEM)
        return pl.pallas_call(
            kernel,
            out_shape=jax.ShapeDtypeStruct((rows, feats), bf),
            in_specs=[vm] * 8,
            out_specs=vm,
            scratch_shapes=[
                pltpu.VMEM((layers + banks - 1, tp, q * rows, feats), bf),
                pltpu.VMEM((layers, 3, model, width), bf),
                pltpu.VMEM((layers, sp, width, out_cols), bf),
                pltpu.VMEM((banks, q * rows, width), bf),
                pltpu.VMEM((banks, q * rows, width), bf),
                pltpu.VMEM((banks, q * rows + 8, width), f32),
                pltpu.VMEM((banks, q * rows, width), bf),
                pltpu.VMEM((layers, tp, q * rows, feats), bf),
                pltpu.VMEM((layers, others, q * rows, feats), bf),
                pltpu.VMEM((layers, q, rows, feats), bf),
                pltpu.VMEM((layers, q, rows, feats), bf),
                pltpu.VMEM((rows, feats), f32),
                pltpu.VMEM((layers, halves, half_rows, LANES), f32),
                pltpu.VMEM((layers, tp, halves, half_rows, LANES), f32),
                pltpu.VMEM((layers, 2, 8, width), f32),
                dma((units,)), dma((units,)), *lines,
                dma((sets,)), dma((sets, 3, halves)), dma((1,)),
                dma((sets, others)), dma((sets, others, 2)),
                dma((layers, others)), dma((layers, max(others, 2), q)),
                dma((layers,)), dma((layers, 2)),
                dma((layers, others)), dma((layers, others, halves)),
                dma((layers,)), dma((layers,)),
                dma((1,)), dma((2, 3, 2)), dma((1,)), dma((4,)), dma((1,)), dma((4,)),
                dma((relays, 2, 2)), dma((relays, 2, 2)), dma((2,)),
            ],
            compiler_params=pltpu.CompilerParams(
                collective_id=0, has_side_effects=True, vmem_limit_bytes=60 * 1024 * 1024
            ),
        )(tokens, value_weight, outer_weight, inner_weight, jnp.swapaxes(conv_taps, 0, 1), output_weight, norm_gain, norm_bias)

    in_specs = (
        P("sp", "tp"),
        P(None, "sp", "tp"),
        P(None, "sp", "tp"),
        P(None, "sp", "tp"),
        P(None, None, "tp"),
        P(None, "tp", "sp"),
        P(None, "tp"),
        P(None, "tp"),
    )
    return jax.shard_map(shards, mesh=mesh, in_specs=in_specs, out_specs=P("sp", "tp"), check_vma=False)
```

```python
import jax
import jax.numpy as jnp
from jax import lax
from jax.experimental import pallas as pl
from jax.experimental.pallas import tpu as pltpu
from jax.sharding import PartitionSpec as P

LANES = 128
EPS = 1e-5


def flip(j, i):
    if i & 1:
        j = j + 1 - 2 * lax.rem(j, 2)
    if i & 2:
        j = j + 2 - 4 * lax.rem(lax.div(j, 2), 2)
    return j


def plane_size(sp, channels):
    q = 4
    while q > 1 and (sp % q or channels // q < LANES or channels % q):
        q //= 2
    return q


def helped(line, q, tp, layers):
    return line == 4 and q == 4 and tp == 2 and layers == 2


def make_kernel(sp, tp, q, layers, taps_count, rows, feats, depth, width, out_cols, alpha):
    line = sp // q
    units = layers * 4
    model = feats * tp
    per_half = sp // tp
    steps = line - 1
    halves = 2 if q == 4 else 1
    half_rows = rows // halves
    timed = helped(line, q, tp, layers)
    slots = line // tp if timed else 1
    block_cols = q * out_cols

    def kernel(
        tok, val, outw, inn, taps, prj, gain, bias, res,
        xg, win, wout, ubuf, obuf, zpad, gated, part, rec1, snd2, rec2, acc, stat, stat_in, halo,
        a_send, a_recv, u_send, u_recv, d_send, d_recv,
        g_send, g_recv, g_loc, t_send, t_recv, p_send, p_recv, r_send, r_recv, s_send, s_recv, h_send, h_recv,
        b_send, b_recv, n_send, n_recv, k_send, k_recv,
        v_recv, w_recv, e_recv,
    ):
        me = lax.axis_index("sp")
        c = lax.axis_index("tp")
        l = lax.div(me, q)
        j = lax.rem(me, q)

        def at_sp(other):
            return {"sp": other, "tp": c}

        def at_tp(r):
            return {"sp": me, "tp": lax.rem(c + r, tp)}

        def remote(src, dst, ssem, rsem, dev):
            return pltpu.make_async_remote_copy(
                src_ref=src, dst_ref=dst, send_sem=ssem, recv_sem=rsem,
                device_id=dev, device_id_type=pl.DeviceIdType.MESH,
            )

        def peer(i):
            return l * q + flip(j, i)

        barrier = pltpu.get_barrier_semaphore()

        def greet(dev):
            pl.semaphore_signal(barrier, inc=1, device_id=dev, device_id_type=pl.DeviceIdType.MESH)

        for i in range(1, q):
            greet(at_sp(peer(i)))
        for r in range(1, tp):
            greet(at_tp(r))

        @pl.when(l > 0)
        def _():
            greet(at_sp(me - q))

        @pl.when(l < line - 1)
        def _():
            greet(at_sp(me + q))

        neighbours = (l > 0).astype(jnp.int32) + (l < line - 1).astype(jnp.int32)
        pl.semaphore_wait(barrier, (q - 1) + (tp - 1) + neighbours)


        ORDER = (val, inn, outw, prj)

        def own_piece(k, jd):
            layer, w = divmod(k, 4)
            at = pl.ds(pl.multiple_of(jd * width, width), width)
            if w == 3:
                return prj.at[layer, at, :]
            return ORDER[w].at[layer, :, at]

        def landed(k, s):
            layer, w = divmod(k, 4)
            if w == 3:
                return wout.at[layer, s]
            return win.at[layer, w, pl.ds(pl.multiple_of(s * depth, depth), depth), :]

        def block(k, b):
            layer, w = divmod(k, 4)
            if w == 3:
                return wout.at[layer, pl.ds(b * q, q)]
            return win.at[layer, w, pl.ds(pl.multiple_of(b * (q * depth), q * depth), q * depth), :]

        def a_copy(k, i):
            return remote(own_piece(k, flip(j, i)), landed(k, me), a_send.at[k], a_recv.at[k], at_sp(peer(i)))

        def a_local(k):
            return pltpu.make_async_copy(own_piece(k, j), landed(k, me), a_recv.at[k])

        def scatter_start(k):
            a_local(k).start()
            for i in range(q - 1, 0, -1):
                a_copy(k, i).start()


        def take(ref, sem):
            pltpu.make_async_copy(ref, ref, sem).wait()

        def scatter_wait(k):
            take(block(k, l), a_recv.at[k])

        def scatter_sent(k):
            layer, w = divmod(k, 4)
            if q > 1:
                n = q - 1
                take(wout.at[layer, pl.ds(0, n)] if w == 3 else win.at[layer, w, pl.ds(0, n * depth), :], a_send.at[k])

        def up(k, s):
            sems = (u_send.at[k], u_recv.at[k, s]) if timed else (u_send.at[k, s], u_recv.at[k, s])
            return remote(block(k, l - s), block(k, l - s), *sems, at_sp(me + q))

        def down(k, s):
            sems = (u_send.at[k], u_recv.at[k, steps - 1 - s]) if timed else (d_send.at[k, s], d_recv.at[k, s])
            return remote(block(k, l + s), block(k, l + s), *sems, at_sp(me - q))

        def line_begin(k):
            scatter_wait(k)

            @pl.when(l < line - 1)
            def _():
                up(k, 0).start()

            @pl.when(l > 0)
            def _():
                down(k, 0).start()

        def line_pass(k, s):
            @pl.when((l - s >= 0) & (l < line - 1))
            def _():
                up(k, s - 1).wait_recv()
                up(k, s).start()

            @pl.when((l + s < line) & (l > 0))
            def _():
                down(k, s - 1).wait_recv()
                down(k, s).start()


        def lower_inner(fn):
            pl.when(l == 1)(fn)

        def upper_inner(fn):
            pl.when(l == 2)(fn)

        def outer(fn):
            pl.when((l == 0) | (l == 3))(fn)

        def inner(fn):
            pl.when((l == 1) | (l == 2))(fn)

        def outer_begin(k):
            @pl.when(l == 0)
            def _():
                scatter_wait(k)
                up(k, 0).start()

            @pl.when(l == 3)
            def _():
                scatter_wait(k)
                down(k, 0).start()

        def inner_ready(k):
            @inner
            def _():
                scatter_wait(k)

        def inward(k, s):
            @lower_inner
            def _():
                if s:
                    up(k, s - 1).wait_recv()
                up(k, s).start()

            @upper_inner
            def _():
                if s:
                    down(k, s - 1).wait_recv()
                down(k, s).start()

        def outward(k, s):
            @lower_inner
            def _():
                if s:
                    down(k, s - 1).wait_recv()
                down(k, s).start()

            @upper_inner
            def _():
                if s:
                    up(k, s - 1).wait_recv()
                up(k, s).start()

        def ends(k):
            return (1, line - 2) if timed and k < 3 else (0, line - 1)

        def line_end(k, s):
            low, high = ends(k)

            @pl.when((l == high) & (l - 1 - s >= 0))
            def _():
                up(k, s).wait_recv()

            @pl.when((l == low) & (l + 1 + s < line))
            def _():
                down(k, s).wait_recv()

        def arrived(k):
            for s in range(steps):
                line_end(k, s)

        def line_sent(k, s):
            @pl.when((l - s >= 0) & (l < line - 1))
            def _():
                up(k, s).wait_send()

            @pl.when((l + s < line) & (l > 0))
            def _():
                down(k, s).wait_send()

        def all_sent(k):
            each = q * depth * width // feats
            scatter_sent(k)

            @outer
            def _():
                take(xg.at[0, 0, pl.ds(0, each), :], u_send.at[k])

            @inner
            def _():
                take(xg.at[0, 0, pl.ds(0, (2 if k < 3 else 5) * each), :], u_send.at[k])


        def part_of(h):
            return pl.ds(h * half_rows, half_rows)

        def spot(layer, jj, h):
            at = pl.ds(pl.multiple_of(jj * rows + h * half_rows, half_rows), half_rows)
            return xg.at[layer, c, at, :]

        def mine(layer, h):
            return tok.at[part_of(h)] if layer == 0 else spot(layer, j, h)

        def g_copy(layer, i, h):
            if i == 3:
                src = spot(layer, flip(j, 1 + h), h)
                return remote(src, src, g_send.at[layer], g_recv.at[layer, i - 1, h], at_sp(peer(2 - h)))
            return remote(
                mine(layer, h), spot(layer, j, h), g_send.at[layer], g_recv.at[layer, i - 1, h], at_sp(peer(i))
            )

        def g_piece(i, e):
            first = (j if i == 2 else flip(j, 2)) * rows + half_rows + e * (half_rows // 2)
            src = xg.at[1, c, pl.ds(pl.multiple_of(first, half_rows // 2), half_rows // 2), :]
            got = e_recv.at[e] if i == 2 else g_recv.at[1, 2, 1]
            return remote(src, src, g_send.at[1], got, at_sp(peer(2 if i == 2 else 1)))

        def g_local(h):
            return pltpu.make_async_copy(tok.at[part_of(h)], spot(0, j, h), g_loc.at[0])

        def rows_like(n):
            return xg.at[0, 0, pl.ds(0, n * rows), :]

        def t_copy(layer, r, i, h):
            src = mine(layer, h) if i == 0 else spot(layer, flip(j, i), h)
            return remote(
                src, spot(layer, flip(j, i), h), t_send.at[layer, r - 1], t_recv.at[layer, r - 1, i // 3], at_tp(r)
            )

        def cross_start(layer, i, h):
            for r in range(1, tp):
                t_copy(layer, r, i, h).start()

        def gather_start(layer, h):
            if layer == 0:
                g_local(h).start()
            for i in range(1, min(q, 3)):
                if timed and layer == 1 and i == 2 and h == 1:
                    for e in range(2):
                        g_piece(2, e).start()
                else:
                    g_copy(layer, i, h).start()
            cross_start(layer, 0, h)

        def gather_pass(layer, h, onward=True):
            first = 1 + h if q == 4 else 1
            for i in range(1, min(q, 3)):
                i = first if i == 1 else 3 - first
                if timed and layer == 1 and i == 2 and h == 1:
                    for e in range(2):
                        g_piece(2, e).wait_recv()
                        g_piece(3, e).start()
                else:
                    g_copy(layer, i, h).wait_recv()
                    if q == 4 and i == first and onward:
                        g_copy(layer, 3, h).start()
                cross_start(layer, i, h)

        def gather_last(layer, h):
            if q == 4:
                g_copy(layer, 3, h).wait_recv()
                cross_start(layer, 3, h)

        def gather_wait(layer, rest):
            for r in range(1, tp):
                take(rows_like(1 if rest else min(q, 3)), t_recv.at[layer, r - 1, 1 if rest else 0])
            if layer == 0 and not rest:
                take(rows_like(1), g_loc.at[0])

        def gather_sent(layer):
            if q > 1:
                take(rows_like(q - 1), g_send.at[layer])
            for r in range(1, tp):
                take(rows_like(q), t_send.at[layer, r - 1])

        def tile_at(jj):
            return pl.ds(pl.multiple_of(jj * rows, rows), rows)


        far = layers
        ALL, MOST, REST = (0, q), (1, q - 1), (0, 1)

        def project(rows_set, layer, w, store, span):
            first = flip(j, q - 1) if span is not ALL else 0

            def tile(n, carry):
                i = lax.rem(first + span[0] + n, q)
                at = tile_at(i)
                total = jnp.zeros((rows, width), jnp.float32)
                for cc in range(tp):
                    total = total + jnp.dot(
                        xg[rows_set, cc, at, :],
                        win[layer, w, pl.ds(cc * feats, feats), :],
                        preferred_element_type=jnp.float32,
                    )
                store(i, total.astype(jnp.bfloat16))
                return carry

            lax.fori_loop(0, span[1], tile, 0)

        def put_u(bank):
            def put(i, v):
                ubuf[bank, tile_at(i), :] = v

            return put

        def put_o(bank):
            def put(i, v):
                obuf[bank, tile_at(i), :] = v

            return put

        def put_z(bank):
            def put(i, v):
                at = pl.ds(pl.multiple_of(8 + i * rows, 8), rows)
                zpad[bank, at, :] = v.astype(jnp.float32) * ubuf[bank, tile_at(i), :].astype(jnp.float32)

            return put

        def h_copy(layer):
            return remote(
                halo.at[layer, 0], halo.at[layer, 1], h_send.at[layer], h_recv.at[layer], at_sp(me + q)
            )

        def halo_start(layer):
            halo[layer, 0] = zpad[0, pl.ds(q * rows, 8), :]

            @pl.when(l < line - 1)
            def _():
                h_copy(layer).start()

        def halo_wait(layer):
            zpad[0, 0:8, :] = jnp.zeros((8, width), jnp.float32)

            @pl.when(l > 0)
            def _():
                h_copy(layer).wait_recv()
                zpad[0, 0:8, :] = halo[layer, 1]

        def convolve(layer, bank, tiles):
            at_c = pl.ds(pl.multiple_of(j * width, width), width)
            rates = [taps[k, pl.ds(layer, 1), at_c] for k in range(taps_count)]
            for i in tiles:
                conv = jnp.zeros((rows, width), jnp.float32)
                for k in range(taps_count):
                    first = 8 - (taps_count - 1) + k + i * rows
                    conv = conv + rates[k] * zpad[bank, first:first + rows, :]
                at = pl.ds(i * rows, rows)
                gated[bank, at, :] = (obuf[bank, at, :].astype(jnp.float32) * conv).astype(jnp.bfloat16)


        def fellow():
            return at_sp(me + q * (1 - 2 * lax.rem(l, 2)))

        def n_copy(n):
            h = n % 2
            src = tok.at[part_of(h)] if n < 2 else spot(far, flip(j, 1 + h), h)
            return remote(
                src, spot(far, j if n < 2 else flip(j, 1 + h), h), n_send.at[0], n_recv.at[n], fellow()
            )

        def e_copy(h):
            return remote(
                tok.at[part_of(h)], spot(far, j, h), g_send.at[far], g_recv.at[far, h, h],
                at_sp(peer(1 + h)),
            )

        def k_copy(tile):
            at = tile_at(tile)
            return remote(gated.at[1, at, :], gated.at[0, at, :], k_send.at[0], k_recv.at[tile], fellow())


        odd = lax.rem(j, 2)
        first_tile, second_tile = flip(j, 1), odd * j + (1 - odd) * flip(j, 2)
        third_tile, fourth_tile = flip(j, 3), odd * flip(j, 2) + (1 - odd) * j

        def far_send():
            @outer
            def _():
                for h in range(2):
                    e_copy(h).start()
                for n in range(2):
                    n_copy(n).start()

        def far_pass():
            @outer
            def _():
                for h in range(2):
                    e_copy(h).wait_recv()
                    n_copy(2 + h).start()

        def far_in(h):
            @inner
            def _():
                n_copy(h).wait_recv()
                g_copy(far, 2 - h, h).start()
                cross_start(far, 0, h)

        def far_side():
            @inner
            def _():
                for h in range(2):
                    g_copy(far, 2 - h, h).wait_recv()
                    cross_start(far, 2 - h, h)

        def far_diag():
            @inner
            def _():
                for h in range(2):
                    n_copy(2 + h).wait_recv()
                    g_copy(far, 3, h).start()
                    cross_start(far, 1 + h, h)

        def inner_gather_start(h):
            @inner
            def _():
                gather_start(0, h)

        def inner_pass(rows_set, h):
            @inner
            def _():
                gather_pass(rows_set, h, False)

        def inner_onward(rows_set, h):
            @inner
            def _():
                g_copy(rows_set, 3, h).start()

        def inner_last(rows_set, h):
            @inner
            def _():
                gather_last(rows_set, h)

        def inner_wait(rows_set, rest):
            @inner
            def _():
                gather_wait(rows_set, rest)

        def inner_project(bank, ws, span):
            @inner
            def _():
                for w in ws:
                    project(far if bank else 0, 0, w, (put_u, put_z, put_o)[w](bank), span)

        def inner_arrived(k):
            @inner
            def _():
                arrived(k)

        def own_edge():
            @lower_inner
            def _():
                halo[0, 0] = zpad[0, pl.ds(q * rows, 8), :]
                h_copy(0).start()

        tail = pl.ds(q * rows, 8)

        def far_tiles(early):
            for t in range(q):
                soon = (t == first_tile) | (t == second_tile)

                @pl.when(soon if early else jnp.logical_not(soon))
                def _():
                    convolve(0, 1, (t,))

        def far_early():
            @pl.when((l == 1) | ((l == 2) & (j == 0)))
            def _():
                zpad[1, 0:8, :] = jnp.zeros((8, width), jnp.float32)

            @pl.when((l == 2) & (j > 0))
            def _():
                zpad[1, 0:8, :] = zpad[0, tail, :]

            @inner
            def _():
                far_tiles(True)
                k_copy(first_tile).start()
                k_copy(second_tile).start()

        def far_gates():
            @inner
            def _():
                far_tiles(False)
                k_copy(third_tile).start()

            @pl.when((l == 1) | ((l == 2) & (j > 0)))
            def _():
                k_copy(fourth_tile).start()

        def far_first():
            @pl.when((l == 2) & (j == 0))
            def _():
                zpad[1, 0:8, :] = zpad[0, tail, :]
                convolve(0, 1, (0,))
                k_copy(fourth_tile).start()

        def own_gates():
            @lower_inner
            def _():
                zpad[0, 0:8, :] = zpad[1, tail, :]

            @upper_inner
            def _():
                h_copy(0).wait_recv()
                zpad[0, 0:8, :] = halo[0, 1]

            @inner
            def _():
                convolve(0, 0, range(q))

        def far_sent():
            @outer
            def _():
                take(rows_like(1), g_send.at[far])
                take(rows_like(2), n_send.at[0])

            @inner
            def _():
                gather_sent(0)
                take(rows_like(2), g_send.at[far])
                for r in range(1, tp):
                    take(rows_like(q), t_send.at[far, r - 1])
                take(gated.at[1], k_send.at[0])

            @lower_inner
            def _():
                h_copy(0).wait_send()


        def p_copy(layer, r, i):
            at = tile_at(flip(j, i))
            return remote(
                part.at[layer, lax.rem(c + r, tp), at, :], rec1.at[layer, r - 1, at, :],
                p_send.at[layer, r - 1], p_recv.at[layer, r - 1, i], at_tp(r),
            )


        bit_rows = half_rows // 2

        def bit_of(h, e):
            return pl.ds(h * half_rows + e * bit_rows, bit_rows)

        def r_copy(layer, i, h):
            at = part_of(h)
            return remote(
                snd2.at[layer, i, at, :], rec2.at[layer, i, at, :],
                r_send.at[layer], r_recv.at[layer, i - 1], at_sp(peer(i)),
            )

        def w_copy(layer, h, e):
            at = bit_of(h, e)
            return remote(
                snd2.at[layer, 2 - h, at, :], rec2.at[layer, 2 - h, at, :],
                r_send.at[layer], w_recv.at[layer, h, e], at_sp(peer(2 - h)),
            )

        def v_copy(layer, h, e):
            at = bit_of(h, e)
            return remote(
                snd2.at[layer, 3, at, :], rec2.at[layer, 3, at, :],
                r_send.at[layer], v_recv.at[layer, h, e], at_sp(peer(1 + h)),
            )

        def reduce_tile(layer, i):
            at = tile_at(flip(j, i))
            total = part[layer, c, at, :].astype(jnp.float32)
            for r in range(1, tp):
                p_copy(layer, r, i).wait_recv()
                total = total + rec1[layer, r - 1, at, :].astype(jnp.float32)
            if i == 0:
                acc[...] = total
                return
            snd2[layer, i] = total.astype(jnp.bfloat16)
            if i == 3:
                for e in range(2):
                    for h in range(2):
                        v_copy(layer, h, e).start()
            elif halves == 1:
                r_copy(layer, i, 0).start()
            elif i == 1:
                r_copy(layer, 1, 0).start()

        def relay(layer, h, e):
            if halves == 2:
                v_copy(layer, h, e).wait_recv()
                i, at = 2 - h, bit_of(h, e)
                snd2[layer, i, at, :] = (
                    snd2[layer, i, at, :].astype(jnp.float32) + rec2[layer, 3, at, :].astype(jnp.float32)
                ).astype(jnp.bfloat16)
                w_copy(layer, h, e).start()
                if h == 0 and e == 1:
                    r_copy(layer, 2, 1).start()

        def out_product(layer):
            for i in range(q - 1, -1, -1):
                at = tile_at(flip(j, i))

                def half(n, carry):
                    cc = lax.rem(c + 1 + n, tp)
                    weight = jnp.concatenate([wout[layer, cc * per_half + b] for b in range(per_half)], axis=1)
                    part[layer, cc, at, :] = jnp.dot(
                        gated[0, at, :], weight, preferred_element_type=jnp.float32
                    ).astype(jnp.bfloat16)
                    return carry

                lax.fori_loop(0, tp, half, 0)
                for r in range(1, tp):
                    p_copy(layer, r, i).start()
                if i < q - 1:
                    reduce_tile(layer, i + 1)
            reduce_tile(layer, 0)


        def late_half():
            return (l < line // 2).astype(jnp.int32)

        def half_tile(second, i):
            cc = late_half() if second else 1 - late_half()
            weight = jnp.concatenate([wout[0, cc * per_half + b] for b in range(per_half)], axis=1)
            at = tile_at(flip(j, i))
            if not second:
                @outer
                def _():
                    k_copy(flip(j, i)).wait_recv()

            part[0, cc, at, :] = jnp.dot(
                gated[0, at, :], weight, preferred_element_type=jnp.float32
            ).astype(jnp.bfloat16)

            @pl.when(cc != c)
            def _():
                p_copy(0, 1, i).start()

        def half_sum(second, i):
            @pl.when((late_half() == c) if second else (late_half() != c))
            def _():
                reduce_tile(0, i)

        def inner_late_tile(i):
            @inner
            def _():
                half_tile(True, i)

        def inner_late_sum(i):
            @inner
            def _():
                half_sum(True, i)

        def outer_late_tile(i):
            @outer
            def _():
                half_tile(True, i)

        def outer_late_sum(i):
            @outer
            def _():
                half_sum(True, i)

        def half_relay(second, h, e):
            @pl.when((late_half() == c) if second else (late_half() != c))
            def _():
                relay(0, h, e)


        last = layers - 1

        def nth_block(n):
            upper = (l >= line // 2).astype(jnp.int32)
            inner = ((l > 0) & (l < line - 1)).astype(jnp.int32)
            b = n
            if n < 2:
                b = n + inner * (1 - 2 * n)
            return b + upper * (line - 1 - 2 * b)

        def cols_of(m):
            return pl.ds(pl.multiple_of(m * block_cols, block_cols), block_cols)

        def q_copy(n, i):
            b = nth_block(n)
            m = lax.rem(b, slots)
            at = tile_at(flip(j, i))
            return remote(
                part.at[last, lax.div(b, slots), at, cols_of(m)], rec1.at[last, 0, at, cols_of(m)],
                p_send.at[last, 0], p_recv.at[last, m, i], at_tp(1),
            )

        def b_copy(m, i, h):
            at = part_of(h)
            return remote(
                snd2.at[last, i, at, cols_of(m)], rec2.at[last, i, at, cols_of(m)],
                b_send.at[0], b_recv.at[m, i - 1, h], at_sp(peer(i if i < 3 else 1 + h)),
            )

        def block_product(n):
            b = nth_block(n)
            m = lax.rem(b, slots)
            own = lax.div(b, slots) == c
            weight = jnp.concatenate([wout[last, b * q + e] for e in range(q)], axis=1)
            for i in range(q - 1, -1, -1):
                at = tile_at(flip(j, i))
                part[last, lax.div(b, slots), at, cols_of(m)] = jnp.dot(
                    gated[0, at, :], weight, preferred_element_type=jnp.float32
                ).astype(jnp.bfloat16)

                @pl.when(jnp.logical_not(own))
                def _():
                    q_copy(n, i).start()

        def block_sum(n):
            b = nth_block(n)
            m = lax.rem(b, slots)

            @pl.when(lax.div(b, slots) == c)
            def _():
                for i in range(q - 1, -1, -1):
                    at = tile_at(flip(j, i))
                    q_copy(n, i).wait_recv()
                    total = part[last, c, at, cols_of(m)].astype(jnp.float32)
                    total = total + rec1[last, 0, at, cols_of(m)].astype(jnp.float32)
                    if i == 0:
                        acc[:, cols_of(m)] = total
                        continue
                    snd2[last, i, :, cols_of(m)] = total.astype(jnp.bfloat16)
                    if i == 3:
                        b_copy(m, 3, 0).start()
                        b_copy(m, 3, 1).start()
                    elif i == 1:
                        b_copy(m, 1, 0).start()

        def block_relay(n):
            b = nth_block(n)
            m = lax.rem(b, slots)

            @pl.when(lax.div(b, slots) == c)
            def _():
                for h in range(2):
                    b_copy(m, 3, h).wait_recv()
                    i, at = 2 - h, part_of(h)
                    snd2[last, i, at, cols_of(m)] = (
                        snd2[last, i, at, cols_of(m)].astype(jnp.float32)
                        + rec2[last, 3, at, cols_of(m)].astype(jnp.float32)
                    ).astype(jnp.bfloat16)
                    b_copy(m, i, h).start()
                    if h == 0:
                        b_copy(m, 2, 1).start()

        def sums_sent(layer):
            for r in range(1, tp):
                take(part.at[layer, 0], p_send.at[layer, r - 1])
                take(stat.at[layer], s_send.at[layer, r - 1])
            if q > 1:
                take(snd2.at[layer, pl.ds(0, q - 1)], b_send.at[0] if timed and layer == last else r_send.at[layer])

        def s_copy(layer, r, h):
            return remote(
                stat.at[layer, h], stat_in.at[layer, r, h], s_send.at[layer, r - 1], s_recv.at[layer, r - 1, h], at_tp(r)
            )

        def finish(layer, h):
            at = part_of(h)
            pre = alpha * mine(layer, h)[...].astype(jnp.float32) + acc[at, :]
            for i in range(1, min(q, 3)):
                if timed and layer == last:
                    for m in range(slots):
                        b_copy(m, i, h).wait_recv()
                elif halves == 2 and i == 2 - h:
                    for e in range(2):
                        w_copy(layer, h, e).wait_recv()
                else:
                    r_copy(layer, i, h).wait_recv()
                pre = pre + rec2[layer, i, at, :].astype(jnp.float32)
            acc[at, :] = pre
            own = jnp.sum(pre, axis=-1, keepdims=True)
            away = pre - own * (1.0 / feats)
            spread = jnp.sum(away * away, axis=-1, keepdims=True)
            lane = lax.broadcasted_iota(jnp.int32, (half_rows, LANES), 1)
            stat[layer, h] = jnp.where(lane == 0, own, spread)
            for r in range(1, tp):
                s_copy(layer, r, h).start()
            sums, spreads = [own], [spread]
            for r in range(1, tp):
                s_copy(layer, r, h).wait_recv()
                sums.append(stat_in[layer, r, h, :, 0:1])
                spreads.append(stat_in[layer, r, h, :, 1:2])
            mean = sum(sums[1:], sums[0]) * (1.0 / model)
            var = sum(spreads[1:], spreads[0])
            for s in sums:
                off = s * (1.0 / feats) - mean
                var = var + feats * off * off
            scale = lax.rsqrt(var * (1.0 / model) + EPS)
            normed = (acc[at, :] - mean) * scale
            y = (normed * gain[pl.ds(layer, 1), :] + bias[pl.ds(layer, 1), :]).astype(jnp.bfloat16)
            if layer == last:
                res[at, :] = y
            else:
                mine(layer + 1, h)[...] = y


        tasks = []

        def at_time(when, fn, *args):
            tasks.append((when, len(tasks), fn, args))

        def first_half(layer, w0, w1, w2):
            def start():
                gather_wait(layer, False)
                if q > 3:
                    gather_wait(layer, True)
                arrived(layer * 4)
                project(layer, layer, 0, put_u(0), ALL)

            def middle():
                arrived(layer * 4 + 1)
                project(layer, layer, 1, put_z(0), ALL)
                halo_start(layer)

            def gates():
                arrived(layer * 4 + 2)
                project(layer, layer, 2, put_o(0), ALL)
                halo_wait(layer)
                convolve(layer, 0, range(q))
                halo_sent(layer)

            at_time(w0, start)
            at_time(w1, middle)
            at_time(w2, gates)

        def most_of(layer, ws):
            for w in ws:
                arrived(layer * 4 + w)
                project(layer, layer, w, (put_u, put_z, put_o)[w](0), MOST)

        def rest_of(layer):
            gather_wait(layer, True)
            project(layer, layer, 0, put_u(0), REST)
            project(layer, layer, 1, put_z(0), REST)
            halo_start(layer)

        def gates_of(layer):
            project(layer, layer, 2, put_o(0), REST)
            halo_wait(layer)
            convolve(layer, 0, range(q))

        def halo_sent(layer):
            @pl.when(l < line - 1)
            def _():
                h_copy(layer).wait_send()

        def second_half(layer, when):
            def go():
                arrived(layer * 4 + 3)
                out_product(layer)

            at_time(when, go)

        if timed:
            at_time(-1.0, far_send)
            for when, k in ((0.0, 0), (0.1, 1), (0.2, 3), (0.3, 4), (0.5, 2), (0.6, 5), (0.7, 6), (0.8, 7)):
                at_time(when, scatter_start, k)
            for h in range(halves):
                at_time(0.4, inner_gather_start, h)
                at_time((8.6, 13.6)[h], far_in, h)
                at_time((20.0, 26.0)[h], inner_pass, 0, h)
                at_time(42.55 + 0.01 * h, inner_onward, 0, h)
                at_time(53.19 + 0.001 * h, inner_last, 0, h)
                at_time(51.0 + 0.05 * h, inner_last, far, h)
            at_time(15.1, far_pass)
            at_time(43.1, far_side)
            at_time(42.5, far_diag)
            for k, when in enumerate((3.5, 6.5, 15.0, 15.2, 15.3, 18.0, 22.0, 24.0)):
                at_time(when, outer_begin, k)
            for k, when in enumerate((3.5, 6.5, 27.5, 9.5, 12.5, 30.0, 38.0, 41.0)):
                at_time(when, inner_ready, k)
            for k, when in enumerate((3.6, 6.6, 27.6, 9.6, 43.2, 57.1, 61.92, 66.2)):
                at_time(when, inward, k, 0)
            for k, when in enumerate((19.0, 25.0, 31.0, 51.5, 57.0, 61.9, 66.1, 67.6)):
                at_time(when, inward, k, 1)
            for k, when in enumerate((9.7, 12.6, 30.1, 38.1, 41.1)):
                at_time(when, outward, k + 3, 0)
            for k, when in enumerate((23.5, 61.91, 67.5, 79.0, 87.1)):
                at_time(when, outward, k + 3, 1)
            for k, when in enumerate((54.2, 66.0, 72.5, 82.0)):
                at_time(when, outward, k + 3, 2)
            at_time(33.1, inner_wait, 0, False)
            at_time(33.1, inner_arrived, 0)
            at_time(33.2, inner_project, 0, (0,), MOST)
            at_time(37.0, inner_arrived, 1)
            at_time(37.0, inner_project, 0, (1,), MOST)
            at_time(43.5, inner_wait, far, False)
            at_time(43.6, inner_project, 1, (0, 1), MOST)
            at_time(45.5, inner_arrived, 2)
            at_time(45.6, inner_project, 1, (2,), MOST)
            at_time(45.7, far_early)
            at_time(52.0, inner_wait, far, True)
            at_time(52.1, inner_project, 1, (0, 1, 2), REST)
            at_time(53.1, far_gates)
            at_time(53.18, inner_project, 0, (2,), MOST)
            at_time(53.2, inner_wait, 0, True)
            at_time(53.21, inner_project, 0, (0, 1), REST)
            at_time(53.22, own_edge)
            at_time(53.23, far_first)
            at_time(54.21, inner_project, 0, (2,), REST)
            at_time(55.3, own_gates)
            o = 58.0
            at_time(o, line_end, 3, 0)
            for n, i in enumerate((1, 3, 2, 0)):
                at_time(o + 0.1 * n, half_tile, False, i)
                at_time(o + 0.1 * n + 0.15, half_sum, False, i)
            for e in range(2):
                for h in range(2):
                    at_time(o + 8.5 + 0.1 * e + 0.01 * h, half_relay, False, h, e)
            at_time(o + 8.75, line_end, 3, 1)
            at_time(o + 8.75, line_end, 3, 2)
            for n, i in enumerate((3, 2, 1, 0)):
                at_time(o + 4.3 + 0.1 * n, inner_late_tile, i)
                at_time(o + 4.3 + 0.1 * n + 0.15, inner_late_sum, i)
                at_time(o + 8.8 + 0.01 * n, outer_late_tile, i)
                at_time(o + 8.8 + 0.01 * n + 0.015, outer_late_sum, i)
            for e in range(2):
                for h in range(2):
                    at_time(o + 9.0 + 0.1 * e + 0.01 * h, half_relay, True, h, e)
            for h in range(halves):
                f = o + 14.0 + 6.0 * h
                at_time(f, finish, 0, h)
                at_time(f + 0.1, gather_start, 1, h)
                at_time(f + 9.0, gather_pass, 1, h)
                at_time(93.0 + 0.1 * h, gather_last, 1, h)
            at_time(88.0, gather_wait, 1, False)
            at_time(88.1, most_of, 1, (0, 1))
            at_time(93.2, rest_of, 1)
            at_time(93.4, most_of, 1, (2,))
            at_time(93.5, outward, units - 1, 2)
            at_time(94.0, gates_of, 1)
            at_time(128.0, halo_sent, 1)
            for n in range(1, line):
                at_time((110.0, 110.1, 111.0, 113.0)[n], line_end, units - 1, n - 1)
            for n in range(line):
                at_time((110.0, 110.2, 111.0, 113.0)[n], block_product, n)
                at_time((110.3, 110.4, 111.1, 113.5)[n], block_sum, n)
                at_time((113.1, 113.2, 114.0, 114.1)[n], block_relay, n)
            at_time(127.5, far_sent)
            at_time(128.0, gather_sent, 1)
            at_time(128.1, sums_sent, 0)
            for k in range(units):
                at_time(129.5, all_sent, k)
            for h in range(halves):
                at_time(130.0 + h, finish, last, h)
            at_time(140.0, sums_sent, last)
        else:
            for k in range(units):
                at_time(-2.0 if k < 2 else -1.0, scatter_start, k)
            for h in range(halves):
                at_time(-1.5, gather_start, 0, h)
            begin = [k + k // 4 for k in range(units)]
            for k in range(units):
                at_time(begin[k], line_begin, k)
                for s in range(1, steps):
                    at_time(begin[k] + s, line_pass, k, s)
            end = begin[-1] + max(steps, 1) + 1
            ready = [begin[k] + steps for k in range(units)]
            for layer in range(layers):
                if layer == 0:
                    base = ready[0] + 0.5
                else:
                    base = max(ready[4 * layer - 1] + 4.0, end if layer > 1 else 0) + 0.5
                for h in range(halves):
                    at_time(base - 1.3, gather_pass, layer, h)
                    at_time(base - 1.2, gather_last, layer, h)
                w1 = max(base + 0.1, ready[4 * layer + 1] + 0.5)
                w2 = max(w1 + 0.1, ready[4 * layer + 2] + 0.5)
                first_half(layer, base, w1, w2)
                o = max(w2 + 0.1, ready[4 * layer + 3] + 0.5)
                second_half(layer, o)
                for e in range(2):
                    for h in range(2):
                        at_time(o + 0.1, relay, layer, h, e)
                for h in range(halves):
                    at_time(o + 0.3, finish, layer, h)
                    if layer < last:
                        at_time(o + 0.4, gather_start, layer + 1, h)

        for _, _, fn, args in sorted(tasks, key=lambda task: task[:2]):
            fn(*args)
        if not timed:
            for layer in range(layers):
                gather_sent(layer)
                sums_sent(layer)
            for k in range(units):
                scatter_sent(k)
                for s in range(steps):
                    line_sent(k, s)

    return kernel


def solution(mesh):
    sp, tp = mesh.shape["sp"], mesh.shape["tp"]

    def shards(tokens, value_weight, outer_weight, inner_weight, conv_taps, output_weight, norm_gain, norm_bias):
        rows, feats = tokens.shape
        layers, depth, channels = value_weight.shape
        taps_count = conv_taps.shape[1]
        q = plane_size(sp, channels)
        width = channels // q
        line = sp // q
        model = feats * tp
        alpha = (2.0 * layers) ** 0.25
        out_cols = output_weight.shape[2]
        bf, f32 = jnp.bfloat16, jnp.float32
        kernel = make_kernel(sp, tp, q, layers, taps_count, rows, feats, depth, width, out_cols, alpha)
        dma = pltpu.SemaphoreType.DMA
        units, steps = 4 * layers, max(line - 1, 1)
        others = max(tp - 1, 1)
        banks = 2 if helped(line, q, tp, layers) else 1
        sets = layers + banks - 1
        relays = 1 if banks == 2 else layers
        if banks == 2:
            lines = [dma((units,)), dma((units, steps)), dma((1,)), dma((1,))]
        else:
            lines = [dma((units, steps))] * 4
        halves = 2 if q == 4 else 1
        half_rows = rows // halves
        vm = pl.BlockSpec(memory_space=pltpu.VMEM)
        return pl.pallas_call(
            kernel,
            out_shape=jax.ShapeDtypeStruct((rows, feats), bf),
            in_specs=[vm] * 8,
            out_specs=vm,
            scratch_shapes=[
                pltpu.VMEM((layers + banks - 1, tp, q * rows, feats), bf),
                pltpu.VMEM((layers, 3, model, width), bf),
                pltpu.VMEM((layers, sp, width, out_cols), bf),
                pltpu.VMEM((banks, q * rows, width), bf),
                pltpu.VMEM((banks, q * rows, width), bf),
                pltpu.VMEM((banks, q * rows + 8, width), f32),
                pltpu.VMEM((banks, q * rows, width), bf),
                pltpu.VMEM((layers, tp, q * rows, feats), bf),
                pltpu.VMEM((layers, others, q * rows, feats), bf),
                pltpu.VMEM((layers, q, rows, feats), bf),
                pltpu.VMEM((layers, q, rows, feats), bf),
                pltpu.VMEM((rows, feats), f32),
                pltpu.VMEM((layers, halves, half_rows, LANES), f32),
                pltpu.VMEM((layers, tp, halves, half_rows, LANES), f32),
                pltpu.VMEM((layers, 2, 8, width), f32),
                dma((units,)), dma((units,)), *lines,
                dma((sets,)), dma((sets, 3, halves)), dma((1,)),
                dma((sets, others)), dma((sets, others, 2)),
                dma((layers, others)), dma((layers, max(others, 2), q)),
                dma((layers,)), dma((layers, 2)),
                dma((layers, others)), dma((layers, others, halves)),
                dma((layers,)), dma((layers,)),
                dma((1,)), dma((2, 3, 2)), dma((1,)), dma((4,)), dma((1,)), dma((4,)),
                dma((relays, 2, 2)), dma((relays, 2, 2)), dma((2,)),
            ],
            compiler_params=pltpu.CompilerParams(
                collective_id=0, has_side_effects=True, vmem_limit_bytes=60 * 1024 * 1024
            ),
        )(tokens, value_weight, outer_weight, inner_weight, jnp.swapaxes(conv_taps, 0, 1), output_weight, norm_gain, norm_bias)

    in_specs = (
        P("sp", "tp"),
        P(None, "sp", "tp"),
        P(None, "sp", "tp"),
        P(None, "sp", "tp"),
        P(None, None, "tp"),
        P(None, "tp", "sp"),
        P(None, "tp"),
        P(None, "tp"),
    )
    return jax.shard_map(shards, mesh=mesh, in_specs=in_specs, out_specs=P("sp", "tp"), check_vma=False)
```

```python
import jax
import jax.numpy as jnp
from jax import lax
from jax.experimental import pallas as pl
from jax.experimental.pallas import tpu as pltpu
from jax.sharding import PartitionSpec as P

LANES = 128
EPS = 1e-5


def flip(j, i):
    if i & 1:
        j = j + 1 - 2 * lax.rem(j, 2)
    if i & 2:
        j = j + 2 - 4 * lax.rem(lax.div(j, 2), 2)
    return j


def plane_size(sp, channels):
    q = 4
    while q > 1 and (sp % q or channels // q < LANES or channels % q):
        q //= 2
    return q


def helped(line, q, tp, layers):
    return line == 4 and q == 4 and tp == 2 and layers == 2


def make_kernel(sp, tp, q, layers, taps_count, rows, feats, depth, width, out_cols, alpha):
    line = sp // q
    units = layers * 4
    model = feats * tp
    per_half = sp // tp
    steps = line - 1
    halves = 2 if q == 4 else 1
    half_rows = rows // halves
    timed = helped(line, q, tp, layers)
    slots = line // tp if timed else 1
    block_cols = q * out_cols

    def kernel(
        tok_in, val_in, outw_in, inn_in, taps, prj_in, gain, bias, res,
        xg, win, wout, ubuf, obuf, zpad, gated, part, rec1, snd2, rec2, acc, stat, stat_in, halo,
        a_send, a_recv, u_send, u_recv, d_send, d_recv,
        g_send, g_recv, g_loc, t_send, t_recv, p_send, p_recv, r_send, r_recv, s_send, s_recv, h_send, h_recv,
        b_send, b_recv, n_send, n_recv, k_send, k_recv,
        v_recv, w_recv, e_recv, tok, val, outw, inn, prj, in_sem,
    ):
        me = lax.axis_index("sp")
        c = lax.axis_index("tp")
        l = lax.div(me, q)
        j = lax.rem(me, q)

        def at_sp(other):
            return {"sp": other, "tp": c}

        def at_tp(r):
            return {"sp": me, "tp": lax.rem(c + r, tp)}

        def remote(src, dst, ssem, rsem, dev):
            return pltpu.make_async_remote_copy(
                src_ref=src, dst_ref=dst, send_sem=ssem, recv_sem=rsem,
                device_id=dev, device_id_type=pl.DeviceIdType.MESH,
            )

        def peer(i):
            return l * q + flip(j, i)

        loads = [
            pltpu.make_async_copy(src, dst, in_sem.at[n])
            for n, (src, dst) in enumerate(
                ((tok_in, tok), (val_in, val), (inn_in, inn), (prj_in, prj), (outw_in, outw))
            )
        ]
        for load in loads:
            load.start()

        barrier = pltpu.get_barrier_semaphore()

        def greet(dev):
            pl.semaphore_signal(barrier, inc=1, device_id=dev, device_id_type=pl.DeviceIdType.MESH)

        for i in range(1, q):
            greet(at_sp(peer(i)))
        for r in range(1, tp):
            greet(at_tp(r))

        @pl.when(l > 0)
        def _():
            greet(at_sp(me - q))

        @pl.when(l < line - 1)
        def _():
            greet(at_sp(me + q))

        neighbours = (l > 0).astype(jnp.int32) + (l < line - 1).astype(jnp.int32)
        pl.semaphore_wait(barrier, (q - 1) + (tp - 1) + neighbours)
        for load in loads:
            load.wait()


        ORDER = (val, inn, outw, prj)

        def own_piece(k, jd):
            layer, w = divmod(k, 4)
            at = pl.ds(pl.multiple_of(jd * width, width), width)
            if w == 3:
                return prj.at[layer, at, :]
            return ORDER[w].at[layer, :, at]

        def landed(k, s):
            layer, w = divmod(k, 4)
            if w == 3:
                return wout.at[layer, s]
            return win.at[layer, w, pl.ds(pl.multiple_of(s * depth, depth), depth), :]

        def block(k, b):
            layer, w = divmod(k, 4)
            if w == 3:
                return wout.at[layer, pl.ds(b * q, q)]
            return win.at[layer, w, pl.ds(pl.multiple_of(b * (q * depth), q * depth), q * depth), :]

        def a_copy(k, i):
            return remote(own_piece(k, flip(j, i)), landed(k, me), a_send.at[k], a_recv.at[k], at_sp(peer(i)))

        def a_local(k):
            return pltpu.make_async_copy(own_piece(k, j), landed(k, me), a_recv.at[k])

        def scatter_start(k):
            a_local(k).start()
            for i in range(q - 1, 0, -1):
                a_copy(k, i).start()


        def take(ref, sem):
            pltpu.make_async_copy(ref, ref, sem).wait()

        def scatter_wait(k):
            take(block(k, l), a_recv.at[k])

        def scatter_sent(k):
            layer, w = divmod(k, 4)
            if q > 1:
                n = q - 1
                take(wout.at[layer, pl.ds(0, n)] if w == 3 else win.at[layer, w, pl.ds(0, n * depth), :], a_send.at[k])

        def up(k, s):
            sems = (u_send.at[k], u_recv.at[k, s]) if timed else (u_send.at[k, s], u_recv.at[k, s])
            return remote(block(k, l - s), block(k, l - s), *sems, at_sp(me + q))

        def down(k, s):
            sems = (u_send.at[k], u_recv.at[k, steps - 1 - s]) if timed else (d_send.at[k, s], d_recv.at[k, s])
            return remote(block(k, l + s), block(k, l + s), *sems, at_sp(me - q))

        def line_begin(k):
            scatter_wait(k)

            @pl.when(l < line - 1)
            def _():
                up(k, 0).start()

            @pl.when(l > 0)
            def _():
                down(k, 0).start()

        def line_pass(k, s):
            @pl.when((l - s >= 0) & (l < line - 1))
            def _():
                up(k, s - 1).wait_recv()
                up(k, s).start()

            @pl.when((l + s < line) & (l > 0))
            def _():
                down(k, s - 1).wait_recv()
                down(k, s).start()


        def lower_inner(fn):
            pl.when(l == 1)(fn)

        def upper_inner(fn):
            pl.when(l == 2)(fn)

        def outer(fn):
            pl.when((l == 0) | (l == 3))(fn)

        def inner(fn):
            pl.when((l == 1) | (l == 2))(fn)

        def outer_begin(k):
            @pl.when(l == 0)
            def _():
                scatter_wait(k)
                up(k, 0).start()

            @pl.when(l == 3)
            def _():
                scatter_wait(k)
                down(k, 0).start()

        def inner_ready(k):
            @inner
            def _():
                scatter_wait(k)

        def inward(k, s):
            @lower_inner
            def _():
                if s:
                    up(k, s - 1).wait_recv()
                up(k, s).start()

            @upper_inner
            def _():
                if s:
                    down(k, s - 1).wait_recv()
                down(k, s).start()

        def outward(k, s):
            @lower_inner
            def _():
                if s:
                    down(k, s - 1).wait_recv()
                down(k, s).start()

            @upper_inner
            def _():
                if s:
                    up(k, s - 1).wait_recv()
                up(k, s).start()

        def ends(k):
            return (1, line - 2) if timed and k < 3 else (0, line - 1)

        def line_end(k, s):
            low, high = ends(k)

            @pl.when((l == high) & (l - 1 - s >= 0))
            def _():
                up(k, s).wait_recv()

            @pl.when((l == low) & (l + 1 + s < line))
            def _():
                down(k, s).wait_recv()

        def arrived(k):
            for s in range(steps):
                line_end(k, s)

        def line_sent(k, s):
            @pl.when((l - s >= 0) & (l < line - 1))
            def _():
                up(k, s).wait_send()

            @pl.when((l + s < line) & (l > 0))
            def _():
                down(k, s).wait_send()

        def all_sent(k):
            each = q * depth * width // feats
            scatter_sent(k)

            @outer
            def _():
                take(xg.at[0, 0, pl.ds(0, each), :], u_send.at[k])

            @inner
            def _():
                take(xg.at[0, 0, pl.ds(0, (2 if k < 3 else 5) * each), :], u_send.at[k])


        def part_of(h):
            return pl.ds(h * half_rows, half_rows)

        def spot(layer, jj, h):
            at = pl.ds(pl.multiple_of(jj * rows + h * half_rows, half_rows), half_rows)
            return xg.at[layer, c, at, :]

        def mine(layer, h):
            return tok.at[part_of(h)] if layer == 0 else spot(layer, j, h)

        def g_copy(layer, i, h):
            if i == 3:
                src = spot(layer, flip(j, 1 + h), h)
                return remote(src, src, g_send.at[layer], g_recv.at[layer, i - 1, h], at_sp(peer(2 - h)))
            return remote(
                mine(layer, h), spot(layer, j, h), g_send.at[layer], g_recv.at[layer, i - 1, h], at_sp(peer(i))
            )

        def g_piece(i, e):
            first = (j if i == 2 else flip(j, 2)) * rows + half_rows + e * (half_rows // 2)
            src = xg.at[1, c, pl.ds(pl.multiple_of(first, half_rows // 2), half_rows // 2), :]
            got = e_recv.at[e] if i == 2 else g_recv.at[1, 2, 1]
            return remote(src, src, g_send.at[1], got, at_sp(peer(2 if i == 2 else 1)))

        def g_local(h):
            return pltpu.make_async_copy(tok.at[part_of(h)], spot(0, j, h), g_loc.at[0])

        def rows_like(n):
            return xg.at[0, 0, pl.ds(0, n * rows), :]

        def kind(layer, i):
            return 1 if i == 3 else 2 if i == 0 and timed and layer else 0

        def t_copy(layer, r, i, h):
            src = mine(layer, h) if i == 0 else spot(layer, flip(j, i), h)
            return remote(
                src, spot(layer, flip(j, i), h), t_send.at[layer, r - 1], t_recv.at[layer, r - 1, kind(layer, i)], at_tp(r)
            )

        def cross_start(layer, i, h):
            for r in range(1, tp):
                t_copy(layer, r, i, h).start()

        def gather_start(layer, h):
            if layer == 0:
                g_local(h).start()
            for i in range(1, min(q, 3)):
                if timed and layer == 1 and i == 2 and h == 1:
                    for e in range(2):
                        g_piece(2, e).start()
                else:
                    g_copy(layer, i, h).start()
            cross_start(layer, 0, h)

        def gather_pass(layer, h, onward=True):
            first = 1 + h if q == 4 else 1
            for i in range(1, min(q, 3)):
                i = first if i == 1 else 3 - first
                if timed and layer == 1 and i == 2 and h == 1:
                    for e in range(2):
                        g_piece(2, e).wait_recv()
                        g_piece(3, e).start()
                else:
                    g_copy(layer, i, h).wait_recv()
                    if q == 4 and i == first and onward:
                        g_copy(layer, 3, h).start()
                cross_start(layer, i, h)

        def gather_last(layer, h):
            if q == 4:
                g_copy(layer, 3, h).wait_recv()
                cross_start(layer, 3, h)

        def gather_wait(layer, rest):
            for r in range(1, tp):
                n = 1 if rest else 2 if timed and layer else min(q, 3)
                take(rows_like(n), t_recv.at[layer, r - 1, 1 if rest else 0])
            if layer == 0 and not rest:
                take(rows_like(1), g_loc.at[0])

        def gather_own(layer):
            for r in range(1, tp):
                take(rows_like(1), t_recv.at[layer, r - 1, 2])

        def gather_sent(layer):
            if q > 1:
                take(rows_like(q - 1), g_send.at[layer])
            for r in range(1, tp):
                take(rows_like(q), t_send.at[layer, r - 1])

        def tile_at(jj):
            return pl.ds(pl.multiple_of(jj * rows, rows), rows)


        far = layers
        ALL, MOST, REST, OWN, SIDE = (0, q), (1, q - 1), (0, 1), (0, 1, 0), (0, 2, 0)

        def project(rows_set, layer, w, store, span):
            first = flip(j, q - 1) if span is not ALL else 0

            def tile(n, carry):
                if span is OWN:
                    i = j
                elif span is SIDE:
                    i = flip(j, 1) + n * (flip(j, 2) - flip(j, 1))
                else:
                    i = lax.rem(first + span[0] + n, q)
                at = tile_at(i)
                total = jnp.zeros((rows, width), jnp.float32)
                for cc in range(tp):
                    total = total + jnp.dot(
                        xg[rows_set, cc, at, :],
                        win[layer, w, pl.ds(cc * feats, feats), :],
                        preferred_element_type=jnp.float32,
                    )
                store(i, total.astype(jnp.bfloat16))
                return carry

            lax.fori_loop(0, span[1], tile, 0)

        def put_u(bank):
            def put(i, v):
                ubuf[bank, tile_at(i), :] = v

            return put

        def put_o(bank):
            def put(i, v):
                obuf[bank, tile_at(i), :] = v

            return put

        def put_z(bank):
            def put(i, v):
                at = pl.ds(pl.multiple_of(8 + i * rows, 8), rows)
                zpad[bank, at, :] = v.astype(jnp.float32) * ubuf[bank, tile_at(i), :].astype(jnp.float32)

            return put

        def h_copy(layer):
            return remote(
                halo.at[layer, 0], halo.at[layer, 1], h_send.at[layer], h_recv.at[layer], at_sp(me + q)
            )

        def halo_start(layer):
            halo[layer, 0] = zpad[0, pl.ds(q * rows, 8), :]

            @pl.when(l < line - 1)
            def _():
                h_copy(layer).start()

        def halo_wait(layer):
            zpad[0, 0:8, :] = jnp.zeros((8, width), jnp.float32)

            @pl.when(l > 0)
            def _():
                h_copy(layer).wait_recv()
                zpad[0, 0:8, :] = halo[layer, 1]

        def convolve(layer, bank, tiles):
            at_c = pl.ds(pl.multiple_of(j * width, width), width)
            rates = [taps[k, pl.ds(layer, 1), at_c] for k in range(taps_count)]
            for i in tiles:
                conv = jnp.zeros((rows, width), jnp.float32)
                for k in range(taps_count):
                    first = 8 - (taps_count - 1) + k + i * rows
                    conv = conv + rates[k] * zpad[bank, first:first + rows, :]
                at = pl.ds(i * rows, rows)
                gated[bank, at, :] = (obuf[bank, at, :].astype(jnp.float32) * conv).astype(jnp.bfloat16)


        def fellow():
            return at_sp(me + q * (1 - 2 * lax.rem(l, 2)))

        def n_copy(n):
            h = n % 2
            src = tok.at[part_of(h)] if n < 2 else spot(far, flip(j, 1 + h), h)
            return remote(
                src, spot(far, j if n < 2 else flip(j, 1 + h), h), n_send.at[0], n_recv.at[n], fellow()
            )

        def e_copy(h):
            return remote(
                tok.at[part_of(h)], spot(far, j, h), g_send.at[far], g_recv.at[far, h, h],
                at_sp(peer(1 + h)),
            )

        def k_copy(tile):
            at = tile_at(tile)
            return remote(gated.at[1, at, :], gated.at[0, at, :], k_send.at[0], k_recv.at[tile], fellow())


        odd = lax.rem(j, 2)
        first_tile, second_tile = flip(j, 1), odd * j + (1 - odd) * flip(j, 2)
        third_tile, fourth_tile = flip(j, 3), odd * flip(j, 2) + (1 - odd) * j

        def far_send():
            @outer
            def _():
                for h in range(2):
                    e_copy(h).start()
                for n in range(2):
                    n_copy(n).start()

        def far_pass():
            @outer
            def _():
                for h in range(2):
                    e_copy(h).wait_recv()
                    n_copy(2 + h).start()

        def far_in(h):
            @inner
            def _():
                n_copy(h).wait_recv()
                g_copy(far, 2 - h, h).start()
                cross_start(far, 0, h)

        def far_side():
            @inner
            def _():
                for h in range(2):
                    g_copy(far, 2 - h, h).wait_recv()
                    cross_start(far, 2 - h, h)

        def far_diag():
            @inner
            def _():
                for h in range(2):
                    n_copy(2 + h).wait_recv()
                    g_copy(far, 3, h).start()
                    cross_start(far, 1 + h, h)

        def inner_gather_start(h):
            @inner
            def _():
                gather_start(0, h)

        def inner_pass(rows_set, h):
            @inner
            def _():
                gather_pass(rows_set, h, False)

        def inner_onward(rows_set, h):
            @inner
            def _():
                g_copy(rows_set, 3, h).start()

        def inner_last(rows_set, h):
            @inner
            def _():
                gather_last(rows_set, h)

        def inner_wait(rows_set, rest):
            @inner
            def _():
                gather_wait(rows_set, rest)

        def inner_project(bank, ws, span):
            @inner
            def _():
                for w in ws:
                    project(far if bank else 0, 0, w, (put_u, put_z, put_o)[w](bank), span)

        def inner_own():
            @inner
            def _():
                gather_own(far)

        def inner_arrived(k):
            @inner
            def _():
                arrived(k)

        def own_edge():
            @lower_inner
            def _():
                halo[0, 0] = zpad[0, pl.ds(q * rows, 8), :]
                h_copy(0).start()

        tail = pl.ds(q * rows, 8)

        def far_tiles(early):
            for t in range(q):
                soon = (t == first_tile) | (t == second_tile)

                @pl.when(soon if early else jnp.logical_not(soon))
                def _():
                    convolve(0, 1, (t,))

        def far_early():
            @pl.when((l == 1) | ((l == 2) & (j == 0)))
            def _():
                zpad[1, 0:8, :] = jnp.zeros((8, width), jnp.float32)

            @pl.when((l == 2) & (j > 0))
            def _():
                zpad[1, 0:8, :] = zpad[0, tail, :]

            @inner
            def _():
                far_tiles(True)
                k_copy(first_tile).start()
                k_copy(second_tile).start()

        def far_gates():
            @inner
            def _():
                far_tiles(False)
                k_copy(third_tile).start()

            @pl.when((l == 1) | ((l == 2) & (j > 0)))
            def _():
                k_copy(fourth_tile).start()

        def far_first():
            @pl.when((l == 2) & (j == 0))
            def _():
                zpad[1, 0:8, :] = zpad[0, tail, :]
                convolve(0, 1, (0,))
                k_copy(fourth_tile).start()

        def own_gates():
            @lower_inner
            def _():
                zpad[0, 0:8, :] = zpad[1, tail, :]

            @upper_inner
            def _():
                h_copy(0).wait_recv()
                zpad[0, 0:8, :] = halo[0, 1]

            @inner
            def _():
                convolve(0, 0, range(q))

        def far_sent():
            @outer
            def _():
                take(rows_like(1), g_send.at[far])
                take(rows_like(2), n_send.at[0])

            @inner
            def _():
                gather_sent(0)
                take(rows_like(2), g_send.at[far])
                for r in range(1, tp):
                    take(rows_like(q), t_send.at[far, r - 1])
                take(gated.at[1], k_send.at[0])

            @lower_inner
            def _():
                h_copy(0).wait_send()


        def p_copy(layer, r, i):
            at = tile_at(flip(j, i))
            return remote(
                part.at[layer, lax.rem(c + r, tp), at, :], rec1.at[layer, r - 1, at, :],
                p_send.at[layer, r - 1], p_recv.at[layer, r - 1, i], at_tp(r),
            )


        bit_rows = half_rows // 2

        def bit_of(h, e):
            return pl.ds(h * half_rows + e * bit_rows, bit_rows)

        def r_copy(layer, i, h):
            at = part_of(h)
            return remote(
                snd2.at[layer, i, at, :], rec2.at[layer, i, at, :],
                r_send.at[layer], r_recv.at[layer, i - 1], at_sp(peer(i)),
            )

        def w_copy(layer, h, e):
            at = bit_of(h, e)
            return remote(
                snd2.at[layer, 2 - h, at, :], rec2.at[layer, 2 - h, at, :],
                r_send.at[layer], w_recv.at[layer, h, e], at_sp(peer(2 - h)),
            )

        def v_copy(layer, h, e):
            at = bit_of(h, e)
            return remote(
                snd2.at[layer, 3, at, :], rec2.at[layer, 3, at, :],
                r_send.at[layer], v_recv.at[layer, h, e], at_sp(peer(1 + h)),
            )

        def reduce_tile(layer, i):
            at = tile_at(flip(j, i))
            total = part[layer, c, at, :].astype(jnp.float32)
            for r in range(1, tp):
                p_copy(layer, r, i).wait_recv()
                total = total + rec1[layer, r - 1, at, :].astype(jnp.float32)
            if i == 0:
                acc[...] = total
                return
            snd2[layer, i] = total.astype(jnp.bfloat16)
            if i == 3:
                for e in range(2):
                    for h in range(2):
                        v_copy(layer, h, e).start()
            elif halves == 1:
                r_copy(layer, i, 0).start()
            elif i == 1:
                r_copy(layer, 1, 0).start()

        def relay(layer, h, e):
            if halves == 2:
                v_copy(layer, h, e).wait_recv()
                i, at = 2 - h, bit_of(h, e)
                snd2[layer, i, at, :] = (
                    snd2[layer, i, at, :].astype(jnp.float32) + rec2[layer, 3, at, :].astype(jnp.float32)
                ).astype(jnp.bfloat16)
                w_copy(layer, h, e).start()
                if h == 0 and e == 1:
                    r_copy(layer, 2, 1).start()

        def out_product(layer):
            for i in range(q - 1, -1, -1):
                at = tile_at(flip(j, i))

                def half(n, carry):
                    cc = lax.rem(c + 1 + n, tp)
                    weight = jnp.concatenate([wout[layer, cc * per_half + b] for b in range(per_half)], axis=1)
                    part[layer, cc, at, :] = jnp.dot(
                        gated[0, at, :], weight, preferred_element_type=jnp.float32
                    ).astype(jnp.bfloat16)
                    return carry

                lax.fori_loop(0, tp, half, 0)
                for r in range(1, tp):
                    p_copy(layer, r, i).start()
                if i < q - 1:
                    reduce_tile(layer, i + 1)
            reduce_tile(layer, 0)


        def late_half():
            return (l < line // 2).astype(jnp.int32)

        def half_tile(second, i):
            cc = late_half() if second else 1 - late_half()
            weight = jnp.concatenate([wout[0, cc * per_half + b] for b in range(per_half)], axis=1)
            at = tile_at(flip(j, i))
            if not second:
                @outer
                def _():
                    k_copy(flip(j, i)).wait_recv()

            part[0, cc, at, :] = jnp.dot(
                gated[0, at, :], weight, preferred_element_type=jnp.float32
            ).astype(jnp.bfloat16)

            @pl.when(cc != c)
            def _():
                p_copy(0, 1, i).start()

        def half_sum(second, i):
            @pl.when((late_half() == c) if second else (late_half() != c))
            def _():
                reduce_tile(0, i)

        def inner_late_tile(i):
            @inner
            def _():
                half_tile(True, i)

        def inner_late_sum(i):
            @inner
            def _():
                half_sum(True, i)

        def outer_late_tile(i):
            @outer
            def _():
                half_tile(True, i)

        def outer_late_sum(i):
            @outer
            def _():
                half_sum(True, i)

        def half_relay(second, h, e):
            @pl.when((late_half() == c) if second else (late_half() != c))
            def _():
                relay(0, h, e)


        last = layers - 1

        def nth_block(n):
            upper = (l >= line // 2).astype(jnp.int32)
            inner = ((l > 0) & (l < line - 1)).astype(jnp.int32)
            b = n
            if n < 2:
                b = n + inner * (1 - 2 * n)
            return b + upper * (line - 1 - 2 * b)

        def cols_of(m):
            return pl.ds(pl.multiple_of(m * block_cols, block_cols), block_cols)

        def q_copy(n, i):
            b = nth_block(n)
            m = lax.rem(b, slots)
            at = tile_at(flip(j, i))
            return remote(
                part.at[last, lax.div(b, slots), at, cols_of(m)], rec1.at[last, 0, at, cols_of(m)],
                p_send.at[last, 0], p_recv.at[last, m, i], at_tp(1),
            )

        def b_copy(m, i, h):
            at = part_of(h)
            return remote(
                snd2.at[last, i, at, cols_of(m)], rec2.at[last, i, at, cols_of(m)],
                b_send.at[0], b_recv.at[m, i - 1, h], at_sp(peer(i if i < 3 else 1 + h)),
            )

        def block_product(n):
            b = nth_block(n)
            m = lax.rem(b, slots)
            own = lax.div(b, slots) == c
            weight = jnp.concatenate([wout[last, b * q + e] for e in range(q)], axis=1)
            for i in range(q - 1, -1, -1):
                at = tile_at(flip(j, i))
                part[last, lax.div(b, slots), at, cols_of(m)] = jnp.dot(
                    gated[0, at, :], weight, preferred_element_type=jnp.float32
                ).astype(jnp.bfloat16)

                @pl.when(jnp.logical_not(own))
                def _():
                    q_copy(n, i).start()

        def block_sum(n):
            b = nth_block(n)
            m = lax.rem(b, slots)

            @pl.when(lax.div(b, slots) == c)
            def _():
                for i in range(q - 1, -1, -1):
                    at = tile_at(flip(j, i))
                    q_copy(n, i).wait_recv()
                    total = part[last, c, at, cols_of(m)].astype(jnp.float32)
                    total = total + rec1[last, 0, at, cols_of(m)].astype(jnp.float32)
                    if i == 0:
                        acc[:, cols_of(m)] = total
                        continue
                    snd2[last, i, :, cols_of(m)] = total.astype(jnp.bfloat16)
                    if i == 3:
                        b_copy(m, 3, 0).start()
                        b_copy(m, 3, 1).start()
                    elif i == 1:
                        b_copy(m, 1, 0).start()

        def block_relay(n):
            b = nth_block(n)
            m = lax.rem(b, slots)

            @pl.when(lax.div(b, slots) == c)
            def _():
                for h in range(2):
                    b_copy(m, 3, h).wait_recv()
                    i, at = 2 - h, part_of(h)
                    snd2[last, i, at, cols_of(m)] = (
                        snd2[last, i, at, cols_of(m)].astype(jnp.float32)
                        + rec2[last, 3, at, cols_of(m)].astype(jnp.float32)
                    ).astype(jnp.bfloat16)
                    b_copy(m, i, h).start()
                    if h == 0:
                        b_copy(m, 2, 1).start()

        def sums_sent(layer):
            for r in range(1, tp):
                take(part.at[layer, 0], p_send.at[layer, r - 1])
                take(stat.at[layer], s_send.at[layer, r - 1])
            if q > 1:
                take(snd2.at[layer, pl.ds(0, q - 1)], b_send.at[0] if timed and layer == last else r_send.at[layer])

        def s_copy(layer, r, h):
            return remote(
                stat.at[layer, h], stat_in.at[layer, r, h], s_send.at[layer, r - 1], s_recv.at[layer, r - 1, h], at_tp(r)
            )

        def finish(layer, h):
            at = part_of(h)
            pre = alpha * mine(layer, h)[...].astype(jnp.float32) + acc[at, :]
            for i in range(1, min(q, 3)):
                if timed and layer == last:
                    for m in range(slots):
                        b_copy(m, i, h).wait_recv()
                elif halves == 2 and i == 2 - h:
                    for e in range(2):
                        w_copy(layer, h, e).wait_recv()
                else:
                    r_copy(layer, i, h).wait_recv()
                pre = pre + rec2[layer, i, at, :].astype(jnp.float32)
            acc[at, :] = pre
            own = jnp.sum(pre, axis=-1, keepdims=True)
            away = pre - own * (1.0 / feats)
            spread = jnp.sum(away * away, axis=-1, keepdims=True)
            lane = lax.broadcasted_iota(jnp.int32, (half_rows, LANES), 1)
            stat[layer, h] = jnp.where(lane == 0, own, spread)
            for r in range(1, tp):
                s_copy(layer, r, h).start()
            sums, spreads = [own], [spread]
            for r in range(1, tp):
                s_copy(layer, r, h).wait_recv()
                sums.append(stat_in[layer, r, h, :, 0:1])
                spreads.append(stat_in[layer, r, h, :, 1:2])
            mean = sum(sums[1:], sums[0]) * (1.0 / model)
            var = sum(spreads[1:], spreads[0])
            for s in sums:
                off = s * (1.0 / feats) - mean
                var = var + feats * off * off
            scale = lax.rsqrt(var * (1.0 / model) + EPS)
            normed = (acc[at, :] - mean) * scale
            y = (normed * gain[pl.ds(layer, 1), :] + bias[pl.ds(layer, 1), :]).astype(jnp.bfloat16)
            if layer == last:
                res[at, :] = y
            else:
                mine(layer + 1, h)[...] = y


        tasks = []

        def at_time(when, fn, *args):
            tasks.append((when, len(tasks), fn, args))

        def first_half(layer, w0, w1, w2):
            def start():
                gather_wait(layer, False)
                if q > 3:
                    gather_wait(layer, True)
                arrived(layer * 4)
                project(layer, layer, 0, put_u(0), ALL)

            def middle():
                arrived(layer * 4 + 1)
                project(layer, layer, 1, put_z(0), ALL)
                halo_start(layer)

            def gates():
                arrived(layer * 4 + 2)
                project(layer, layer, 2, put_o(0), ALL)
                halo_wait(layer)
                convolve(layer, 0, range(q))
                halo_sent(layer)

            at_time(w0, start)
            at_time(w1, middle)
            at_time(w2, gates)

        def some_of(layer, w, span, fresh):
            if fresh:
                arrived(layer * 4 + w)
            project(layer, layer, w, (put_u, put_z, put_o)[w](0), span)

        def rest_of(layer):
            gather_wait(layer, True)
            project(layer, layer, 0, put_u(0), REST)
            project(layer, layer, 1, put_z(0), REST)
            halo_start(layer)

        def gates_of(layer):
            project(layer, layer, 2, put_o(0), REST)
            halo_wait(layer)
            convolve(layer, 0, range(q))

        def halo_sent(layer):
            @pl.when(l < line - 1)
            def _():
                h_copy(layer).wait_send()

        def second_half(layer, when):
            def go():
                arrived(layer * 4 + 3)
                out_product(layer)

            at_time(when, go)

        if timed:
            at_time(-1.0, far_send)
            for when, k in ((0.0, 0), (0.1, 1), (0.2, 3), (0.3, 4), (0.5, 2), (0.6, 5), (0.7, 6), (0.8, 7)):
                at_time(when, scatter_start, k)
            for h in range(halves):
                at_time(0.4, inner_gather_start, h)
                at_time((8.6, 13.6)[h], far_in, h)
                at_time((20.0, 26.0)[h], inner_pass, 0, h)
                at_time(42.55 + 0.01 * h, inner_onward, 0, h)
                at_time(53.19 + 0.001 * h, inner_last, 0, h)
                at_time(51.0 + 0.05 * h, inner_last, far, h)
            at_time(15.1, far_pass)
            at_time(43.1, far_side)
            at_time(42.5, far_diag)
            for k, when in enumerate((3.5, 6.5, 15.0, 15.2, 15.3, 18.0, 22.0, 24.0)):
                at_time(when, outer_begin, k)
            for k, when in enumerate((3.5, 6.5, 27.5, 9.5, 12.5, 30.0, 38.0, 41.0)):
                at_time(when, inner_ready, k)
            for k, when in enumerate((3.6, 6.6, 27.6, 9.6, 43.2, 57.1, 61.92, 66.2)):
                at_time(when, inward, k, 0)
            for k, when in enumerate((19.0, 25.0, 31.0, 51.5, 57.0, 61.9, 66.1, 67.6)):
                at_time(when, inward, k, 1)
            for k, when in enumerate((9.7, 12.6, 30.1, 38.1, 41.1)):
                at_time(when, outward, k + 3, 0)
            for k, when in enumerate((23.5, 61.91, 67.5, 79.0, 87.1)):
                at_time(when, outward, k + 3, 1)
            for k, when in enumerate((54.2, 66.0, 72.5, 82.0)):
                at_time(when, outward, k + 3, 2)
            at_time(33.1, inner_wait, 0, False)
            at_time(33.1, inner_arrived, 0)
            at_time(33.2, inner_project, 0, (0,), MOST)
            at_time(37.0, inner_arrived, 1)
            at_time(37.0, inner_project, 0, (1,), MOST)
            at_time(43.5, inner_wait, far, False)
            at_time(38.2, inner_own)
            at_time(38.2, inner_project, 1, (0, 1), OWN)
            at_time(43.6, inner_project, 1, (0, 1), SIDE)
            at_time(45.5, inner_arrived, 2)
            at_time(45.6, inner_project, 1, (2,), MOST)
            at_time(45.7, far_early)
            at_time(52.0, inner_wait, far, True)
            at_time(52.1, inner_project, 1, (0, 1, 2), REST)
            at_time(53.1, far_gates)
            at_time(53.18, inner_project, 0, (2,), MOST)
            at_time(53.2, inner_wait, 0, True)
            at_time(53.21, inner_project, 0, (0, 1), REST)
            at_time(53.22, own_edge)
            at_time(53.23, far_first)
            at_time(54.21, inner_project, 0, (2,), REST)
            at_time(55.3, own_gates)
            o = 58.0
            at_time(o, line_end, 3, 0)
            for n, i in enumerate((1, 3, 2, 0)):
                at_time(o + 0.1 * n, half_tile, False, i)
                at_time(o + 0.1 * n + 0.15, half_sum, False, i)
            for e in range(2):
                for h in range(2):
                    at_time(o + 8.5 + 0.1 * e + 0.01 * h, half_relay, False, h, e)
            at_time(o + 8.75, line_end, 3, 1)
            at_time(o + 8.75, line_end, 3, 2)
            for n, i in enumerate((3, 2, 1, 0)):
                at_time(o + 4.3 + 0.1 * n, inner_late_tile, i)
                at_time(o + 4.3 + 0.1 * n + 0.15, inner_late_sum, i)
                at_time(o + 8.8 + 0.01 * n, outer_late_tile, i)
                at_time(o + 8.8 + 0.01 * n + 0.015, outer_late_sum, i)
            for e in range(2):
                for h in range(2):
                    at_time(o + 9.0 + 0.1 * e + 0.01 * h, half_relay, True, h, e)
            for h in range(halves):
                f = o + 14.0 + 6.0 * h
                at_time(f, finish, 0, h)
                at_time(f + 0.1, gather_start, 1, h)
                at_time(f + 9.0, gather_pass, 1, h)
                at_time(93.0 + 0.1 * h, gather_last, 1, h)
            at_time(88.0, gather_wait, 1, False)
            at_time(82.5, gather_own, 1)
            at_time(82.5, some_of, 1, 0, OWN, True)
            at_time(87.2, some_of, 1, 1, OWN, True)
            at_time(88.1, some_of, 1, 0, SIDE, False)
            at_time(88.1, some_of, 1, 1, SIDE, False)
            at_time(93.15, some_of, 1, 2, MOST, True)
            at_time(93.2, rest_of, 1)
            at_time(93.5, outward, units - 1, 2)
            at_time(94.0, gates_of, 1)
            at_time(128.0, halo_sent, 1)
            for n in range(1, line):
                at_time((110.0, 110.1, 111.0, 113.0)[n], line_end, units - 1, n - 1)
            for n in range(line):
                at_time((110.0, 110.2, 111.0, 113.0)[n], block_product, n)
                at_time((110.3, 110.4, 111.1, 113.5)[n], block_sum, n)
                at_time((113.1, 113.2, 114.0, 114.1)[n], block_relay, n)
            at_time(127.5, far_sent)
            at_time(128.0, gather_sent, 1)
            at_time(128.1, sums_sent, 0)
            for k in range(units):
                at_time(129.5, all_sent, k)
            for h in range(halves):
                at_time(130.0 + h, finish, last, h)
            at_time(140.0, sums_sent, last)
        else:
            for k in range(units):
                at_time(-2.0 if k < 2 else -1.0, scatter_start, k)
            for h in range(halves):
                at_time(-1.5, gather_start, 0, h)
            begin = [k + k // 4 for k in range(units)]
            for k in range(units):
                at_time(begin[k], line_begin, k)
                for s in range(1, steps):
                    at_time(begin[k] + s, line_pass, k, s)
            end = begin[-1] + max(steps, 1) + 1
            ready = [begin[k] + steps for k in range(units)]
            for layer in range(layers):
                if layer == 0:
                    base = ready[0] + 0.5
                else:
                    base = max(ready[4 * layer - 1] + 4.0, end if layer > 1 else 0) + 0.5
                for h in range(halves):
                    at_time(base - 1.3, gather_pass, layer, h)
                    at_time(base - 1.2, gather_last, layer, h)
                w1 = max(base + 0.1, ready[4 * layer + 1] + 0.5)
                w2 = max(w1 + 0.1, ready[4 * layer + 2] + 0.5)
                first_half(layer, base, w1, w2)
                o = max(w2 + 0.1, ready[4 * layer + 3] + 0.5)
                second_half(layer, o)
                for e in range(2):
                    for h in range(2):
                        at_time(o + 0.1, relay, layer, h, e)
                for h in range(halves):
                    at_time(o + 0.3, finish, layer, h)
                    if layer < last:
                        at_time(o + 0.4, gather_start, layer + 1, h)

        for _, _, fn, args in sorted(tasks, key=lambda task: task[:2]):
            fn(*args)
        if not timed:
            for layer in range(layers):
                gather_sent(layer)
                sums_sent(layer)
            for k in range(units):
                scatter_sent(k)
                for s in range(steps):
                    line_sent(k, s)

    return kernel


def solution(mesh):
    sp, tp = mesh.shape["sp"], mesh.shape["tp"]

    def shards(tokens, value_weight, outer_weight, inner_weight, conv_taps, output_weight, norm_gain, norm_bias):
        rows, feats = tokens.shape
        layers, depth, channels = value_weight.shape
        taps_count = conv_taps.shape[1]
        q = plane_size(sp, channels)
        width = channels // q
        line = sp // q
        model = feats * tp
        alpha = (2.0 * layers) ** 0.25
        out_cols = output_weight.shape[2]
        bf, f32 = jnp.bfloat16, jnp.float32
        kernel = make_kernel(sp, tp, q, layers, taps_count, rows, feats, depth, width, out_cols, alpha)
        dma = pltpu.SemaphoreType.DMA
        units, steps = 4 * layers, max(line - 1, 1)
        others = max(tp - 1, 1)
        banks = 2 if helped(line, q, tp, layers) else 1
        sets = layers + banks - 1
        relays = 1 if banks == 2 else layers
        if banks == 2:
            lines = [dma((units,)), dma((units, steps)), dma((1,)), dma((1,))]
        else:
            lines = [dma((units, steps))] * 4
        halves = 2 if q == 4 else 1
        half_rows = rows // halves
        vm, hbm = pl.BlockSpec(memory_space=pltpu.VMEM), pl.BlockSpec(memory_space=pl.ANY)
        return pl.pallas_call(
            kernel,
            out_shape=jax.ShapeDtypeStruct((rows, feats), bf),
            in_specs=[hbm] * 4 + [vm, hbm, vm, vm],
            out_specs=vm,
            scratch_shapes=[
                pltpu.VMEM((layers + banks - 1, tp, q * rows, feats), bf),
                pltpu.VMEM((layers, 3, model, width), bf),
                pltpu.VMEM((layers, sp, width, out_cols), bf),
                pltpu.VMEM((banks, q * rows, width), bf),
                pltpu.VMEM((banks, q * rows, width), bf),
                pltpu.VMEM((banks, q * rows + 8, width), f32),
                pltpu.VMEM((banks, q * rows, width), bf),
                pltpu.VMEM((layers, tp, q * rows, feats), bf),
                pltpu.VMEM((layers, others, q * rows, feats), bf),
                pltpu.VMEM((layers, q, rows, feats), bf),
                pltpu.VMEM((layers, q, rows, feats), bf),
                pltpu.VMEM((rows, feats), f32),
                pltpu.VMEM((layers, halves, half_rows, LANES), f32),
                pltpu.VMEM((layers, tp, halves, half_rows, LANES), f32),
                pltpu.VMEM((layers, 2, 8, width), f32),
                dma((units,)), dma((units,)), *lines,
                dma((sets,)), dma((sets, 3, halves)), dma((1,)),
                dma((sets, others)), dma((sets, others, 3)),
                dma((layers, others)), dma((layers, max(others, 2), q)),
                dma((layers,)), dma((layers, 2)),
                dma((layers, others)), dma((layers, others, halves)),
                dma((layers,)), dma((layers,)),
                dma((1,)), dma((2, 3, 2)), dma((1,)), dma((4,)), dma((1,)), dma((4,)),
                dma((relays, 2, 2)), dma((relays, 2, 2)), dma((2,)),
                *[pltpu.VMEM(a.shape, bf) for a in (tokens, value_weight, outer_weight, inner_weight, output_weight)],
                dma((5,)),
            ],
            compiler_params=pltpu.CompilerParams(
                collective_id=0, has_side_effects=True, vmem_limit_bytes=60 * 1024 * 1024
            ),
        )(tokens, value_weight, outer_weight, inner_weight, jnp.swapaxes(conv_taps, 0, 1), output_weight, norm_gain, norm_bias)

    in_specs = (
        P("sp", "tp"),
        P(None, "sp", "tp"),
        P(None, "sp", "tp"),
        P(None, "sp", "tp"),
        P(None, None, "tp"),
        P(None, "tp", "sp"),
        P(None, "tp"),
        P(None, "tp"),
    )
    return jax.shard_map(shards, mesh=mesh, in_specs=in_specs, out_specs=P("sp", "tp"), check_vma=False)
```

```python
import jax
import jax.numpy as jnp
from jax import lax
from jax.experimental import pallas as pl
from jax.experimental.pallas import tpu as pltpu
from jax.sharding import PartitionSpec as P

LANES = 128
EPS = 1e-5


def flip(j, i):
    if i & 1:
        j = j + 1 - 2 * lax.rem(j, 2)
    if i & 2:
        j = j + 2 - 4 * lax.rem(lax.div(j, 2), 2)
    return j


def plane_size(sp, channels):
    q = 4
    while q > 1 and (sp % q or channels // q < LANES or channels % q):
        q //= 2
    return q


def helped(line, q, tp, layers):
    return line == 4 and q == 4 and tp == 2 and layers == 2


def make_kernel(sp, tp, q, layers, taps_count, rows, feats, depth, width, out_cols, alpha):
    line = sp // q
    units = layers * 4
    model = feats * tp
    per_half = sp // tp
    steps = line - 1
    halves = 2 if q == 4 else 1
    half_rows = rows // halves
    timed = helped(line, q, tp, layers)
    slots = line // tp if timed else 1
    block_cols = q * out_cols

    def kernel(
        tok_in, val_in, outw_in, inn_in, taps, prj_in, gain, bias, res,
        xg, win, wout, ubuf, obuf, zpad, gated, part, rec1, snd2, rec2, acc, stat, stat_in, halo,
        a_send, a_recv, u_send, u_recv, d_send, d_recv,
        g_send, g_recv, g_loc, t_send, t_recv, p_send, p_recv, r_send, r_recv, s_send, s_recv, h_send, h_recv,
        b_send, b_recv, n_send, n_recv, k_send, k_recv,
        v_recv, w_recv, e_recv, tok, val, outw, inn, prj, in_sem,
    ):
        me = lax.axis_index("sp")
        c = lax.axis_index("tp")
        l = lax.div(me, q)
        j = lax.rem(me, q)

        def at_sp(other):
            return {"sp": other, "tp": c}

        def at_tp(r):
            return {"sp": me, "tp": lax.rem(c + r, tp)}

        def remote(src, dst, ssem, rsem, dev):
            return pltpu.make_async_remote_copy(
                src_ref=src, dst_ref=dst, send_sem=ssem, recv_sem=rsem,
                device_id=dev, device_id_type=pl.DeviceIdType.MESH,
            )

        def peer(i):
            return l * q + flip(j, i)

        loads = [
            pltpu.make_async_copy(src, dst, in_sem.at[n])
            for n, (src, dst) in enumerate(
                ((tok_in, tok), (val_in, val), (inn_in, inn), (prj_in, prj), (outw_in, outw))
            )
        ]
        for load in loads:
            load.start()

        barrier = pltpu.get_barrier_semaphore()

        def greet(dev):
            pl.semaphore_signal(barrier, inc=1, device_id=dev, device_id_type=pl.DeviceIdType.MESH)

        for i in range(1, q):
            greet(at_sp(peer(i)))
        for r in range(1, tp):
            greet(at_tp(r))

        @pl.when(l > 0)
        def _():
            greet(at_sp(me - q))

        @pl.when(l < line - 1)
        def _():
            greet(at_sp(me + q))

        neighbours = (l > 0).astype(jnp.int32) + (l < line - 1).astype(jnp.int32)
        pl.semaphore_wait(barrier, (q - 1) + (tp - 1) + neighbours)
        for load in loads:
            load.wait()


        ORDER = (val, inn, outw, prj)

        def own_piece(k, jd):
            layer, w = divmod(k, 4)
            at = pl.ds(pl.multiple_of(jd * width, width), width)
            if w == 3:
                return prj.at[layer, at, :]
            return ORDER[w].at[layer, :, at]

        def landed(k, s):
            layer, w = divmod(k, 4)
            if w == 3:
                return wout.at[layer, s]
            return win.at[layer, w, pl.ds(pl.multiple_of(s * depth, depth), depth), :]

        def block(k, b):
            layer, w = divmod(k, 4)
            if w == 3:
                return wout.at[layer, pl.ds(b * q, q)]
            return win.at[layer, w, pl.ds(pl.multiple_of(b * (q * depth), q * depth), q * depth), :]

        def a_copy(k, i):
            return remote(own_piece(k, flip(j, i)), landed(k, me), a_send.at[k], a_recv.at[k], at_sp(peer(i)))

        def a_local(k):
            return pltpu.make_async_copy(own_piece(k, j), landed(k, me), a_recv.at[k])

        def scatter_start(k):
            a_local(k).start()
            for i in range(q - 1, 0, -1):
                a_copy(k, i).start()


        def take(ref, sem):
            pltpu.make_async_copy(ref, ref, sem).wait()

        def scatter_wait(k):
            take(block(k, l), a_recv.at[k])

        def scatter_sent(k):
            layer, w = divmod(k, 4)
            if q > 1:
                n = q - 1
                take(wout.at[layer, pl.ds(0, n)] if w == 3 else win.at[layer, w, pl.ds(0, n * depth), :], a_send.at[k])

        def up(k, s):
            sems = (u_send.at[k], u_recv.at[k, s]) if timed else (u_send.at[k, s], u_recv.at[k, s])
            return remote(block(k, l - s), block(k, l - s), *sems, at_sp(me + q))

        def down(k, s):
            sems = (u_send.at[k], u_recv.at[k, steps - 1 - s]) if timed else (d_send.at[k, s], d_recv.at[k, s])
            return remote(block(k, l + s), block(k, l + s), *sems, at_sp(me - q))

        def line_begin(k):
            scatter_wait(k)

            @pl.when(l < line - 1)
            def _():
                up(k, 0).start()

            @pl.when(l > 0)
            def _():
                down(k, 0).start()

        def line_pass(k, s):
            @pl.when((l - s >= 0) & (l < line - 1))
            def _():
                up(k, s - 1).wait_recv()
                up(k, s).start()

            @pl.when((l + s < line) & (l > 0))
            def _():
                down(k, s - 1).wait_recv()
                down(k, s).start()


        def lower_inner(fn):
            pl.when(l == 1)(fn)

        def upper_inner(fn):
            pl.when(l == 2)(fn)

        def outer(fn):
            pl.when((l == 0) | (l == 3))(fn)

        def inner(fn):
            pl.when((l == 1) | (l == 2))(fn)

        def outer_begin(k):
            @pl.when(l == 0)
            def _():
                scatter_wait(k)
                up(k, 0).start()

            @pl.when(l == 3)
            def _():
                scatter_wait(k)
                down(k, 0).start()

        def inner_ready(k):
            @inner
            def _():
                scatter_wait(k)

        def inward(k, s):
            @lower_inner
            def _():
                if s:
                    up(k, s - 1).wait_recv()
                up(k, s).start()

            @upper_inner
            def _():
                if s:
                    down(k, s - 1).wait_recv()
                down(k, s).start()

        def outward(k, s):
            @lower_inner
            def _():
                if s:
                    down(k, s - 1).wait_recv()
                down(k, s).start()

            @upper_inner
            def _():
                if s:
                    up(k, s - 1).wait_recv()
                up(k, s).start()

        def ends(k):
            return (1, line - 2) if timed and k < 3 else (0, line - 1)

        def line_end(k, s):
            low, high = ends(k)

            @pl.when((l == high) & (l - 1 - s >= 0))
            def _():
                up(k, s).wait_recv()

            @pl.when((l == low) & (l + 1 + s < line))
            def _():
                down(k, s).wait_recv()

        def arrived(k):
            for s in range(steps):
                line_end(k, s)

        def line_sent(k, s):
            @pl.when((l - s >= 0) & (l < line - 1))
            def _():
                up(k, s).wait_send()

            @pl.when((l + s < line) & (l > 0))
            def _():
                down(k, s).wait_send()

        def all_sent(k):
            each = q * depth * width // feats
            scatter_sent(k)

            @outer
            def _():
                take(xg.at[0, 0, pl.ds(0, each), :], u_send.at[k])

            @inner
            def _():
                take(xg.at[0, 0, pl.ds(0, (2 if k < 3 else 5) * each), :], u_send.at[k])

        def outward_for(held, k, s):
            holder = (l == 1) & (c == 1)

            @pl.when(holder if held else jnp.logical_not(holder))
            def _():
                outward(k, s)


        def part_of(h):
            return pl.ds(h * half_rows, half_rows)

        def spot(layer, jj, h):
            at = pl.ds(pl.multiple_of(jj * rows + h * half_rows, half_rows), half_rows)
            return xg.at[layer, c, at, :]

        def mine(layer, h):
            return tok.at[part_of(h)] if layer == 0 else spot(layer, j, h)

        def g_copy(layer, i, h):
            if i == 3:
                src = spot(layer, flip(j, 1 + h), h)
                return remote(src, src, g_send.at[layer], g_recv.at[layer, i - 1, h], at_sp(peer(2 - h)))
            return remote(
                mine(layer, h), spot(layer, j, h), g_send.at[layer], g_recv.at[layer, i - 1, h], at_sp(peer(i))
            )

        def g_piece(i, e):
            first = (j if i == 2 else flip(j, 2)) * rows + half_rows + e * (half_rows // 2)
            src = xg.at[1, c, pl.ds(pl.multiple_of(first, half_rows // 2), half_rows // 2), :]
            got = e_recv.at[e] if i == 2 else g_recv.at[1, 2, 1]
            return remote(src, src, g_send.at[1], got, at_sp(peer(2 if i == 2 else 1)))

        def g_local(h):
            return pltpu.make_async_copy(tok.at[part_of(h)], spot(0, j, h), g_loc.at[0])

        def rows_like(n):
            return xg.at[0, 0, pl.ds(0, n * rows), :]

        def kind(layer, i):
            return 1 if i == 3 else 2 if i == 0 and timed and layer else 0

        def t_copy(layer, r, i, h):
            src = mine(layer, h) if i == 0 else spot(layer, flip(j, i), h)
            return remote(
                src, spot(layer, flip(j, i), h), t_send.at[layer, r - 1], t_recv.at[layer, r - 1, kind(layer, i)], at_tp(r)
            )

        def cross_start(layer, i, h):
            for r in range(1, tp):
                t_copy(layer, r, i, h).start()

        def gather_start(layer, h):
            if layer == 0:
                g_local(h).start()
            for i in range(1, min(q, 3)):
                if timed and layer == 1 and i == 2 and h == 1:
                    for e in range(2):
                        g_piece(2, e).start()
                else:
                    g_copy(layer, i, h).start()
            cross_start(layer, 0, h)

        def gather_pass(layer, h, onward=True):
            first = 1 + h if q == 4 else 1
            for i in range(1, min(q, 3)):
                i = first if i == 1 else 3 - first
                if timed and layer == 1 and i == 2 and h == 1:
                    for e in range(2):
                        g_piece(2, e).wait_recv()
                        g_piece(3, e).start()
                else:
                    g_copy(layer, i, h).wait_recv()
                    if q == 4 and i == first and onward:
                        g_copy(layer, 3, h).start()
                cross_start(layer, i, h)

        def gather_last(layer, h):
            if q == 4:
                g_copy(layer, 3, h).wait_recv()
                cross_start(layer, 3, h)

        def gather_wait(layer, rest):
            for r in range(1, tp):
                n = 1 if rest else 2 if timed and layer else min(q, 3)
                take(rows_like(n), t_recv.at[layer, r - 1, 1 if rest else 0])
            if layer == 0 and not rest:
                take(rows_like(1), g_loc.at[0])

        def gather_own(layer):
            for r in range(1, tp):
                take(rows_like(1), t_recv.at[layer, r - 1, 2])

        def gather_sent(layer):
            if q > 1:
                take(rows_like(q - 1), g_send.at[layer])
            for r in range(1, tp):
                take(rows_like(q), t_send.at[layer, r - 1])

        def tile_at(jj):
            return pl.ds(pl.multiple_of(jj * rows, rows), rows)


        far = layers
        ALL, MOST, REST, OWN, SIDE = (0, q), (1, q - 1), (0, 1), (0, 1, 0), (0, 2, 0)

        def project(rows_set, layer, w, store, span):
            first = flip(j, q - 1) if span is not ALL else 0

            def tile(n, carry):
                if span is OWN:
                    i = j
                elif span is SIDE:
                    i = flip(j, 1) + n * (flip(j, 2) - flip(j, 1))
                else:
                    i = lax.rem(first + span[0] + n, q)
                at = tile_at(i)
                total = jnp.zeros((rows, width), jnp.float32)
                for cc in range(tp):
                    total = total + jnp.dot(
                        xg[rows_set, cc, at, :],
                        win[layer, w, pl.ds(cc * feats, feats), :],
                        preferred_element_type=jnp.float32,
                    )
                store(i, total.astype(jnp.bfloat16))
                return carry

            lax.fori_loop(0, span[1], tile, 0)

        def put_u(bank):
            def put(i, v):
                ubuf[bank, tile_at(i), :] = v

            return put

        def put_o(bank):
            def put(i, v):
                obuf[bank, tile_at(i), :] = v

            return put

        def put_z(bank):
            def put(i, v):
                at = pl.ds(pl.multiple_of(8 + i * rows, 8), rows)
                zpad[bank, at, :] = v.astype(jnp.float32) * ubuf[bank, tile_at(i), :].astype(jnp.float32)

            return put

        def h_copy(layer):
            return remote(
                halo.at[layer, 0], halo.at[layer, 1], h_send.at[layer], h_recv.at[layer], at_sp(me + q)
            )

        def halo_start(layer):
            halo[layer, 0] = zpad[0, pl.ds(q * rows, 8), :]

            @pl.when(l < line - 1)
            def _():
                h_copy(layer).start()

        def halo_wait(layer):
            zpad[0, 0:8, :] = jnp.zeros((8, width), jnp.float32)

            @pl.when(l > 0)
            def _():
                h_copy(layer).wait_recv()
                zpad[0, 0:8, :] = halo[layer, 1]

        def convolve(layer, bank, tiles):
            at_c = pl.ds(pl.multiple_of(j * width, width), width)
            rates = [taps[k, pl.ds(layer, 1), at_c] for k in range(taps_count)]
            for i in tiles:
                conv = jnp.zeros((rows, width), jnp.float32)
                for k in range(taps_count):
                    first = 8 - (taps_count - 1) + k + i * rows
                    conv = conv + rates[k] * zpad[bank, first:first + rows, :]
                at = pl.ds(i * rows, rows)
                gated[bank, at, :] = (obuf[bank, at, :].astype(jnp.float32) * conv).astype(jnp.bfloat16)


        def fellow():
            return at_sp(me + q * (1 - 2 * lax.rem(l, 2)))

        def n_copy(n):
            h = n % 2
            src = tok.at[part_of(h)] if n < 2 else spot(far, flip(j, 1 + h), h)
            return remote(
                src, spot(far, j if n < 2 else flip(j, 1 + h), h), n_send.at[0], n_recv.at[n], fellow()
            )

        def e_copy(h):
            return remote(
                tok.at[part_of(h)], spot(far, j, h), g_send.at[far], g_recv.at[far, h, h],
                at_sp(peer(1 + h)),
            )

        def k_copy(tile):
            at = tile_at(tile)
            return remote(gated.at[1, at, :], gated.at[0, at, :], k_send.at[0], k_recv.at[tile], fellow())


        odd = lax.rem(j, 2)
        first_tile, second_tile = flip(j, 1), odd * j + (1 - odd) * flip(j, 2)
        third_tile, fourth_tile = flip(j, 3), odd * flip(j, 2) + (1 - odd) * j

        def far_send():
            @outer
            def _():
                for h in range(2):
                    e_copy(h).start()
                for n in range(2):
                    n_copy(n).start()

        def far_pass():
            @outer
            def _():
                for h in range(2):
                    e_copy(h).wait_recv()
                    n_copy(2 + h).start()

        def far_in(h):
            @inner
            def _():
                n_copy(h).wait_recv()
                g_copy(far, 2 - h, h).start()
                cross_start(far, 0, h)

        def far_side():
            @inner
            def _():
                for h in range(2):
                    g_copy(far, 2 - h, h).wait_recv()
                    cross_start(far, 2 - h, h)

        def far_diag():
            @inner
            def _():
                for h in range(2):
                    n_copy(2 + h).wait_recv()
                    g_copy(far, 3, h).start()
                    cross_start(far, 1 + h, h)

        def inner_gather_start(h):
            @inner
            def _():
                gather_start(0, h)

        def inner_pass(rows_set, h):
            @inner
            def _():
                gather_pass(rows_set, h, False)

        def inner_onward(rows_set, h):
            @inner
            def _():
                g_copy(rows_set, 3, h).start()

        def inner_last(rows_set, h):
            @inner
            def _():
                gather_last(rows_set, h)

        def inner_wait(rows_set, rest):
            @inner
            def _():
                gather_wait(rows_set, rest)

        def inner_project(bank, ws, span):
            @inner
            def _():
                for w in ws:
                    project(far if bank else 0, 0, w, (put_u, put_z, put_o)[w](bank), span)

        def inner_own():
            @inner
            def _():
                gather_own(far)

        def inner_arrived(k):
            @inner
            def _():
                arrived(k)

        def own_edge():
            @lower_inner
            def _():
                halo[0, 0] = zpad[0, pl.ds(q * rows, 8), :]
                h_copy(0).start()

        tail = pl.ds(q * rows, 8)

        def far_tiles(early):
            for t in range(q):
                soon = (t == first_tile) | (t == second_tile)

                @pl.when(soon if early else jnp.logical_not(soon))
                def _():
                    convolve(0, 1, (t,))

        def far_early():
            @pl.when((l == 1) | ((l == 2) & (j == 0)))
            def _():
                zpad[1, 0:8, :] = jnp.zeros((8, width), jnp.float32)

            @pl.when((l == 2) & (j > 0))
            def _():
                zpad[1, 0:8, :] = zpad[0, tail, :]

            @inner
            def _():
                far_tiles(True)
                k_copy(first_tile).start()
                k_copy(second_tile).start()

        def far_gates():
            @inner
            def _():
                far_tiles(False)
                k_copy(third_tile).start()

            @pl.when((l == 1) | ((l == 2) & (j > 0)))
            def _():
                k_copy(fourth_tile).start()

        def far_first():
            @pl.when((l == 2) & (j == 0))
            def _():
                zpad[1, 0:8, :] = zpad[0, tail, :]
                convolve(0, 1, (0,))
                k_copy(fourth_tile).start()

        def own_gates():
            @lower_inner
            def _():
                zpad[0, 0:8, :] = zpad[1, tail, :]

            @upper_inner
            def _():
                h_copy(0).wait_recv()
                zpad[0, 0:8, :] = halo[0, 1]

            @inner
            def _():
                convolve(0, 0, range(q))

        def far_sent():
            @outer
            def _():
                take(rows_like(1), g_send.at[far])
                take(rows_like(2), n_send.at[0])

            @inner
            def _():
                gather_sent(0)
                take(rows_like(2), g_send.at[far])
                for r in range(1, tp):
                    take(rows_like(q), t_send.at[far, r - 1])
                take(gated.at[1], k_send.at[0])

            @lower_inner
            def _():
                h_copy(0).wait_send()


        def p_copy(layer, r, i):
            at = tile_at(flip(j, i))
            return remote(
                part.at[layer, lax.rem(c + r, tp), at, :], rec1.at[layer, r - 1, at, :],
                p_send.at[layer, r - 1], p_recv.at[layer, r - 1, i], at_tp(r),
            )


        bit_rows = half_rows // 2

        def bit_of(h, e):
            return pl.ds(h * half_rows + e * bit_rows, bit_rows)

        def r_copy(layer, i, h):
            at = part_of(h)
            return remote(
                snd2.at[layer, i, at, :], rec2.at[layer, i, at, :],
                r_send.at[layer], r_recv.at[layer, i - 1], at_sp(peer(i)),
            )

        def w_copy(layer, h, e):
            at = bit_of(h, e)
            return remote(
                snd2.at[layer, 2 - h, at, :], rec2.at[layer, 2 - h, at, :],
                r_send.at[layer], w_recv.at[layer, h, e], at_sp(peer(2 - h)),
            )

        def v_copy(layer, h, e):
            at = bit_of(h, e)
            return remote(
                snd2.at[layer, 3, at, :], rec2.at[layer, 3, at, :],
                r_send.at[layer], v_recv.at[layer, h, e], at_sp(peer(1 + h)),
            )

        def reduce_tile(layer, i):
            at = tile_at(flip(j, i))
            total = part[layer, c, at, :].astype(jnp.float32)
            for r in range(1, tp):
                p_copy(layer, r, i).wait_recv()
                total = total + rec1[layer, r - 1, at, :].astype(jnp.float32)
            if i == 0:
                acc[...] = total
                return
            snd2[layer, i] = total.astype(jnp.bfloat16)
            if i == 3:
                for e in range(2):
                    for h in range(2):
                        v_copy(layer, h, e).start()
            elif halves == 1:
                r_copy(layer, i, 0).start()
            elif i == 1:
                r_copy(layer, 1, 0).start()

        def relay(layer, h, e):
            if halves == 2:
                v_copy(layer, h, e).wait_recv()
                i, at = 2 - h, bit_of(h, e)
                snd2[layer, i, at, :] = (
                    snd2[layer, i, at, :].astype(jnp.float32) + rec2[layer, 3, at, :].astype(jnp.float32)
                ).astype(jnp.bfloat16)
                w_copy(layer, h, e).start()
                if h == 0 and e == 1:
                    r_copy(layer, 2, 1).start()

        def out_product(layer):
            for i in range(q - 1, -1, -1):
                at = tile_at(flip(j, i))

                def half(n, carry):
                    cc = lax.rem(c + 1 + n, tp)
                    weight = jnp.concatenate([wout[layer, cc * per_half + b] for b in range(per_half)], axis=1)
                    part[layer, cc, at, :] = jnp.dot(
                        gated[0, at, :], weight, preferred_element_type=jnp.float32
                    ).astype(jnp.bfloat16)
                    return carry

                lax.fori_loop(0, tp, half, 0)
                for r in range(1, tp):
                    p_copy(layer, r, i).start()
                if i < q - 1:
                    reduce_tile(layer, i + 1)
            reduce_tile(layer, 0)


        def late_half():
            return (l < line // 2).astype(jnp.int32)

        def half_tile(second, i):
            cc = late_half() if second else 1 - late_half()
            weight = jnp.concatenate([wout[0, cc * per_half + b] for b in range(per_half)], axis=1)
            at = tile_at(flip(j, i))
            if not second:
                @outer
                def _():
                    k_copy(flip(j, i)).wait_recv()

            part[0, cc, at, :] = jnp.dot(
                gated[0, at, :], weight, preferred_element_type=jnp.float32
            ).astype(jnp.bfloat16)

            @pl.when(cc != c)
            def _():
                p_copy(0, 1, i).start()

        def half_sum(second, i):
            @pl.when((late_half() == c) if second else (late_half() != c))
            def _():
                reduce_tile(0, i)

        def inner_late_tile(i):
            @inner
            def _():
                half_tile(True, i)

        def inner_late_sum(i):
            @inner
            def _():
                half_sum(True, i)

        def outer_late_tile(i):
            @outer
            def _():
                half_tile(True, i)

        def outer_late_sum(i):
            @outer
            def _():
                half_sum(True, i)

        def half_relay(second, h, e):
            @pl.when((late_half() == c) if second else (late_half() != c))
            def _():
                relay(0, h, e)


        last = layers - 1

        def nth_block(n):
            upper = (l >= line // 2).astype(jnp.int32)
            inner = ((l > 0) & (l < line - 1)).astype(jnp.int32)
            b = n
            if n < 2:
                b = n + inner * (1 - 2 * n)
            return b + upper * (line - 1 - 2 * b)

        def cols_of(m):
            return pl.ds(pl.multiple_of(m * block_cols, block_cols), block_cols)

        def q_copy(n, i):
            b = nth_block(n)
            m = lax.rem(b, slots)
            at = tile_at(flip(j, i))
            return remote(
                part.at[last, lax.div(b, slots), at, cols_of(m)], rec1.at[last, 0, at, cols_of(m)],
                p_send.at[last, 0], p_recv.at[last, m, i], at_tp(1),
            )

        def b_copy(m, i, h):
            at = part_of(h)
            return remote(
                snd2.at[last, i, at, cols_of(m)], rec2.at[last, i, at, cols_of(m)],
                b_send.at[0], b_recv.at[m, i - 1, h], at_sp(peer(i if i < 3 else 1 + h)),
            )

        def block_product(n):
            b = nth_block(n)
            m = lax.rem(b, slots)
            own = lax.div(b, slots) == c
            weight = jnp.concatenate([wout[last, b * q + e] for e in range(q)], axis=1)
            for i in range(q - 1, -1, -1):
                at = tile_at(flip(j, i))
                part[last, lax.div(b, slots), at, cols_of(m)] = jnp.dot(
                    gated[0, at, :], weight, preferred_element_type=jnp.float32
                ).astype(jnp.bfloat16)

                @pl.when(jnp.logical_not(own))
                def _():
                    q_copy(n, i).start()

        def block_sum(n):
            b = nth_block(n)
            m = lax.rem(b, slots)

            @pl.when(lax.div(b, slots) == c)
            def _():
                for i in range(q - 1, -1, -1):
                    at = tile_at(flip(j, i))
                    q_copy(n, i).wait_recv()
                    total = part[last, c, at, cols_of(m)].astype(jnp.float32)
                    total = total + rec1[last, 0, at, cols_of(m)].astype(jnp.float32)
                    if i == 0:
                        acc[:, cols_of(m)] = total
                        continue
                    snd2[last, i, :, cols_of(m)] = total.astype(jnp.bfloat16)
                    if i == 3:
                        b_copy(m, 3, 0).start()
                        b_copy(m, 3, 1).start()
                    elif i == 1:
                        b_copy(m, 1, 0).start()

        def block_relay(n):
            b = nth_block(n)
            m = lax.rem(b, slots)

            @pl.when(lax.div(b, slots) == c)
            def _():
                for h in range(2):
                    b_copy(m, 3, h).wait_recv()
                    i, at = 2 - h, part_of(h)
                    snd2[last, i, at, cols_of(m)] = (
                        snd2[last, i, at, cols_of(m)].astype(jnp.float32)
                        + rec2[last, 3, at, cols_of(m)].astype(jnp.float32)
                    ).astype(jnp.bfloat16)
                    b_copy(m, i, h).start()
                    if h == 0:
                        b_copy(m, 2, 1).start()

        def sums_sent(layer):
            for r in range(1, tp):
                take(part.at[layer, 0], p_send.at[layer, r - 1])
                take(stat.at[layer], s_send.at[layer, r - 1])
            if q > 1:
                take(snd2.at[layer, pl.ds(0, q - 1)], b_send.at[0] if timed and layer == last else r_send.at[layer])

        def s_copy(layer, r, h):
            return remote(
                stat.at[layer, h], stat_in.at[layer, r, h], s_send.at[layer, r - 1], s_recv.at[layer, r - 1, h], at_tp(r)
            )

        def finish(layer, h):
            at = part_of(h)
            pre = alpha * mine(layer, h)[...].astype(jnp.float32) + acc[at, :]
            for i in range(1, min(q, 3)):
                if timed and layer == last:
                    for m in range(slots):
                        b_copy(m, i, h).wait_recv()
                elif halves == 2 and i == 2 - h:
                    for e in range(2):
                        w_copy(layer, h, e).wait_recv()
                else:
                    r_copy(layer, i, h).wait_recv()
                pre = pre + rec2[layer, i, at, :].astype(jnp.float32)
            acc[at, :] = pre
            own = jnp.sum(pre, axis=-1, keepdims=True)
            away = pre - own * (1.0 / feats)
            spread = jnp.sum(away * away, axis=-1, keepdims=True)
            lane = lax.broadcasted_iota(jnp.int32, (half_rows, LANES), 1)
            stat[layer, h] = jnp.where(lane == 0, own, spread)
            for r in range(1, tp):
                s_copy(layer, r, h).start()
            sums, spreads = [own], [spread]
            for r in range(1, tp):
                s_copy(layer, r, h).wait_recv()
                sums.append(stat_in[layer, r, h, :, 0:1])
                spreads.append(stat_in[layer, r, h, :, 1:2])
            mean = sum(sums[1:], sums[0]) * (1.0 / model)
            var = sum(spreads[1:], spreads[0])
            for s in sums:
                off = s * (1.0 / feats) - mean
                var = var + feats * off * off
            scale = lax.rsqrt(var * (1.0 / model) + EPS)
            normed = (acc[at, :] - mean) * scale
            y = (normed * gain[pl.ds(layer, 1), :] + bias[pl.ds(layer, 1), :]).astype(jnp.bfloat16)
            if layer == last:
                res[at, :] = y
            else:
                mine(layer + 1, h)[...] = y


        tasks = []

        def at_time(when, fn, *args):
            tasks.append((when, len(tasks), fn, args))

        def first_half(layer, w0, w1, w2):
            def start():
                gather_wait(layer, False)
                if q > 3:
                    gather_wait(layer, True)
                arrived(layer * 4)
                project(layer, layer, 0, put_u(0), ALL)

            def middle():
                arrived(layer * 4 + 1)
                project(layer, layer, 1, put_z(0), ALL)
                halo_start(layer)

            def gates():
                arrived(layer * 4 + 2)
                project(layer, layer, 2, put_o(0), ALL)
                halo_wait(layer)
                convolve(layer, 0, range(q))
                halo_sent(layer)

            at_time(w0, start)
            at_time(w1, middle)
            at_time(w2, gates)

        def some_of(layer, w, span, fresh):
            if fresh:
                arrived(layer * 4 + w)
            project(layer, layer, w, (put_u, put_z, put_o)[w](0), span)

        def rest_of(layer):
            gather_wait(layer, True)
            project(layer, layer, 0, put_u(0), REST)
            project(layer, layer, 1, put_z(0), REST)
            halo_start(layer)

        def gates_of(layer):
            project(layer, layer, 2, put_o(0), REST)
            halo_wait(layer)
            convolve(layer, 0, range(q))

        def halo_sent(layer):
            @pl.when(l < line - 1)
            def _():
                h_copy(layer).wait_send()

        def second_half(layer, when):
            def go():
                arrived(layer * 4 + 3)
                out_product(layer)

            at_time(when, go)

        if timed:
            at_time(-1.0, far_send)
            for when, k in ((0.0, 0), (0.1, 1), (0.2, 3), (0.3, 4), (0.5, 2), (0.6, 5), (0.7, 6), (0.8, 7)):
                at_time(when, scatter_start, k)
            for h in range(halves):
                at_time(0.4, inner_gather_start, h)
                at_time((8.6, 13.6)[h], far_in, h)
                at_time((20.0, 26.0)[h], inner_pass, 0, h)
                at_time(42.55 + 0.01 * h, inner_onward, 0, h)
                at_time(53.19 + 0.001 * h, inner_last, 0, h)
                at_time(51.0 + 0.05 * h, inner_last, far, h)
            at_time(15.1, far_pass)
            at_time(43.1, far_side)
            at_time(42.5, far_diag)
            for k, when in enumerate((3.5, 6.5, 15.0, 15.2, 15.3, 18.0, 22.0, 24.0)):
                at_time(when, outer_begin, k)
            for k, when in enumerate((3.5, 6.5, 27.5, 9.5, 12.5, 30.0, 38.0, 41.0)):
                at_time(when, inner_ready, k)
            for k, when in enumerate((3.6, 6.6, 27.6, 9.6, 43.2, 57.1, 61.92, 66.2)):
                at_time(when, inward, k, 0)
            for k, when in enumerate((19.0, 25.0, 31.0, 51.5, 57.0, 61.9, 66.1, 67.6)):
                at_time(when, inward, k, 1)
            for k, when in enumerate((9.7, 12.6, 30.1, 38.1, 41.1)):
                at_time(when, outward, k + 3, 0)
            for k, when in ((3, 23.5), (5, 67.5), (6, 79.0), (7, 87.1)):
                at_time(when, outward, k, 1)
            for k, when in ((3, 54.2), (5, 72.5), (6, 82.0)):
                at_time(when, outward, k, 2)
            for s in range(1, 3):
                at_time((61.91, 66.0)[s - 1], outward_for, False, 4, s)
                at_time(67.0005 + 0.0001 * s, outward_for, True, 4, s)
            at_time(33.1, inner_wait, 0, False)
            at_time(33.1, inner_arrived, 0)
            at_time(33.2, inner_project, 0, (0,), MOST)
            at_time(37.0, inner_arrived, 1)
            at_time(37.0, inner_project, 0, (1,), MOST)
            at_time(43.5, inner_wait, far, False)
            at_time(38.2, inner_own)
            at_time(38.2, inner_project, 1, (0, 1), OWN)
            at_time(43.6, inner_project, 1, (0, 1), SIDE)
            at_time(45.5, inner_arrived, 2)
            at_time(45.6, inner_project, 1, (2,), MOST)
            at_time(45.7, far_early)
            at_time(52.0, inner_wait, far, True)
            at_time(52.1, inner_project, 1, (0, 1, 2), REST)
            at_time(53.1, far_gates)
            at_time(53.18, inner_project, 0, (2,), MOST)
            at_time(53.2, inner_wait, 0, True)
            at_time(53.21, inner_project, 0, (0, 1), REST)
            at_time(53.22, own_edge)
            at_time(53.23, far_first)
            at_time(54.21, inner_project, 0, (2,), REST)
            at_time(55.3, own_gates)
            o = 58.0
            at_time(o, line_end, 3, 0)
            for n, i in enumerate((1, 3, 2, 0)):
                at_time(o + 0.1 * n, half_tile, False, i)
                at_time(o + 0.1 * n + 0.15, half_sum, False, i)
            for e in range(2):
                for h in range(2):
                    at_time(o + 8.5 + 0.1 * e + 0.01 * h, half_relay, False, h, e)
            at_time(o + 8.75, line_end, 3, 1)
            at_time(o + 8.75, line_end, 3, 2)
            for n, i in enumerate((3, 2, 1, 0)):
                at_time(o + 4.3 + 0.1 * n, inner_late_tile, i)
                at_time(o + 4.3 + 0.1 * n + 0.15, inner_late_sum, i)
                at_time(o + 8.8 + 0.01 * n, outer_late_tile, i)
                at_time(o + 8.8 + 0.01 * n + 0.015, outer_late_sum, i)
            for e in range(2):
                for h in range(2):
                    at_time(o + 9.0 + 0.1 * e + 0.01 * h, half_relay, True, h, e)
            for h in range(halves):
                f = o + 14.0 + 6.0 * h
                at_time(f, finish, 0, h)
                at_time(f + 0.1, gather_start, 1, h)
                at_time(f + 9.0, gather_pass, 1, h)
                at_time(93.0 + 0.1 * h, gather_last, 1, h)
            at_time(88.0, gather_wait, 1, False)
            at_time(82.5, gather_own, 1)
            at_time(82.5, some_of, 1, 0, OWN, True)
            at_time(87.2, some_of, 1, 1, OWN, True)
            at_time(88.1, some_of, 1, 0, SIDE, False)
            at_time(88.1, some_of, 1, 1, SIDE, False)
            at_time(93.15, some_of, 1, 2, MOST, True)
            at_time(93.2, rest_of, 1)
            at_time(93.5, outward, units - 1, 2)
            at_time(94.0, gates_of, 1)
            at_time(128.0, halo_sent, 1)
            for n in range(1, line):
                at_time((110.0, 110.1, 111.0, 113.0)[n], line_end, units - 1, n - 1)
            for n in range(line):
                at_time((110.0, 110.2, 111.0, 113.0)[n], block_product, n)
                at_time((110.3, 110.4, 111.1, 113.5)[n], block_sum, n)
                at_time((113.1, 113.2, 114.0, 114.1)[n], block_relay, n)
            at_time(127.5, far_sent)
            at_time(128.0, gather_sent, 1)
            at_time(128.1, sums_sent, 0)
            for k in range(units):
                at_time(129.5, all_sent, k)
            for h in range(halves):
                at_time(130.0 + h, finish, last, h)
            at_time(140.0, sums_sent, last)
        else:
            for k in range(units):
                at_time(-2.0 if k < 2 else -1.0, scatter_start, k)
            for h in range(halves):
                at_time(-1.5, gather_start, 0, h)
            begin = [k + k // 4 for k in range(units)]
            for k in range(units):
                at_time(begin[k], line_begin, k)
                for s in range(1, steps):
                    at_time(begin[k] + s, line_pass, k, s)
            end = begin[-1] + max(steps, 1) + 1
            ready = [begin[k] + steps for k in range(units)]
            for layer in range(layers):
                if layer == 0:
                    base = ready[0] + 0.5
                else:
                    base = max(ready[4 * layer - 1] + 4.0, end if layer > 1 else 0) + 0.5
                for h in range(halves):
                    at_time(base - 1.3, gather_pass, layer, h)
                    at_time(base - 1.2, gather_last, layer, h)
                w1 = max(base + 0.1, ready[4 * layer + 1] + 0.5)
                w2 = max(w1 + 0.1, ready[4 * layer + 2] + 0.5)
                first_half(layer, base, w1, w2)
                o = max(w2 + 0.1, ready[4 * layer + 3] + 0.5)
                second_half(layer, o)
                for e in range(2):
                    for h in range(2):
                        at_time(o + 0.1, relay, layer, h, e)
                for h in range(halves):
                    at_time(o + 0.3, finish, layer, h)
                    if layer < last:
                        at_time(o + 0.4, gather_start, layer + 1, h)

        for _, _, fn, args in sorted(tasks, key=lambda task: task[:2]):
            fn(*args)
        if not timed:
            for layer in range(layers):
                gather_sent(layer)
                sums_sent(layer)
            for k in range(units):
                scatter_sent(k)
                for s in range(steps):
                    line_sent(k, s)

    return kernel


def solution(mesh):
    sp, tp = mesh.shape["sp"], mesh.shape["tp"]

    def shards(tokens, value_weight, outer_weight, inner_weight, conv_taps, output_weight, norm_gain, norm_bias):
        rows, feats = tokens.shape
        layers, depth, channels = value_weight.shape
        taps_count = conv_taps.shape[1]
        q = plane_size(sp, channels)
        width = channels // q
        line = sp // q
        model = feats * tp
        alpha = (2.0 * layers) ** 0.25
        out_cols = output_weight.shape[2]
        bf, f32 = jnp.bfloat16, jnp.float32
        kernel = make_kernel(sp, tp, q, layers, taps_count, rows, feats, depth, width, out_cols, alpha)
        dma = pltpu.SemaphoreType.DMA
        units, steps = 4 * layers, max(line - 1, 1)
        others = max(tp - 1, 1)
        banks = 2 if helped(line, q, tp, layers) else 1
        sets = layers + banks - 1
        relays = 1 if banks == 2 else layers
        if banks == 2:
            lines = [dma((units,)), dma((units, steps)), dma((1,)), dma((1,))]
        else:
            lines = [dma((units, steps))] * 4
        halves = 2 if q == 4 else 1
        half_rows = rows // halves
        vm, hbm = pl.BlockSpec(memory_space=pltpu.VMEM), pl.BlockSpec(memory_space=pl.ANY)
        return pl.pallas_call(
            kernel,
            out_shape=jax.ShapeDtypeStruct((rows, feats), bf),
            in_specs=[hbm] * 4 + [vm, hbm, vm, vm],
            out_specs=vm,
            scratch_shapes=[
                pltpu.VMEM((layers + banks - 1, tp, q * rows, feats), bf),
                pltpu.VMEM((layers, 3, model, width), bf),
                pltpu.VMEM((layers, sp, width, out_cols), bf),
                pltpu.VMEM((banks, q * rows, width), bf),
                pltpu.VMEM((banks, q * rows, width), bf),
                pltpu.VMEM((banks, q * rows + 8, width), f32),
                pltpu.VMEM((banks, q * rows, width), bf),
                pltpu.VMEM((layers, tp, q * rows, feats), bf),
                pltpu.VMEM((layers, others, q * rows, feats), bf),
                pltpu.VMEM((layers, q, rows, feats), bf),
                pltpu.VMEM((layers, q, rows, feats), bf),
                pltpu.VMEM((rows, feats), f32),
                pltpu.VMEM((layers, halves, half_rows, LANES), f32),
                pltpu.VMEM((layers, tp, halves, half_rows, LANES), f32),
                pltpu.VMEM((layers, 2, 8, width), f32),
                dma((units,)), dma((units,)), *lines,
                dma((sets,)), dma((sets, 3, halves)), dma((1,)),
                dma((sets, others)), dma((sets, others, 3)),
                dma((layers, others)), dma((layers, max(others, 2), q)),
                dma((layers,)), dma((layers, 2)),
                dma((layers, others)), dma((layers, others, halves)),
                dma((layers,)), dma((layers,)),
                dma((1,)), dma((2, 3, 2)), dma((1,)), dma((4,)), dma((1,)), dma((4,)),
                dma((relays, 2, 2)), dma((relays, 2, 2)), dma((2,)),
                *[pltpu.VMEM(a.shape, bf) for a in (tokens, value_weight, outer_weight, inner_weight, output_weight)],
                dma((5,)),
            ],
            compiler_params=pltpu.CompilerParams(
                collective_id=0, has_side_effects=True, vmem_limit_bytes=60 * 1024 * 1024
            ),
        )(tokens, value_weight, outer_weight, inner_weight, jnp.swapaxes(conv_taps, 0, 1), output_weight, norm_gain, norm_bias)

    in_specs = (
        P("sp", "tp"),
        P(None, "sp", "tp"),
        P(None, "sp", "tp"),
        P(None, "sp", "tp"),
        P(None, None, "tp"),
        P(None, "tp", "sp"),
        P(None, "tp"),
        P(None, "tp"),
    )
    return jax.shard_map(shards, mesh=mesh, in_specs=in_specs, out_specs=P("sp", "tp"), check_vma=False)
```
